512 devices in a mesh: sp: 64 (over z, y), tp: 8 (over x, core).
Axes of the slice: x: 4, y: 4, z: 16, core: 2. Of those that a mesh axis runs over, the one named last changes fastest.
Arguments:
- tokens: bfloat16 [24576, 2048], P(('sp', 'tp')), may hold values from -6 to 6
- norm_gain: float32 [2048], replicated, may hold values from 0.1 to 1.9
- conv_in_weight: bfloat16 [2048, 2048], P('sp', 'tp'), may hold values from -0.125 to 0.125
- conv_gate_weight: bfloat16 [2048, 2048], P('sp', 'tp'), may hold values from -0.125 to 0.125
- conv_taps: float32 [3, 2048], replicated, may hold values from -3 to 3
- query_weight: bfloat16 [2048, 1024], P('sp', 'tp'), may hold values from -0.125 to 0.125
- key_weight: bfloat16 [2048, 1024], P('sp', 'tp'), may hold values from -0.125 to 0.125
- value_weight: bfloat16 [2048, 2048], P('sp', 'tp'), may hold values from -0.125 to 0.125
- decay_down: bfloat16 [2048, 16], replicated, may hold values from -0.125 to 0.125
- decay_up: bfloat16 [16, 1024], replicated, may hold values from -1.5 to 1.5
- decay_bias: float32 [1024], replicated, may hold values from 0.2 to 10
- decay_extra: float32 [8, 24576], P('tp', 'sp'), may hold values from -2.2 to 0
- head_gain: float32 [2048], replicated, may hold values from 0.1 to 1.9
- conv_out_weight: bfloat16 [2048, 2048], P('tp', 'sp'), may hold values from -0.125 to 0.125
- value_out_weight: bfloat16 [2048, 2048], P('tp', 'sp'), may hold values from -0.125 to 0.125
Outputs:
- mixed: bfloat16 [24576, 2048], P(('sp', 'tp'))
The draws below stay inside these ranges and needn't reach their ends.
All inputs are finite; a program needn't handle non-finite values.
Results may differ from the reference program's by a relative error of at most 0.02.
Values may be sent and summed in bfloat16 or wider, within the bound.
A program may use at most 64 MiB of HBM per device.

```python
import math
import jax
import jax.numpy as jnp
from jax import lax

D = 2048
HEADS = 8
KEY_DIM = 128
VAL_DIM = 256
RANK = 16
BLOCK = 64
TOK_DEV = 384
SEQUENCE_TOKENS = 24576
KEYS = 1024
VALS = 2048
N_TP = 8


def head_ranking(key):
    return jax.random.permutation(jax.random.fold_in(key, 5), HEADS)


def role_counts():
    return (max(1, HEADS // 4), max(1, HEADS // 4))


def draw_decay_bias(key, part):
    folded_key = jax.random.fold_in(key, 11)
    slow_key, fast_key = jax.random.split(folded_key, 2)
    ranking = head_ranking(key)
    fast_count, middle_count = role_counts()
    fast_heads = ranking < fast_count
    slow_values = jax.random.uniform(slow_key, (HEADS, KEY_DIM), jnp.float32, 8.0, 10.0)
    fast_values = jax.random.uniform(fast_key, (HEADS, KEY_DIM), jnp.float32, 0.2, 1.2)
    return jnp.where(fast_heads[:, None], fast_values, slow_values).reshape(HEADS * KEY_DIM).astype(jnp.float32)


def draw_decay_extra(key, part):
    folded_key = jax.random.fold_in(key, 23)
    rate_key, place_key, keep_key, middle_key = jax.random.split(folded_key, 4)
    segments = SEQUENCE_TOKENS // TOK_DEV
    ranking = head_ranking(key)
    fast_count, middle_count = role_counts()
    middle_heads = (ranking >= fast_count) & (ranking < fast_count + middle_count)
    lowest, highest = (0.25, 1.0)
    slow_rates = jnp.exp(jax.random.uniform(rate_key, (HEADS, segments), jnp.float32, math.log(lowest), math.log(highest))) / SEQUENCE_TOKENS
    middle_rates = jnp.exp(jax.random.uniform(middle_key, (HEADS, segments), jnp.float32, math.log(0.25), math.log(1.0))) / TOK_DEV
    rates = jnp.where(middle_heads[:, None], middle_rates, slow_rates)
    steady_part = -jnp.repeat(rates, TOK_DEV, axis=1)
    element_slots = jax.random.randint(place_key, (HEADS, 3), 0, SEQUENCE_TOKENS)
    retain_selector = jax.random.uniform(keep_key, (HEADS, 3), jnp.float32, 0.5, 0.8)
    element_indices = jnp.arange(SEQUENCE_TOKENS)
    element_runs = jnp.sum(jnp.where(element_indices[None, None, :] == element_slots[:, :, None], jnp.log(retain_selector)[:, :, None], 0.0), axis=1)
    return (steady_part + element_runs).astype(jnp.float32)


def block_levels(own_key, dims, cuts, least, top_value):
    def one(position, shards_of):
        draws = jax.random.uniform(jax.random.fold_in(jax.random.fold_in(own_key, 6), position), (shards_of,), jnp.float32, least / len(cuts), top_value / len(cuts))
        return jnp.repeat(jnp.exp(draws), dims[position] // shards_of).reshape((-1,) + (1,) * (len(dims) - position - 1))

    gain = one(*cuts[0])
    for cut in cuts[1:]:
        gain = gain * one(*cut)
    return gain


def scatter_about(key, dims, scale, bound, shards=(), dtype=jnp.bfloat16):
    level = block_levels(key, dims, shards, -0.22, 0.18) if shards else 1.0
    values = jax.random.normal(key, dims, jnp.float32) * scale * level
    return jnp.minimum(jnp.maximum(values, -bound), bound).astype(dtype)


def setup_inputs(seed: int = 0) -> dict:
    arg_keys = jax.random.split(jax.random.key(seed), 16)
    tokens = scatter_about(arg_keys[0], (SEQUENCE_TOKENS, D), 1.0, 6.0, ((0, 512),))
    norm_gain = jnp.clip(1.0 + 0.18 * jax.random.normal(arg_keys[1], (D,), jnp.float32), 0.1, 1.9)
    conv_in_weight = scatter_about(arg_keys[2], (D, D), D ** -0.5, 0.125, ((0, 64), (1, 8)))
    conv_gate_weight = scatter_about(arg_keys[3], (D, D), D ** -0.5, 0.125, ((0, 64), (1, 8)))
    conv_taps = scatter_about(arg_keys[4], (3, D), 0.6, 3.0, (), jnp.float32)
    query_weight = scatter_about(arg_keys[5], (D, KEYS), D ** -0.5, 0.125, ((0, 64), (1, 8)))
    key_weight = scatter_about(arg_keys[6], (D, KEYS), D ** -0.5, 0.125, ((0, 64), (1, 8)))
    value_weight = scatter_about(arg_keys[7], (D, VALS), D ** -0.5, 0.125, ((0, 64), (1, 8)))
    decay_down = scatter_about(arg_keys[8], (D, RANK), D ** -0.5, 0.125)
    decay_up = scatter_about(arg_keys[9], (RANK, KEYS), RANK ** -0.5, 1.5)
    decay_bias = draw_decay_bias(jax.random.fold_in(arg_keys[15], 71), 0)
    decay_extra = draw_decay_extra(jax.random.fold_in(arg_keys[15], 71), 0)
    head_gain = jnp.clip(1.0 + 0.18 * jax.random.normal(arg_keys[12], (VALS,), jnp.float32), 0.1, 1.9)
    conv_out_weight = scatter_about(arg_keys[13], (D, D), D ** -0.5, 0.125, ((0, 8), (1, 64)))
    value_out_weight = scatter_about(arg_keys[14], (VALS, D), VALS ** -0.5, 0.125, ((0, 8), (1, 64)))
    return dict(tokens=tokens, norm_gain=norm_gain, conv_in_weight=conv_in_weight, conv_gate_weight=conv_gate_weight, conv_taps=conv_taps, query_weight=query_weight, key_weight=key_weight, value_weight=value_weight, decay_down=decay_down, decay_up=decay_up, decay_bias=decay_bias, decay_extra=decay_extra, head_gain=head_gain, conv_out_weight=conv_out_weight, value_out_weight=value_out_weight)


precise = lax.Precision.HIGHEST
EPSILON = 1e-06

def rms_rows(inputs, scale_gain):
    floats = inputs.astype(jnp.float32)
    return floats * lax.rsqrt(lax.optimization_barrier(jnp.mean(floats * floats, axis=-1, keepdims=True)) + EPSILON) * scale_gain

def rounded(inputs):
    return lax.optimization_barrier(inputs.astype(jnp.bfloat16)).astype(jnp.float32)

def forward_block(passed_along_state, inputs):
    query_float, key_float, value_float, decay_block = inputs
    cumul = jnp.cumsum(decay_block, axis=0)
    totals = cumul[-1]
    element_indices = jnp.arange(query_float.shape[0])
    lower_mask = element_indices[:, None] >= element_indices[None, :]
    query_decayed = query_float * jnp.exp(cumul)
    scores = jnp.einsum('ihd,jhd->hij', query_decayed, key_float * jnp.exp(-cumul), precision=precise)
    scores = jnp.where(lower_mask[None], scores, 0.0)
    result = jnp.einsum('hij,jhe->ihe', scores, value_float, precision=precise)
    result = result + jnp.einsum('ihd,hde->ihe', query_decayed, passed_along_state, precision=precise)
    key_end = key_float * jnp.exp(totals[None] - cumul)
    updated = jnp.exp(totals)[..., None] * passed_along_state + jnp.einsum('jhd,jhe->hde', key_end, value_float, precision=precise)
    return (updated, result)

def backward_block(passed_along_state, inputs):
    query_float, key_float, value_float, decay_block = inputs
    cumul = jnp.cumsum(decay_block, axis=0)
    before = cumul - decay_block
    totals = cumul[-1]
    element_indices = jnp.arange(query_float.shape[0])
    upper_triangle_mask = element_indices[:, None] <= element_indices[None, :]
    key_start = key_float * jnp.exp(before)
    scores = jnp.einsum('ihd,jhd->hij', query_float * jnp.exp(-before), key_start, precision=precise)
    scores = jnp.where(upper_triangle_mask[None], scores, 0.0)
    result = jnp.einsum('hij,jhe->ihe', scores, value_float, precision=precise)
    result = result + jnp.einsum('ihd,hde->ihe', query_float * jnp.exp(totals[None] - before), passed_along_state, precision=precise)
    updated = jnp.exp(totals)[..., None] * passed_along_state + jnp.einsum('jhd,jhe->hde', key_start, value_float, precision=precise)
    return (updated, result)

def reference(tokens, norm_gain, conv_in_weight, conv_gate_weight, conv_taps, query_weight, key_weight, value_weight, decay_down, decay_up, decay_bias, decay_extra, head_gain, conv_out_weight, value_out_weight):
    normed = rms_rows(tokens, norm_gain).astype(jnp.bfloat16)
    conv_in = rounded(jnp.dot(normed, conv_in_weight, preferred_element_type=jnp.float32))
    conv_gate = rounded(jnp.dot(normed, conv_gate_weight, preferred_element_type=jnp.float32))
    padded = jnp.pad(conv_in, ((1, 1), (0, 0)))
    mixed_conv = padded[:-2] * conv_taps[0] + padded[1:-1] * conv_taps[1] + padded[2:] * conv_taps[2]
    conv_mixed = (mixed_conv * jax.nn.silu(conv_gate)).astype(jnp.bfloat16)
    queries = (jnp.dot(normed, query_weight, preferred_element_type=jnp.float32) * (1.0 / math.sqrt(KEY_DIM))).astype(jnp.bfloat16)
    key_rows = jnp.dot(normed, key_weight, preferred_element_type=jnp.float32).astype(jnp.bfloat16)
    values = jnp.dot(normed, value_weight, preferred_element_type=jnp.float32).astype(jnp.bfloat16)
    low_rank = jnp.dot(normed, decay_down, preferred_element_type=jnp.float32).astype(jnp.bfloat16)
    log_decay = jax.nn.log_sigmoid(jnp.dot(low_rank, decay_up, preferred_element_type=jnp.float32) + decay_bias) / 16.0
    log_decay = log_decay.reshape(SEQUENCE_TOKENS, HEADS, KEY_DIM) + decay_extra.T[:, :, None]
    blocks = SEQUENCE_TOKENS // BLOCK
    query_float = queries.astype(jnp.float32).reshape(blocks, BLOCK, HEADS, KEY_DIM)
    key_float = key_rows.astype(jnp.float32).reshape(blocks, BLOCK, HEADS, KEY_DIM)
    value_float = values.astype(jnp.float32).reshape(blocks, BLOCK, HEADS, VAL_DIM)
    decay_blocks = log_decay.reshape(blocks, BLOCK, HEADS, KEY_DIM)
    blank_memory = jnp.zeros((HEADS, KEY_DIM, VAL_DIM), jnp.float32)
    inputs = (query_float, key_float, value_float, decay_blocks)
    _, forward_out = lax.scan(forward_block, blank_memory, inputs)
    _, backward_out = lax.scan(backward_block, blank_memory, inputs, reverse=True)
    raw_mixed = (forward_out + backward_out).reshape(SEQUENCE_TOKENS, HEADS, VAL_DIM)
    gla_mixed = rms_rows(raw_mixed, head_gain.reshape(HEADS, VAL_DIM)).astype(jnp.bfloat16).reshape(SEQUENCE_TOKENS, VALS)
    channels = D // N_TP
    val_width = VALS // N_TP
    summed = jnp.zeros((SEQUENCE_TOKENS, D), jnp.float32)
    for member in range(N_TP):
        partial_value = jnp.dot(conv_mixed[:, member * channels:(member + 1) * channels], conv_out_weight[member * channels:(member + 1) * channels], preferred_element_type=jnp.float32)
        partial_value = partial_value + jnp.dot(gla_mixed[:, member * val_width:(member + 1) * val_width], value_out_weight[member * val_width:(member + 1) * val_width], preferred_element_type=jnp.float32)
        summed = summed + rounded(partial_value)
    return summed.astype(jnp.bfloat16)
```

```python
import functools
import math

import jax
import jax.numpy as jnp
from jax import lax
from jax.experimental import pallas as pl
from jax.experimental.pallas import tpu as pltpu
from jax.sharding import Mesh
from jax.sharding import PartitionSpec as P

NZ, NY, NX, NC = 16, 4, 4, 2
KEY_DIM = 128
VAL_DIM = 256
BLOCK = 64
ROWS = 48
LEN = 384
WIDTH = 2048
EPSILON = 1e-06
SP = ("z", "y")
TP = ("x", "c")
SP_TP = ("z", "y", "x", "c")
F32 = jnp.float32
BF16 = jnp.bfloat16
MESH = pl.DeviceIdType.MESH
N_SEND = 192
N_RECV = 192


def mm(a, b):
    return lax.dot_general(a, b, (((1,), (0,)), ((), ())), preferred_element_type=F32)


def mm_nt(a, b):
    return lax.dot_general(a, b, (((1,), (1,)), ((), ())), preferred_element_type=F32)


def mm_tn(a, b):
    return lax.dot_general(a, b, (((0,), (0,)), ((), ())), preferred_element_type=F32)


def wrap(value, size):
    return lax.rem(value + size, size)


def split3(row):
    hi = row.astype(BF16)
    rest = row - hi.astype(F32)
    mid = rest.astype(BF16)
    low = (rest - mid.astype(F32)).astype(BF16)
    return hi, mid, low


def log_rows(row):
    hi, mid, low = split3(row)
    index = lax.broadcasted_iota(jnp.int32, (16, KEY_DIM), 0)
    spread = [jnp.broadcast_to(p.astype(F32), (16, KEY_DIM)) for p in (hi, mid, low)]
    out = jnp.where(index == 0, spread[0], jnp.where(index == 1, spread[1], jnp.where(index == 2, spread[2], 0.0)))
    return out.astype(BF16)


def log_total(rows16):
    return jnp.sum(rows16.astype(F32), axis=0, keepdims=True)


def kernel(
    tok, norm_gain, wa, wb, taps, ddown, dup, dbias, dextra, hgain,
    out,
    WA, WB, T, SS, R1, M2, R2, M3, IF, IB, CI, CP, HP, HN, XC, PO, PS, PR, XS, XR,
    ssem, rsem,
):
    z, y, x, c = (lax.axis_index(a) for a in SP_TP)
    tp = x * 2 + c
    s = z * 4 + y
    other = 1 - c
    names = {}
    sends = []

    def at(dz=0, dy=0, dx=0, flip=False):
        return (wrap(z + dz, NZ), wrap(y + dy, NY), wrap(x + dx, NX), other if flip else c)

    def sem(name):
        return rsem.at[names.setdefault(name, len(names))]

    def send(src, dst, name, device):
        copy = pltpu.make_async_remote_copy(
            src_ref=src, dst_ref=dst, send_sem=ssem.at[len(sends)], recv_sem=sem(name),
            device_id=device, device_id_type=MESH,
        )
        copy.start()
        sends.append(copy)

    def arrived(dst, name):
        pltpu.make_async_remote_copy(
            src_ref=dst, dst_ref=dst, send_sem=ssem.at[0], recv_sem=sem(name),
            device_id=(z, y, x, c), device_id_type=MESH,
        ).wait_recv()

    after = lax.rem(s + 1, NZ * NY)
    ahead = lax.rem(s + NZ * NY - 1, NZ * NY)
    next_dev = (after // NY, lax.rem(after, NY), x, c)
    prev_dev = (ahead // NY, lax.rem(ahead, NY), x, c)
    peers = [at(dz=d) for d in range(1, NZ)]
    peers += [at(dy=d) for d in range(1, NY)]
    peers += [at(dx=d) for d in range(1, NX)]
    peers += [at(flip=True), next_dev, prev_dev]
    barrier = pltpu.get_barrier_semaphore()
    for peer in peers:
        pl.semaphore_signal(barrier, inc=1, device_id=peer, device_id_type=MESH)

    def token_rows(dx=0, flip=False):
        index = wrap(x + dx, NX) * 2 + (other if flip else c)
        return pl.ds(pl.multiple_of(index * ROWS, 16), ROWS)

    raw_rows = tok[...].astype(F32)
    scale = lax.rsqrt(jnp.mean(raw_rows * raw_rows, axis=-1, keepdims=True) + EPSILON)
    T[token_rows(), :] = (raw_rows * scale * norm_gain[...]).astype(BF16)

    def slot(dz=0, dy=0):
        index = wrap(z + dz, NZ) * NY + wrap(y + dy, NY)
        return pl.ds(pl.multiple_of(index * 32, 32), 32)

    def plane(dz=0):
        return pl.ds(pl.multiple_of(wrap(z + dz, NZ) * 128, 128), 128)

    WA[slot(), :] = wa[...]
    WB[slot(), :] = wb[...]

    pl.semaphore_wait(barrier, len(peers))

    for d in range(1, NY):
        send(wa, WA.at[slot()], ("ay", d), at(dy=d))
    own_rows = T.at[token_rows()]
    send(own_rows, own_rows, "tm", at(dx=1))
    send(own_rows, own_rows, "tp", at(dx=-1))
    send(own_rows, own_rows, ("tc", 0), at(flip=True))
    send(wb, WB.at[slot()], ("zm", 1), at(dz=1))
    send(wb, WB.at[slot()], ("zp", 1), at(dz=-1))
    send(wb, WB.at[slot()], ("ym", 0), at(dy=1))
    send(wb, WB.at[slot()], ("yp", 0), at(dy=-1))

    for d in range(1, NY):
        arrived(WA.at[slot(dy=-d)], ("ay", d))
    send(WA.at[plane()], WA.at[plane()], ("am", 1), at(dz=1))
    send(WA.at[plane()], WA.at[plane()], ("ap", 1), at(dz=-1))

    half = WIDTH // 2

    def token_step(stage):
        if stage == 0:
            ref = T.at[token_rows(dx=-1)]
            arrived(ref, "tm")
            piece = T.at[token_rows(dx=-1), pl.ds(0, half)]
            send(piece, piece, "t2a", at(dx=1))
            send(ref, ref, ("tc", 1), at(flip=True))
            ref = T.at[token_rows(dx=1)]
            arrived(ref, "tp")
            piece = T.at[token_rows(dx=1), pl.ds(half, half)]
            send(piece, piece, "t2b", at(dx=-1))
            send(ref, ref, ("tc", 2), at(flip=True))
        else:
            arrived(T.at[token_rows(dx=2), pl.ds(0, half)], "t2a")
            arrived(T.at[token_rows(dx=2), pl.ds(half, half)], "t2b")
            ref = T.at[token_rows(dx=2)]
            send(ref, ref, ("tc", 3), at(flip=True))

    def place(j):
        return 0 if j == 0 else (-j if j <= 8 else j - 8)

    def plus(j):
        return (j % 2 == 0) if j <= 8 else ((j - 8) % 2 == 1)

    def column_step(j):
        dz = place(j)
        ref = WB.at[slot(dz, -1)]
        arrived(ref, ("ym", j))
        if plus(j):
            send(ref, ref, ("y2", j), at(dy=1))
        ref = WB.at[slot(dz, 1)]
        arrived(ref, ("yp", j))
        if not plus(j):
            send(ref, ref, ("y2", j), at(dy=-1))

    def fan_out(j):
        ref = WB.at[slot(place(j))]
        send(ref, ref, ("ym", j), at(dy=1))
        send(ref, ref, ("yp", j), at(dy=-1))

    for k in range(1, 9):
        ref = WA.at[plane(-k)]
        arrived(ref, ("am", k))
        if k < 8:
            send(ref, ref, ("am", k + 1), at(dz=1))
            ref = WA.at[plane(k)]
            arrived(ref, ("ap", k))
            if k < 7:
                send(ref, ref, ("ap", k + 1), at(dz=-1))
        ref = WB.at[slot(-k)]
        arrived(ref, ("zm", k))
        if k < 8:
            send(ref, ref, ("zm", k + 1), at(dz=1))
        fan_out(k)
        if k < 8:
            ref = WB.at[slot(k)]
            arrived(ref, ("zp", k))
            if k < 7:
                send(ref, ref, ("zp", k + 1), at(dz=-1))
            fan_out(8 + k)
        if k == 2:
            token_step(0)
        if k == 4:
            token_step(1)
        column_step(k - 1)
        if k > 1:
            column_step(7 + k)
    column_step(8)
    for j in range(4):
        arrived(T.at[token_rows(dx=(0, -1, 1, 2)[j], flip=True)], ("tc", j))
    for j in range(16):
        arrived(WB.at[slot(place(j), 2)], ("y2", j))

    normed = T[...]
    kv = mm(normed, WA[...])
    key_f = kv[:, :KEY_DIM].astype(BF16).astype(F32)
    value = kv[:, KEY_DIM:].astype(BF16)
    low = mm(normed, ddown[...]).astype(BF16)
    key_cols = pl.ds(pl.multiple_of(tp * KEY_DIM, KEY_DIM), KEY_DIM)
    val_cols = pl.ds(pl.multiple_of(tp * VAL_DIM, VAL_DIM), VAL_DIM)
    pre = mm(low, dup[:, key_cols]) + dbias[:, key_cols]
    log_sig = jnp.minimum(pre, 0.0) - jnp.log1p(jnp.exp(-jnp.abs(pre)))
    extra = jnp.transpose(jnp.broadcast_to(dextra[...], (KEY_DIM, LEN)))
    log_decay = log_sig / 16.0 + extra
    ri = lax.broadcasted_iota(jnp.int32, (LEN, LEN), 0)
    ci = lax.broadcasted_iota(jnp.int32, (LEN, LEN), 1)
    tri = jnp.where((ri >= ci) & (ri // BLOCK == ci // BLOCK), 1.0, 0.0).astype(F32)
    cumul = lax.dot_general(
        tri, log_decay, (((1,), (0,)), ((), ())), precision=lax.Precision.HIGHEST, preferred_element_type=F32
    )
    before = cumul - log_decay
    blocks = LEN // BLOCK

    def part(array, n):
        return array[n * BLOCK : (n + 1) * BLOCK]

    totals = [cumul[(n + 1) * BLOCK - 1 : (n + 1) * BLOCK] for n in range(blocks)]
    offsets = [jnp.zeros((1, KEY_DIM), F32)]
    for n in range(blocks):
        offsets.append(offsets[-1] + totals[n])
    whole = offsets[blocks]
    suffix = [jnp.zeros((1, KEY_DIM), F32)]
    for n in reversed(range(blocks)):
        suffix.append(suffix[-1] + totals[n])
    suffix = suffix[::-1][1:]
    to_end = jnp.concatenate([suffix[n] + totals[n] - part(cumul, n) for n in range(blocks)], axis=0)
    from_start = jnp.concatenate([offsets[n] + part(before, n) for n in range(blocks)], axis=0)
    fwd_device = mm_tn(value, (key_f * jnp.exp(to_end)).astype(BF16))
    back_device = mm_tn(value, (key_f * jnp.exp(from_start)).astype(BF16))

    marks = log_rows(whole)
    for q in range(NY):
        SS[q * 144 : q * 144 + 64, :] = fwd_device[q * 64 : q * 64 + 64].astype(BF16)
        SS[q * 144 + 64 : q * 144 + 128, :] = back_device[q * 64 : q * 64 + 64].astype(BF16)
        SS[q * 144 + 128 : q * 144 + 144, :] = marks

    def message(dy=0):
        return pl.ds(pl.multiple_of(wrap(y + dy, NY) * 144, 16), 144)

    R1[message(), :] = SS[message(), :]
    for d in range(1, NY):
        send(SS.at[message(d)], R1.at[message()], ("s1", d), at(dy=d))

    qcg = mm(normed, WB[:, 0:640])
    query_f = (qcg[:, :KEY_DIM] * (1.0 / math.sqrt(KEY_DIM))).astype(BF16).astype(F32)
    conv_in = qcg[:, KEY_DIM : KEY_DIM + 256].astype(BF16)
    gate = qcg[:, KEY_DIM + 256 :].astype(BF16).astype(F32)
    CI[...] = conv_in
    CP[8 : 8 + LEN, :] = conv_in.astype(F32)
    send(CI.at[pl.ds(LEN - 16, 16)], HP, "hp", next_dev)
    send(CI.at[pl.ds(0, 16)], HN, "hn", prev_dev)

    for d in range(1, NY):
        arrived(R1.at[message(-d)], ("s1", d))
    in_f, in_b, in_l = [], [], []
    for q in range(NY):
        in_f.append(R1[q * 144 : q * 144 + 64, :].astype(F32))
        in_b.append(R1[q * 144 + 64 : q * 144 + 128, :].astype(F32))
        in_l.append(log_total(R1[q * 144 + 128 : q * 144 + 144, :]))
    total_f = jnp.zeros((64, KEY_DIM), F32)
    total_b = jnp.zeros((64, KEY_DIM), F32)
    log_f = jnp.zeros((1, KEY_DIM), F32)
    log_b = jnp.zeros((1, KEY_DIM), F32)
    plane_f, plane_b, gap_f, gap_b = ([None] * NY for _ in range(4))
    for q in range(NY):
        plane_f[q], gap_f[q] = total_f, log_f
        total_f = jnp.exp(in_l[q]) * total_f + in_f[q]
        log_f = log_f + in_l[q]
    for q in reversed(range(NY)):
        plane_b[q], gap_b[q] = total_b, log_b
        total_b = jnp.exp(in_l[q]) * total_b + in_b[q]
        log_b = log_b + in_l[q]
    marks = log_rows(log_f)
    M2[0:64, :] = total_f.astype(BF16)
    M2[64:80, :] = marks
    M2[80:144, :] = total_b.astype(BF16)
    M2[144:160, :] = marks

    def depth(dz=0):
        return pl.ds(pl.multiple_of(wrap(z + dz, NZ) * 80, 16), 80)

    R2[depth(), :] = M2[0:80, :]
    for d in (8, 7, 9, 6, 10, 5, 11, 4, 12, 3, 13, 2, 14, 1, 15):
        start = pl.multiple_of(((z + d) // NZ) * 80, 16)
        send(M2.at[pl.ds(start, 80)], R2.at[depth()], ("s2", d), at(dz=d))

    lower = lax.broadcasted_iota(jnp.int32, (BLOCK, BLOCK), 0) >= lax.broadcasted_iota(jnp.int32, (BLOCK, BLOCK), 1)
    upper = lax.broadcasted_iota(jnp.int32, (BLOCK, BLOCK), 0) <= lax.broadcasted_iota(jnp.int32, (BLOCK, BLOCK), 1)
    within = []
    fwd_inc, back_inc, fwd_query, back_query = [], [], [], []
    for n in range(blocks):
        cum_n, bef_n, key_n, query_n, value_n = (part(a, n) for a in (cumul, before, key_f, query_f, value))
        fq = (query_n * jnp.exp(cum_n)).astype(BF16)
        ks = (key_n * jnp.exp(bef_n)).astype(BF16)
        fwd_scores = mm_nt(fq, (key_n * jnp.exp(-cum_n)).astype(BF16))
        back_scores = mm_nt((query_n * jnp.exp(-bef_n)).astype(BF16), ks)
        scores = jnp.where(lower, fwd_scores, 0.0) + jnp.where(upper, back_scores, 0.0)
        within.append(mm(scores.astype(BF16), value_n))
        fwd_inc.append(mm_tn(value_n, (key_n * jnp.exp(totals[n] - cum_n)).astype(BF16)))
        back_inc.append(mm_tn(value_n, ks))
        fwd_query.append(fq)
        back_query.append((query_n * jnp.exp(totals[n] - bef_n)).astype(BF16))
    state = fwd_inc[0]
    for n in range(1, blocks):
        within[n] = within[n] + mm_nt(fwd_query[n], state.astype(BF16))
        state = jnp.exp(totals[n]) * state + fwd_inc[n]
    state = back_inc[blocks - 1]
    for n in reversed(range(blocks - 1)):
        within[n] = within[n] + mm_nt(back_query[n], state.astype(BF16))
        state = jnp.exp(totals[n]) * state + back_inc[n]
    local = jnp.concatenate(within, axis=0)
    far_fwd = jnp.concatenate(
        [part(query_f, n) * jnp.exp(offsets[n] + part(cumul, n)) for n in range(blocks)], axis=0
    ).astype(BF16)
    far_back = jnp.concatenate(
        [part(query_f, n) * jnp.exp(suffix[n] + (totals[n] - part(before, n))) for n in range(blocks)], axis=0
    ).astype(BF16)

    arrived(HP, "hp")
    arrived(HN, "hn")
    first = HP[...].astype(F32)[15:16]
    last = HN[...].astype(F32)[0:1]
    CP[7:8, :] = jnp.where(s > 0, first, 0.0)
    CP[8 + LEN : 9 + LEN, :] = jnp.where(s < NZ * NY - 1, last, 0.0)
    tap = taps[:, val_cols]
    mixed = CP[7 : 7 + LEN, :] * tap[0:1] + CP[8 : 8 + LEN, :] * tap[1:2] + CP[9 : 9 + LEN, :] * tap[2:3]
    XC[:, 0:256] = (mixed * (gate * (1.0 / (1.0 + jnp.exp(-gate))))).astype(BF16)

    for d in range(1, NZ):
        arrived(R2.at[depth(-d)], ("s2", d))
    sum_f = jnp.zeros((64, KEY_DIM), F32)
    sum_b = jnp.zeros((64, KEY_DIM), F32)
    for k in range(NZ):
        step = jnp.exp(log_total(R2[k * 80 + 64 : k * 80 + 80, :])) * sum_f + R2[k * 80 : k * 80 + 64, :].astype(F32)
        sum_f = jnp.where(k < z, step, sum_f)
    for k in reversed(range(NZ)):
        step = jnp.exp(log_total(R2[k * 80 + 64 : k * 80 + 80, :])) * sum_b + R2[k * 80 : k * 80 + 64, :].astype(F32)
        sum_b = jnp.where(k > z, step, sum_b)
    for q in range(NY):
        M3[q * 128 : q * 128 + 64, :] = (plane_f[q] + jnp.exp(gap_f[q]) * sum_f).astype(BF16)
        M3[q * 128 + 64 : q * 128 + 128, :] = (plane_b[q] + jnp.exp(gap_b[q]) * sum_b).astype(BF16)

    def quarter(dy=0):
        return pl.ds(pl.multiple_of(wrap(y + dy, NY) * 64, 64), 64)

    def answer(dy, which):
        return pl.ds(pl.multiple_of(wrap(y + dy, NY) * 128 + 64 * which, 64), 64)

    for d in range(1, NY):
        send(M3.at[answer(d, 0)], IF.at[quarter()], ("s3f", d), at(dy=d))
        send(M3.at[answer(d, 1)], IB.at[quarter()], ("s3b", d), at(dy=d))
    IF[quarter(), :] = M3[answer(0, 0), :]
    IB[quarter(), :] = M3[answer(0, 1), :]
    for d in range(1, NY):
        arrived(IF.at[quarter(-d)], ("s3f", d))
        arrived(IB.at[quarter(-d)], ("s3b", d))
    raw = local + mm_nt(far_fwd, IF[...]) + mm_nt(far_back, IB[...])
    norm = lax.rsqrt(jnp.mean(raw * raw, axis=-1, keepdims=True) + EPSILON)
    XC[:, 256:512] = (raw * norm * hgain[:, val_cols]).astype(BF16)

    def block4(r):
        return pl.ds(r * ROWS, ROWS)

    order = (2, 1, 3, 0)
    there = jnp.concatenate([XC[token_rows(dx=r, flip=True), :] for r in order], axis=0)
    here = jnp.concatenate([XC[token_rows(dx=r), :] for r in order], axis=0)
    for n in range(0, WIDTH, 512):
        PS[:, n : n + 512] = mm_nt(there, WB[n : n + 512, 640:1152]).astype(BF16)
    for i in range(4):
        send(PS.at[block4(i)], PR.at[block4(i)], ("pr", i), at(flip=True))
    for n in range(0, WIDTH, 512):
        PO[:, n : n + 512] = mm_nt(here, WB[n : n + 512, 640:1152])
    for i in range(3):
        arrived(PR.at[block4(i)], ("pr", i))
        XS[i * ROWS : (i + 1) * ROWS, :] = (
            PO[i * ROWS : (i + 1) * ROWS, :] + PR[i * ROWS : (i + 1) * ROWS, :].astype(F32)
        ).astype(BF16)
        send(XS.at[block4(i)], XR.at[block4(i)], ("xr", i), at(dx=order[i]))
    arrived(PR.at[block4(3)], ("pr", 3))
    total = PO[3 * ROWS :, :] + PR[3 * ROWS :, :].astype(F32)
    for i in (1, 2, 0):
        arrived(XR.at[block4(i)], ("xr", i))
        total = total + XR[i * ROWS : (i + 1) * ROWS, :].astype(F32)
    out[...] = total.astype(BF16)

    for copy in sends:
        copy.wait_send()
    assert len(sends) <= N_SEND and len(names) <= N_RECV, (len(sends), len(names))


def local(
    tokens, norm_gain, conv_in_weight, conv_gate_weight, conv_taps, query_weight, key_weight, value_weight,
    decay_down, decay_up, decay_bias, decay_extra, head_gain, conv_out_weight, value_out_weight,
):
    wa = jnp.concatenate([key_weight, value_weight], axis=1)
    wb = jnp.concatenate(
        [query_weight, conv_in_weight, conv_gate_weight, conv_out_weight.T, value_out_weight.T], axis=1
    )
    vmem = pl.BlockSpec(memory_space=pltpu.VMEM)
    return pl.pallas_call(
        kernel,
        out_shape=jax.ShapeDtypeStruct((ROWS, WIDTH), BF16),
        in_specs=[vmem] * 10,
        out_specs=vmem,
        scratch_shapes=[
            pltpu.VMEM((2048, 384), BF16),
            pltpu.VMEM((2048, 1152), BF16),
            pltpu.VMEM((LEN, WIDTH), BF16),
            pltpu.VMEM((NY * 144, KEY_DIM), BF16),
            pltpu.VMEM((NY * 144, KEY_DIM), BF16),
            pltpu.VMEM((160, KEY_DIM), BF16),
            pltpu.VMEM((NZ * 80, KEY_DIM), BF16),
            pltpu.VMEM((NY * 128, KEY_DIM), BF16),
            pltpu.VMEM((VAL_DIM, KEY_DIM), BF16),
            pltpu.VMEM((VAL_DIM, KEY_DIM), BF16),
            pltpu.VMEM((LEN, 256), BF16),
            pltpu.VMEM((LEN + 16, 256), F32),
            pltpu.VMEM((16, 256), BF16),
            pltpu.VMEM((16, 256), BF16),
            pltpu.VMEM((LEN, 512), BF16),
            pltpu.VMEM((4 * ROWS, WIDTH), F32),
            pltpu.VMEM((4 * ROWS, WIDTH), BF16),
            pltpu.VMEM((4 * ROWS, WIDTH), BF16),
            pltpu.VMEM((3 * ROWS, WIDTH), BF16),
            pltpu.VMEM((3 * ROWS, WIDTH), BF16),
            pltpu.SemaphoreType.DMA((N_SEND,)),
            pltpu.SemaphoreType.DMA((N_RECV,)),
        ],
        compiler_params=pltpu.CompilerParams(collective_id=0, has_side_effects=True, vmem_limit_bytes=60 * 1024 * 1024),
        cost_estimate=pl.CostEstimate(flops=3_000_000_000, bytes_accessed=1_000_000, transcendentals=0),
    )(
        tokens, norm_gain.reshape(1, -1), wa, wb, conv_taps, decay_down, decay_up,
        decay_bias.reshape(1, -1), decay_extra, head_gain.reshape(1, -1),
    )


def solution(mesh):
    torus = Mesh(mesh.devices.reshape(NZ, NY, NX, NC), SP_TP)
    return jax.shard_map(
        local,
        mesh=torus,
        in_specs=(
            P(SP_TP, None), P(), P(SP, TP), P(SP, TP), P(), P(SP, TP), P(SP, TP), P(SP, TP),
            P(), P(), P(), P(TP, SP), P(), P(TP, SP), P(TP, SP),
        ),
        out_specs=P(SP_TP, None),
        check_vma=False,
    )
```

```python
import functools
import math

import jax
import jax.numpy as jnp
from jax import lax
from jax.experimental import pallas as pl
from jax.experimental.pallas import tpu as pltpu
from jax.sharding import Mesh
from jax.sharding import PartitionSpec as P

NZ, NY, NX, NC = 16, 4, 4, 2
KEY_DIM = 128
VAL_DIM = 256
BLOCK = 64
ROWS = 48
LEN = 384
WIDTH = 2048
EPSILON = 1e-06
SP = ("z", "y")
TP = ("x", "c")
SP_TP = ("z", "y", "x", "c")
F32 = jnp.float32
BF16 = jnp.bfloat16
MESH = pl.DeviceIdType.MESH
N_SEND = 256
N_RECV = 256


def mm(a, b):
    return lax.dot_general(a, b, (((1,), (0,)), ((), ())), preferred_element_type=F32)


def mm_nt(a, b):
    return lax.dot_general(a, b, (((1,), (1,)), ((), ())), preferred_element_type=F32)


def mm_tn(a, b):
    return lax.dot_general(a, b, (((0,), (0,)), ((), ())), preferred_element_type=F32)


def wrap(value, size):
    return lax.rem(value + size, size)


def split3(row):
    hi = row.astype(BF16)
    rest = row - hi.astype(F32)
    mid = rest.astype(BF16)
    low = (rest - mid.astype(F32)).astype(BF16)
    return hi, mid, low


def log_rows(row):
    hi, mid, low = split3(row)
    index = lax.broadcasted_iota(jnp.int32, (16, KEY_DIM), 0)
    spread = [jnp.broadcast_to(p.astype(F32), (16, KEY_DIM)) for p in (hi, mid, low)]
    out = jnp.where(index == 0, spread[0], jnp.where(index == 1, spread[1], jnp.where(index == 2, spread[2], 0.0)))
    return out.astype(BF16)


def log_total(rows16):
    return jnp.sum(rows16.astype(F32), axis=0, keepdims=True)


def kernel(
    tok_h, gain_h, ci_h, cg_h, taps_h, q_h, k_h, v_h, dd_h, du_h, db_h, de_h, hg_h, co_h, vo_h,
    out,
    tok, norm_gain, taps, ddown, dup, dbias, dextra, hgain,
    WA, WB, WC, T, SS, R1, M2, R2, M3, IF, IB, CI, CP, HP, HN, XC, PO, PS, PR, XS, XR,
    ssem, rsem, lsem,
):
    z, y, x, c = (lax.axis_index(a) for a in SP_TP)
    tp = x * 2 + c
    s = z * 4 + y
    other = 1 - c
    names = {}
    sends = []

    def at(dz=0, dy=0, dx=0, flip=False):
        return (wrap(z + dz, NZ), wrap(y + dy, NY), wrap(x + dx, NX), other if flip else c)

    def sem(name):
        return rsem.at[names.setdefault(name, len(names))]

    def send(src, dst, name, device):
        copy = pltpu.make_async_remote_copy(
            src_ref=src, dst_ref=dst, send_sem=ssem.at[len(sends)], recv_sem=sem(name),
            device_id=device, device_id_type=MESH,
        )
        copy.start()
        sends.append(copy)

    def arrived(dst, name):
        pltpu.make_async_remote_copy(
            src_ref=dst, dst_ref=dst, send_sem=ssem.at[0], recv_sem=sem(name),
            device_id=(z, y, x, c), device_id_type=MESH,
        ).wait_recv()

    after = lax.rem(s + 1, NZ * NY)
    ahead = lax.rem(s + NZ * NY - 1, NZ * NY)
    next_dev = (after // NY, lax.rem(after, NY), x, c)
    prev_dev = (ahead // NY, lax.rem(ahead, NY), x, c)
    peers = [at(dz=d) for d in (1, -1)]
    peers += [at(dy=d) for d in range(1, NY)]
    peers += [at(dx=d) for d in range(1, NX)]
    peers += [at(flip=True), next_dev, prev_dev]
    barrier = pltpu.get_barrier_semaphore()
    for peer in peers:
        pl.semaphore_signal(barrier, inc=1, device_id=peer, device_id_type=MESH)

    def slot(dz=0, dy=0):
        index = wrap(z + dz, NZ) * NY + wrap(y + dy, NY)
        return pl.ds(pl.multiple_of(index * 32, 32), 32)

    def plane(dz=0):
        return pl.ds(pl.multiple_of(wrap(z + dz, NZ) * 128, 128), 128)

    def token_rows(dx=0, flip=False):
        index = wrap(x + dx, NX) * 2 + (other if flip else c)
        return pl.ds(pl.multiple_of(index * ROWS, 16), ROWS)

    loads = []

    def load(src, dst):
        copy = pltpu.make_async_copy(src, dst, lsem.at[len(loads)])
        copy.start()
        loads.append(copy)

    load(k_h, WA.at[slot(), pl.ds(0, 128)])
    load(v_h, WA.at[slot(), pl.ds(128, 256)])
    load(tok_h, tok)
    load(gain_h, norm_gain)
    load(q_h, WB.at[slot(), pl.ds(0, 128)])
    load(ci_h, WB.at[slot(), pl.ds(128, 256)])
    load(cg_h, WB.at[slot(), pl.ds(384, 256)])
    load(co_h, WC.at[slot(), pl.ds(0, 256)])
    load(vo_h, WC.at[slot(), pl.ds(256, 256)])
    load(dd_h, ddown)
    load(du_h, dup)
    load(db_h, dbias)
    load(de_h, dextra)
    load(taps_h, taps)
    load(hg_h, hgain)
    for copy in loads[:4]:
        copy.wait()
    raw_rows = tok[...].astype(F32)
    scale = lax.rsqrt(jnp.mean(raw_rows * raw_rows, axis=-1, keepdims=True) + EPSILON)
    T[token_rows(), :] = (raw_rows * scale * norm_gain[...]).astype(BF16)
    for copy in loads[4:]:
        copy.wait()

    pl.semaphore_wait(barrier, len(peers))

    def place(j):
        return 0 if j == 0 else (-j if j <= 8 else j - 8)

    def plus(j):
        return (j % 2 == 0) if j <= 8 else ((j - 8) % 2 == 1)

    class Ring:
        def __init__(self, W, tag):
            self.W, self.tag = W, tag

        def around(self):
            ref = self.W.at[slot()]
            send(ref, ref, (self.tag, "zm", 1), at(dz=1))
            send(ref, ref, (self.tag, "zp", 1), at(dz=-1))

        def fan_out(self, j):
            ref = self.W.at[slot(place(j))]
            send(ref, ref, (self.tag, "ym", j), at(dy=1))
            send(ref, ref, (self.tag, "yp", j), at(dy=-1))

        def step(self, k):
            ref = self.W.at[slot(-k)]
            arrived(ref, (self.tag, "zm", k))
            if k < 8:
                send(ref, ref, (self.tag, "zm", k + 1), at(dz=1))
            self.fan_out(k)
            if k < 8:
                ref = self.W.at[slot(k)]
                arrived(ref, (self.tag, "zp", k))
                if k < 7:
                    send(ref, ref, (self.tag, "zp", k + 1), at(dz=-1))
                self.fan_out(8 + k)

        def column(self, j):
            dz = place(j)
            ref = self.W.at[slot(dz, -1)]
            arrived(ref, (self.tag, "ym", j))
            if plus(j):
                send(ref, ref, (self.tag, "y2", j), at(dy=1))
            ref = self.W.at[slot(dz, 1)]
            arrived(ref, (self.tag, "yp", j))
            if not plus(j):
                send(ref, ref, (self.tag, "y2", j), at(dy=-1))

        def columns(self, k):
            self.column(k - 1)
            if k > 1:
                self.column(7 + k)

        def finish(self):
            for j in range(16):
                arrived(self.W.at[slot(place(j), 2)], (self.tag, "y2", j))

    ring_b, ring_c = Ring(WB, "b"), Ring(WC, "c")
    own_a = WA.at[slot()]
    for d in range(1, NY):
        send(own_a, own_a, ("ay", d), at(dy=d))
    own_rows = T.at[token_rows()]
    send(own_rows, own_rows, "tm", at(dx=1))
    send(own_rows, own_rows, "tp", at(dx=-1))
    send(own_rows, own_rows, ("tc", 0), at(flip=True))
    ring_b.around()
    ring_b.fan_out(0)
    for d in range(1, NY):
        arrived(WA.at[slot(dy=-d)], ("ay", d))
    send(WA.at[plane()], WA.at[plane()], ("am", 1), at(dz=1))
    send(WA.at[plane()], WA.at[plane()], ("ap", 1), at(dz=-1))

    half = WIDTH // 2
    blocks = LEN // BLOCK
    key_cols = pl.ds(pl.multiple_of(tp * KEY_DIM, KEY_DIM), KEY_DIM)
    val_cols = pl.ds(pl.multiple_of(tp * VAL_DIM, VAL_DIM), VAL_DIM)

    def token_step(stage):
        if stage == 0:
            ref = T.at[token_rows(dx=-1)]
            arrived(ref, "tm")
            piece = T.at[token_rows(dx=-1), pl.ds(0, half)]
            send(piece, piece, "t2a", at(dx=1))
            send(ref, ref, ("tc", 1), at(flip=True))
            ref = T.at[token_rows(dx=1)]
            arrived(ref, "tp")
            piece = T.at[token_rows(dx=1), pl.ds(half, half)]
            send(piece, piece, "t2b", at(dx=-1))
            send(ref, ref, ("tc", 2), at(flip=True))
        elif stage == 1:
            arrived(T.at[token_rows(dx=2), pl.ds(0, half)], "t2a")
            arrived(T.at[token_rows(dx=2), pl.ds(half, half)], "t2b")
            ref = T.at[token_rows(dx=2)]
            send(ref, ref, ("tc", 3), at(flip=True))
        else:
            for j in range(4):
                arrived(T.at[token_rows(dx=(0, -1, 1, 2)[j], flip=True)], ("tc", j))

    def part(array, n):
        return array[n * BLOCK : (n + 1) * BLOCK]

    def decay():
        low = mm_nt(T[...], ddown[...]).astype(BF16)
        pre = mm(low, dup[:, key_cols]) + dbias[:, key_cols]
        log_sig = jnp.minimum(pre, 0.0) - jnp.log1p(jnp.exp(-jnp.abs(pre)))
        extra = jnp.transpose(jnp.broadcast_to(dextra[...], (KEY_DIM, LEN)))
        log_decay = log_sig / 16.0 + extra
        ri = lax.broadcasted_iota(jnp.int32, (LEN, LEN), 0)
        ci = lax.broadcasted_iota(jnp.int32, (LEN, LEN), 1)
        tri = jnp.where((ri >= ci) & (ri // BLOCK == ci // BLOCK), 1.0, 0.0).astype(F32)
        cumul = lax.dot_general(
            tri, log_decay, (((1,), (0,)), ((), ())), precision=lax.Precision.HIGHEST, preferred_element_type=F32
        )
        return cumul, cumul - log_decay

    for k in range(1, 9):
        ref = WA.at[plane(-k)]
        arrived(ref, ("am", k))
        if k < 8:
            send(ref, ref, ("am", k + 1), at(dz=1))
            ref = WA.at[plane(k)]
            arrived(ref, ("ap", k))
            if k < 7:
                send(ref, ref, ("ap", k + 1), at(dz=-1))
        if k < 8:
            ring_b.step(k)
        if k == 2:
            token_step(0)
        if k == 4:
            token_step(1)
        if k < 8:
            ring_b.columns(k)
        if k == 6:
            token_step(2)
            cumul, before = decay()
            totals = [cumul[(n + 1) * BLOCK - 1 : (n + 1) * BLOCK] for n in range(blocks)]
            offsets = [jnp.zeros((1, KEY_DIM), F32)]
            for n in range(blocks):
                offsets.append(offsets[-1] + totals[n])
            whole = offsets[blocks]
            suffix = [jnp.zeros((1, KEY_DIM), F32)]
            for n in reversed(range(blocks)):
                suffix.append(suffix[-1] + totals[n])
            suffix = suffix[::-1][1:]
            to_end = jnp.concatenate([suffix[n] + totals[n] - part(cumul, n) for n in range(blocks)], axis=0)
            from_start = jnp.concatenate([offsets[n] + part(before, n) for n in range(blocks)], axis=0)
            to_end, from_start = jnp.exp(to_end), jnp.exp(from_start)
            marks = log_rows(whole)
        if k == 7:
            ring_c.around()

    normed = T[...]
    kv = mm(normed, WA[...])
    key_f = kv[:, :KEY_DIM].astype(BF16).astype(F32)
    value = kv[:, KEY_DIM:].astype(BF16)
    fwd_device = mm_tn(value, (key_f * to_end).astype(BF16))
    back_device = mm_tn(value, (key_f * from_start).astype(BF16))

    for q in range(NY):
        SS[q * 144 : q * 144 + 64, :] = fwd_device[q * 64 : q * 64 + 64].astype(BF16)
        SS[q * 144 + 64 : q * 144 + 128, :] = back_device[q * 64 : q * 64 + 64].astype(BF16)
        SS[q * 144 + 128 : q * 144 + 144, :] = marks

    def message(dy=0):
        return pl.ds(pl.multiple_of(wrap(y + dy, NY) * 144, 16), 144)

    R1[message(), :] = SS[message(), :]
    for d in range(1, NY):
        send(SS.at[message(d)], R1.at[message()], ("s1", d), at(dy=d))

    ring_b.step(8)
    ring_c.fan_out(0)
    ring_b.columns(8)
    ring_c.step(1)
    ring_b.column(8)
    ring_c.columns(1)
    for d in range(1, NY):
        arrived(R1.at[message(-d)], ("s1", d))
    in_f, in_b, in_l = [], [], []
    for q in range(NY):
        in_f.append(R1[q * 144 : q * 144 + 64, :].astype(F32))
        in_b.append(R1[q * 144 + 64 : q * 144 + 128, :].astype(F32))
        in_l.append(log_total(R1[q * 144 + 128 : q * 144 + 144, :]))
    total_f = jnp.zeros((64, KEY_DIM), F32)
    total_b = jnp.zeros((64, KEY_DIM), F32)
    log_f = jnp.zeros((1, KEY_DIM), F32)
    log_b = jnp.zeros((1, KEY_DIM), F32)
    plane_f, plane_b, gap_f, gap_b = ([None] * NY for _ in range(4))
    for q in range(NY):
        plane_f[q], gap_f[q] = total_f, log_f
        total_f = jnp.exp(in_l[q]) * total_f + in_f[q]
        log_f = log_f + in_l[q]
    for q in reversed(range(NY)):
        plane_b[q], gap_b[q] = total_b, log_b
        total_b = jnp.exp(in_l[q]) * total_b + in_b[q]
        log_b = log_b + in_l[q]
    marks = log_rows(log_f)
    M2[0:64, :] = total_f.astype(BF16)
    M2[64:80, :] = marks
    M2[80:144, :] = total_b.astype(BF16)
    M2[144:160, :] = marks

    def depth(dz=0):
        return pl.ds(pl.multiple_of(wrap(z + dz, NZ) * 80, 16), 80)

    R2[depth(), :] = M2[0:80, :]
    for d in (8, 7, 9, 6, 10, 5, 11, 4, 12, 3, 13, 2, 14, 1, 15):
        start = pl.multiple_of(((z + d) // NZ) * 80, 16)
        send(M2.at[pl.ds(start, 80)], R2.at[depth()], ("s2", d), at(dz=d))

    ring_c.step(2)
    ring_b.finish()
    qcg = mm(normed, WB[...])
    query_f = (qcg[:, :KEY_DIM] * (1.0 / math.sqrt(KEY_DIM))).astype(BF16).astype(F32)
    conv_in = qcg[:, KEY_DIM : KEY_DIM + 256].astype(BF16)
    gate = qcg[:, KEY_DIM + 256 :].astype(BF16).astype(F32)
    CI[...] = conv_in
    CP[8 : 8 + LEN, :] = conv_in.astype(F32)
    send(CI.at[pl.ds(LEN - 16, 16)], HP, "hp", next_dev)
    send(CI.at[pl.ds(0, 16)], HN, "hn", prev_dev)
    ring_c.columns(2)
    ring_c.step(3)
    ring_c.columns(3)

    lower = lax.broadcasted_iota(jnp.int32, (BLOCK, BLOCK), 0) >= lax.broadcasted_iota(jnp.int32, (BLOCK, BLOCK), 1)
    upper = lax.broadcasted_iota(jnp.int32, (BLOCK, BLOCK), 0) <= lax.broadcasted_iota(jnp.int32, (BLOCK, BLOCK), 1)
    within = []
    fwd_inc, back_inc, fwd_query, back_query = [], [], [], []
    for n in range(blocks):
        cum_n, bef_n, key_n, query_n, value_n = (part(a, n) for a in (cumul, before, key_f, query_f, value))
        fq = (query_n * jnp.exp(cum_n)).astype(BF16)
        ks = (key_n * jnp.exp(bef_n)).astype(BF16)
        fwd_scores = mm_nt(fq, (key_n * jnp.exp(-cum_n)).astype(BF16))
        back_scores = mm_nt((query_n * jnp.exp(-bef_n)).astype(BF16), ks)
        scores = jnp.where(lower, fwd_scores, 0.0) + jnp.where(upper, back_scores, 0.0)
        within.append(mm(scores.astype(BF16), value_n))
        fwd_inc.append(mm_tn(value_n, (key_n * jnp.exp(totals[n] - cum_n)).astype(BF16)))
        back_inc.append(mm_tn(value_n, ks))
        fwd_query.append(fq)
        back_query.append((query_n * jnp.exp(totals[n] - bef_n)).astype(BF16))
    state = fwd_inc[0]
    for n in range(1, blocks):
        within[n] = within[n] + mm_nt(fwd_query[n], state.astype(BF16))
        state = jnp.exp(totals[n]) * state + fwd_inc[n]
    state = back_inc[blocks - 1]
    for n in reversed(range(blocks - 1)):
        within[n] = within[n] + mm_nt(back_query[n], state.astype(BF16))
        state = jnp.exp(totals[n]) * state + back_inc[n]
    local = jnp.concatenate(within, axis=0)
    far_fwd = jnp.concatenate(
        [part(query_f, n) * jnp.exp(offsets[n] + part(cumul, n)) for n in range(blocks)], axis=0
    ).astype(BF16)
    far_back = jnp.concatenate(
        [part(query_f, n) * jnp.exp(suffix[n] + (totals[n] - part(before, n))) for n in range(blocks)], axis=0
    ).astype(BF16)

    ring_c.step(4)
    ring_c.columns(4)
    arrived(HP, "hp")
    arrived(HN, "hn")
    first = HP[...].astype(F32)[15:16]
    last = HN[...].astype(F32)[0:1]
    CP[7:8, :] = jnp.where(s > 0, first, 0.0)
    CP[8 + LEN : 9 + LEN, :] = jnp.where(s < NZ * NY - 1, last, 0.0)
    tap = taps[:, val_cols]
    mixed = CP[7 : 7 + LEN, :] * tap[0:1] + CP[8 : 8 + LEN, :] * tap[1:2] + CP[9 : 9 + LEN, :] * tap[2:3]
    XC[:, 0:256] = (mixed * (gate * (1.0 / (1.0 + jnp.exp(-gate))))).astype(BF16)

    ring_c.step(5)
    ring_c.columns(5)
    ring_c.step(6)
    ring_c.columns(6)
    for d in range(1, NZ):
        arrived(R2.at[depth(-d)], ("s2", d))
    sum_f = jnp.zeros((64, KEY_DIM), F32)
    sum_b = jnp.zeros((64, KEY_DIM), F32)
    for k in range(NZ):
        step = jnp.exp(log_total(R2[k * 80 + 64 : k * 80 + 80, :])) * sum_f + R2[k * 80 : k * 80 + 64, :].astype(F32)
        sum_f = jnp.where(k < z, step, sum_f)
    for k in reversed(range(NZ)):
        step = jnp.exp(log_total(R2[k * 80 + 64 : k * 80 + 80, :])) * sum_b + R2[k * 80 : k * 80 + 64, :].astype(F32)
        sum_b = jnp.where(k > z, step, sum_b)
    for q in range(NY):
        M3[q * 128 : q * 128 + 64, :] = (plane_f[q] + jnp.exp(gap_f[q]) * sum_f).astype(BF16)
        M3[q * 128 + 64 : q * 128 + 128, :] = (plane_b[q] + jnp.exp(gap_b[q]) * sum_b).astype(BF16)

    def quarter(dy=0):
        return pl.ds(pl.multiple_of(wrap(y + dy, NY) * 64, 64), 64)

    def answer(dy, which):
        return pl.ds(pl.multiple_of(wrap(y + dy, NY) * 128 + 64 * which, 64), 64)

    for d in range(1, NY):
        send(M3.at[answer(d, 0)], IF.at[quarter()], ("s3f", d), at(dy=d))
        send(M3.at[answer(d, 1)], IB.at[quarter()], ("s3b", d), at(dy=d))
    IF[quarter(), :] = M3[answer(0, 0), :]
    IB[quarter(), :] = M3[answer(0, 1), :]
    ring_c.step(7)
    ring_c.columns(7)
    ring_c.step(8)
    ring_c.columns(8)
    ring_c.column(8)
    for d in range(1, NY):
        arrived(IF.at[quarter(-d)], ("s3f", d))
        arrived(IB.at[quarter(-d)], ("s3b", d))
    raw = local + mm_nt(far_fwd, IF[...]) + mm_nt(far_back, IB[...])
    norm = lax.rsqrt(jnp.mean(raw * raw, axis=-1, keepdims=True) + EPSILON)
    XC[:, 256:512] = (raw * norm * hgain[:, val_cols]).astype(BF16)
    ring_c.finish()

    def block4(r):
        return pl.ds(r * ROWS, ROWS)

    order = (2, 1, 3, 0)
    there = jnp.concatenate([XC[token_rows(dx=r, flip=True), :] for r in order], axis=0)
    here = jnp.concatenate([XC[token_rows(dx=r), :] for r in order], axis=0)
    for n in range(0, WIDTH, 512):
        PS[:, n : n + 512] = mm_nt(there, WC[n : n + 512, :]).astype(BF16)
    for i in range(4):
        send(PS.at[block4(i)], PR.at[block4(i)], ("pr", i), at(flip=True))
    for n in range(0, WIDTH, 512):
        PO[:, n : n + 512] = mm_nt(here, WC[n : n + 512, :])
    for i in range(3):
        arrived(PR.at[block4(i)], ("pr", i))
        XS[i * ROWS : (i + 1) * ROWS, :] = (
            PO[i * ROWS : (i + 1) * ROWS, :] + PR[i * ROWS : (i + 1) * ROWS, :].astype(F32)
        ).astype(BF16)
        send(XS.at[block4(i)], XR.at[block4(i)], ("xr", i), at(dx=order[i]))
    arrived(PR.at[block4(3)], ("pr", 3))
    total = PO[3 * ROWS :, :] + PR[3 * ROWS :, :].astype(F32)
    for i in (1, 2, 0):
        arrived(XR.at[block4(i)], ("xr", i))
        total = total + XR[i * ROWS : (i + 1) * ROWS, :].astype(F32)
    out[...] = total.astype(BF16)

    for copy in sends:
        copy.wait_send()
    assert len(sends) <= N_SEND and len(names) <= N_RECV, (len(sends), len(names))


def local(
    tokens, norm_gain, conv_in_weight, conv_gate_weight, conv_taps, query_weight, key_weight, value_weight,
    decay_down, decay_up, decay_bias, decay_extra, head_gain, conv_out_weight, value_out_weight,
):
    hbm = pl.BlockSpec(memory_space=pl.ANY)
    return pl.pallas_call(
        kernel,
        out_shape=jax.ShapeDtypeStruct((ROWS, WIDTH), BF16),
        in_specs=[hbm] * 15,
        out_specs=pl.BlockSpec(memory_space=pltpu.VMEM),
        scratch_shapes=[
            pltpu.VMEM((ROWS, WIDTH), BF16),
            pltpu.VMEM((1, WIDTH), F32),
            pltpu.VMEM((3, WIDTH), F32),
            pltpu.VMEM((16, WIDTH), BF16),
            pltpu.VMEM((16, 1024), BF16),
            pltpu.VMEM((1, 1024), F32),
            pltpu.VMEM((1, LEN), F32),
            pltpu.VMEM((1, WIDTH), F32),
            pltpu.VMEM((2048, 384), BF16),
            pltpu.VMEM((2048, 640), BF16),
            pltpu.VMEM((2048, 512), BF16),
            pltpu.VMEM((LEN, WIDTH), BF16),
            pltpu.VMEM((NY * 144, KEY_DIM), BF16),
            pltpu.VMEM((NY * 144, KEY_DIM), BF16),
            pltpu.VMEM((160, KEY_DIM), BF16),
            pltpu.VMEM((NZ * 80, KEY_DIM), BF16),
            pltpu.VMEM((NY * 128, KEY_DIM), BF16),
            pltpu.VMEM((VAL_DIM, KEY_DIM), BF16),
            pltpu.VMEM((VAL_DIM, KEY_DIM), BF16),
            pltpu.VMEM((LEN, 256), BF16),
            pltpu.VMEM((LEN + 16, 256), F32),
            pltpu.VMEM((16, 256), BF16),
            pltpu.VMEM((16, 256), BF16),
            pltpu.VMEM((LEN, 512), BF16),
            pltpu.VMEM((4 * ROWS, WIDTH), F32),
            pltpu.VMEM((4 * ROWS, WIDTH), BF16),
            pltpu.VMEM((4 * ROWS, WIDTH), BF16),
            pltpu.VMEM((3 * ROWS, WIDTH), BF16),
            pltpu.VMEM((3 * ROWS, WIDTH), BF16),
            pltpu.SemaphoreType.DMA((N_SEND,)),
            pltpu.SemaphoreType.DMA((N_RECV,)),
            pltpu.SemaphoreType.DMA((15,)),
        ],
        compiler_params=pltpu.CompilerParams(collective_id=0, has_side_effects=True, vmem_limit_bytes=60 * 1024 * 1024),
        cost_estimate=pl.CostEstimate(flops=3_000_000_000, bytes_accessed=1_000_000, transcendentals=0),
    )(
        tokens, norm_gain.reshape(1, -1), conv_in_weight, conv_gate_weight, conv_taps, query_weight, key_weight,
        value_weight, decay_down.T, decay_up, decay_bias.reshape(1, -1), decay_extra, head_gain.reshape(1, -1),
        conv_out_weight.T, value_out_weight.T,
    )


def solution(mesh):
    torus = Mesh(mesh.devices.reshape(NZ, NY, NX, NC), SP_TP)
    return jax.shard_map(
        local,
        mesh=torus,
        in_specs=(
            P(SP_TP, None), P(), P(SP, TP), P(SP, TP), P(), P(SP, TP), P(SP, TP), P(SP, TP),
            P(), P(), P(), P(TP, SP), P(), P(TP, SP), P(TP, SP),
        ),
        out_specs=P(SP_TP, None),
        check_vma=False,
    )
```

```python
import functools
import math

import jax
import jax.numpy as jnp
from jax import lax
from jax.experimental import pallas as pl
from jax.experimental.pallas import tpu as pltpu
from jax.sharding import Mesh
from jax.sharding import PartitionSpec as P

NZ, NY, NX, NC = 16, 4, 4, 2
KEY_DIM = 128
VAL_DIM = 256
BLOCK = 64
ROWS = 48
LEN = 384
WIDTH = 2048
EPSILON = 1e-06
SP = ("z", "y")
TP = ("x", "c")
SP_TP = ("z", "y", "x", "c")
F32 = jnp.float32
BF16 = jnp.bfloat16
MESH = pl.DeviceIdType.MESH
N_SEND = 256
N_RECV = 256


def mm(a, b):
    return lax.dot_general(a, b, (((1,), (0,)), ((), ())), preferred_element_type=F32)


def mm_nt(a, b):
    return lax.dot_general(a, b, (((1,), (1,)), ((), ())), preferred_element_type=F32)


def mm_tn(a, b):
    return lax.dot_general(a, b, (((0,), (0,)), ((), ())), preferred_element_type=F32)


def wrap(value, size):
    return lax.rem(value + size, size)


def split3(row):
    hi = row.astype(BF16)
    rest = row - hi.astype(F32)
    mid = rest.astype(BF16)
    low = (rest - mid.astype(F32)).astype(BF16)
    return hi, mid, low


def log_rows(row):
    hi, mid, low = split3(row)
    index = lax.broadcasted_iota(jnp.int32, (16, KEY_DIM), 0)
    spread = [jnp.broadcast_to(p.astype(F32), (16, KEY_DIM)) for p in (hi, mid, low)]
    out = jnp.where(index == 0, spread[0], jnp.where(index == 1, spread[1], jnp.where(index == 2, spread[2], 0.0)))
    return out.astype(BF16)


def log_total(rows16):
    return jnp.sum(rows16.astype(F32), axis=0, keepdims=True)


def kernel(
    tok_h, gain_h, ci_h, cg_h, taps_h, q_h, k_h, v_h, dd_h, du_h, db_h, de_h, hg_h, co_h, vo_h,
    out,
    tok, norm_gain, taps, ddown, dup, dbias, dextra, hgain,
    WA, WB, WC, T, SS, R1, M2, R2, M3, IF, IB, CI, CP, HP, HN, XC, PO, PS, PR, XS, XR,
    ssem, rsem, lsem,
):
    z, y, x, c = (lax.axis_index(a) for a in SP_TP)
    tp = x * 2 + c
    s = z * 4 + y
    other = 1 - c
    names = {}
    sends = []

    def at(dz=0, dy=0, dx=0, flip=False):
        return (wrap(z + dz, NZ), wrap(y + dy, NY), wrap(x + dx, NX), other if flip else c)

    def sem(name):
        return rsem.at[names.setdefault(name, len(names))]

    def send(src, dst, name, device):
        copy = pltpu.make_async_remote_copy(
            src_ref=src, dst_ref=dst, send_sem=ssem.at[len(sends)], recv_sem=sem(name),
            device_id=device, device_id_type=MESH,
        )
        copy.start()
        sends.append(copy)

    def arrived(dst, name):
        pltpu.make_async_remote_copy(
            src_ref=dst, dst_ref=dst, send_sem=ssem.at[0], recv_sem=sem(name),
            device_id=(z, y, x, c), device_id_type=MESH,
        ).wait_recv()

    after = lax.rem(s + 1, NZ * NY)
    ahead = lax.rem(s + NZ * NY - 1, NZ * NY)
    next_dev = (after // NY, lax.rem(after, NY), x, c)
    prev_dev = (ahead // NY, lax.rem(ahead, NY), x, c)
    peers = [at(dz=d) for d in (1, -1)]
    peers += [at(dy=d) for d in range(1, NY)]
    peers += [at(dx=d) for d in range(1, NX)]
    peers += [at(flip=True), next_dev, prev_dev]
    barrier = pltpu.get_barrier_semaphore()
    for peer in peers:
        pl.semaphore_signal(barrier, inc=1, device_id=peer, device_id_type=MESH)

    def slot(dz=0, dy=0):
        index = wrap(z + dz, NZ) * NY + wrap(y + dy, NY)
        return pl.ds(pl.multiple_of(index * 32, 32), 32)

    def plane(dz=0):
        return pl.ds(pl.multiple_of(wrap(z + dz, NZ) * 128, 128), 128)

    def token_rows(dx=0, flip=False):
        index = wrap(x + dx, NX) * 2 + (other if flip else c)
        return pl.ds(pl.multiple_of(index * ROWS, 16), ROWS)

    loads = []

    def load(src, dst):
        copy = pltpu.make_async_copy(src, dst, lsem.at[len(loads)])
        copy.start()
        loads.append(copy)

    load(k_h, WA.at[slot(), pl.ds(0, 128)])
    load(v_h, WA.at[slot(), pl.ds(128, 256)])
    load(tok_h, tok)
    load(gain_h, norm_gain)
    load(q_h, WB.at[slot(), pl.ds(0, 128)])
    load(ci_h, WB.at[slot(), pl.ds(128, 256)])
    load(cg_h, WB.at[slot(), pl.ds(384, 256)])
    load(co_h, WC.at[slot(), pl.ds(0, 256)])
    load(vo_h, WC.at[slot(), pl.ds(256, 256)])
    load(dd_h, ddown)
    load(du_h, dup)
    load(db_h, dbias)
    load(de_h, dextra)
    load(taps_h, taps)
    load(hg_h, hgain)
    for copy in loads[:4]:
        copy.wait()
    raw_rows = tok[...].astype(F32)
    scale = lax.rsqrt(jnp.mean(raw_rows * raw_rows, axis=-1, keepdims=True) + EPSILON)
    T[token_rows(), :] = (raw_rows * scale * norm_gain[...]).astype(BF16)
    for copy in loads[4:]:
        copy.wait()

    pl.semaphore_wait(barrier, len(peers))

    def place(j):
        return 0 if j == 0 else (-j if j <= 8 else j - 8)

    class Ring:
        def __init__(self, W, tag):
            self.W, self.tag = W, tag

        def hop(self, chain, sign, k):
            ref = self.W.at[slot(-sign * (k - 1), 2 * chain)]
            send(ref, ref, (self.tag, chain, sign, k), at(dz=sign))

        def fan_out(self, j):
            ref = self.W.at[slot(place(j))]
            send(ref, ref, (self.tag, "ym", j), at(dy=1))
            send(ref, ref, (self.tag, "yp", j), at(dy=-1))

        def across(self):
            ref = self.W.at[slot()]
            send(ref, ref, (self.tag, "y2"), at(dy=2))

        def around(self, chain):
            if chain:
                arrived(self.W.at[slot(0, 2)], (self.tag, "y2"))
            self.hop(chain, 1, 1)
            self.hop(chain, -1, 1)

        def step(self, k, chains=(0, 1), fan=True):
            for chain in chains:
                for sign in (1, -1):
                    if sign == -1 and k == 8:
                        continue
                    arrived(self.W.at[slot(-sign * k, 2 * chain)], (self.tag, chain, sign, k))
                    if k < (8 if sign == 1 else 7):
                        self.hop(chain, sign, k + 1)
                    if chain == 0 and fan:
                        self.fan_out(k if sign == 1 else 8 + k)

        def column(self, *js):
            for j in js:
                plus = (j % 2 == 0) if j <= 8 else ((j - 8) % 2 == 1)
                for dy, name in ((-1, "ym"), (1, "yp")):
                    ref = self.W.at[slot(place(j), dy)]
                    arrived(ref, (self.tag, name, j))
                    if plus == (dy == -1):
                        send(ref, ref, (self.tag, "y2", j), at(dy=-dy))

        def last_column(self):
            for j in range(16):
                arrived(self.W.at[slot(place(j), 2)], (self.tag, "y2", j))

        def finish(self):
            for j in range(16):
                arrived(self.W.at[slot(place(j), -1)], (self.tag, "ym", j))
                arrived(self.W.at[slot(place(j), 1)], (self.tag, "yp", j))

    ring_a, ring_b, ring_c = Ring(WA, "a"), Ring(WB, "b"), Ring(WC, "c")
    ring_a.across()
    ring_a.around(0)
    ring_a.fan_out(0)
    own_rows = T.at[token_rows()]
    send(own_rows, own_rows, "tm", at(dx=1))
    send(own_rows, own_rows, "tp", at(dx=-1))
    send(own_rows, own_rows, ("tc", 0), at(flip=True))
    ring_b.across()
    ring_b.around(0)
    ring_b.fan_out(0)
    ring_c.around(0)
    ring_c.fan_out(0)

    half = WIDTH // 2
    blocks = LEN // BLOCK
    key_cols = pl.ds(pl.multiple_of(tp * KEY_DIM, KEY_DIM), KEY_DIM)
    val_cols = pl.ds(pl.multiple_of(tp * VAL_DIM, VAL_DIM), VAL_DIM)

    def token_step(stage):
        if stage == 0:
            ref = T.at[token_rows(dx=-1)]
            arrived(ref, "tm")
            piece = T.at[token_rows(dx=-1), pl.ds(0, half)]
            send(piece, piece, "t2a", at(dx=1))
            send(ref, ref, ("tc", 1), at(flip=True))
            ref = T.at[token_rows(dx=1)]
            arrived(ref, "tp")
            piece = T.at[token_rows(dx=1), pl.ds(half, half)]
            send(piece, piece, "t2b", at(dx=-1))
            send(ref, ref, ("tc", 2), at(flip=True))
        elif stage == 1:
            arrived(T.at[token_rows(dx=2), pl.ds(0, half)], "t2a")
            arrived(T.at[token_rows(dx=2), pl.ds(half, half)], "t2b")
            ref = T.at[token_rows(dx=2)]
            send(ref, ref, ("tc", 3), at(flip=True))
        else:
            for j in range(4):
                arrived(T.at[token_rows(dx=(0, -1, 1, 2)[j], flip=True)], ("tc", j))

    def part(array, n):
        return array[n * BLOCK : (n + 1) * BLOCK]

    def decay():
        low = mm_nt(T[...], ddown[...]).astype(BF16)
        pre = mm(low, dup[:, key_cols]) + dbias[:, key_cols]
        log_sig = jnp.minimum(pre, 0.0) - jnp.log1p(jnp.exp(-jnp.abs(pre)))
        extra = jnp.transpose(jnp.broadcast_to(dextra[...], (KEY_DIM, LEN)))
        log_decay = log_sig / 16.0 + extra
        ri = lax.broadcasted_iota(jnp.int32, (LEN, LEN), 0)
        ci = lax.broadcasted_iota(jnp.int32, (LEN, LEN), 1)
        tri = jnp.where((ri >= ci) & (ri // BLOCK == ci // BLOCK), 1.0, 0.0).astype(F32)
        cumul = lax.dot_general(
            tri, log_decay, (((1,), (0,)), ((), ())), precision=lax.Precision.HIGHEST, preferred_element_type=F32
        )
        return cumul, cumul - log_decay

    for k in range(1, 9):
        ring_a.step(k, (0,))
        if k == 1:
            ring_a.around(1)
        else:
            ring_a.step(k - 1, (1,))
        ring_b.step(k, (0,))
        if k == 1:
            ring_b.around(1)
        else:
            ring_b.step(k - 1, (1,))
        ring_c.step(k, (0,), fan=k <= 4)
        if k == 1:
            token_step(0)
        if k == 3:
            token_step(1)
        if k == 4:
            ring_c.column(0)
        if k > 4:
            ring_c.column(k - 4, k + 4)
        if k == 6:
            token_step(2)
            cumul, before = decay()
            totals = [cumul[(n + 1) * BLOCK - 1 : (n + 1) * BLOCK] for n in range(blocks)]
            offsets = [jnp.zeros((1, KEY_DIM), F32)]
            for n in range(blocks):
                offsets.append(offsets[-1] + totals[n])
            whole = offsets[blocks]
            suffix = [jnp.zeros((1, KEY_DIM), F32)]
            for n in reversed(range(blocks)):
                suffix.append(suffix[-1] + totals[n])
            suffix = suffix[::-1][1:]
            to_end = jnp.concatenate([suffix[n] + totals[n] - part(cumul, n) for n in range(blocks)], axis=0)
            from_start = jnp.concatenate([offsets[n] + part(before, n) for n in range(blocks)], axis=0)
            to_end, from_start = jnp.exp(to_end), jnp.exp(from_start)
            marks = log_rows(whole)
    ring_a.step(8, (1,))
    ring_a.finish()

    normed = T[...]
    kv = mm(normed, WA[...])
    key_f = kv[:, :KEY_DIM].astype(BF16).astype(F32)
    value = kv[:, KEY_DIM:].astype(BF16)
    fwd_device = mm_tn(value, (key_f * to_end).astype(BF16))
    back_device = mm_tn(value, (key_f * from_start).astype(BF16))

    for q in range(NY):
        SS[q * 144 : q * 144 + 64, :] = fwd_device[q * 64 : q * 64 + 64].astype(BF16)
        SS[q * 144 + 64 : q * 144 + 128, :] = back_device[q * 64 : q * 64 + 64].astype(BF16)
        SS[q * 144 + 128 : q * 144 + 144, :] = marks

    def message(dy=0):
        return pl.ds(pl.multiple_of(wrap(y + dy, NY) * 144, 16), 144)

    R1[message(), :] = SS[message(), :]
    for d in range(1, NY):
        send(SS.at[message(d)], R1.at[message()], ("s1", d), at(dy=d))

    ring_b.step(8, (1,))
    ring_c.fan_out(5)
    ring_c.fan_out(13)
    for d in range(1, NY):
        arrived(R1.at[message(-d)], ("s1", d))
    in_f, in_b, in_l = [], [], []
    for q in range(NY):
        in_f.append(R1[q * 144 : q * 144 + 64, :].astype(F32))
        in_b.append(R1[q * 144 + 64 : q * 144 + 128, :].astype(F32))
        in_l.append(log_total(R1[q * 144 + 128 : q * 144 + 144, :]))
    total_f = jnp.zeros((64, KEY_DIM), F32)
    total_b = jnp.zeros((64, KEY_DIM), F32)
    log_f = jnp.zeros((1, KEY_DIM), F32)
    log_b = jnp.zeros((1, KEY_DIM), F32)
    plane_f, plane_b, gap_f, gap_b = ([None] * NY for _ in range(4))
    for q in range(NY):
        plane_f[q], gap_f[q] = total_f, log_f
        total_f = jnp.exp(in_l[q]) * total_f + in_f[q]
        log_f = log_f + in_l[q]
    for q in reversed(range(NY)):
        plane_b[q], gap_b[q] = total_b, log_b
        total_b = jnp.exp(in_l[q]) * total_b + in_b[q]
        log_b = log_b + in_l[q]
    marks = log_rows(log_f)
    M2[0:64, :] = total_f.astype(BF16)
    M2[64:80, :] = marks
    M2[80:144, :] = total_b.astype(BF16)
    M2[144:160, :] = marks

    def depth(dz=0):
        return pl.ds(pl.multiple_of(wrap(z + dz, NZ) * 80, 16), 80)

    R2[depth(), :] = M2[0:80, :]
    for d in (8, 7, 9, 6, 10, 5, 11, 4, 12, 3, 13, 2, 14, 1, 15):
        start = pl.multiple_of(((z + d) // NZ) * 80, 16)
        send(M2.at[pl.ds(start, 80)], R2.at[depth()], ("s2", d), at(dz=d))

    ring_c.fan_out(6)
    ring_c.fan_out(14)
    ring_b.finish()
    qcg = mm(normed, WB[...])
    query_f = (qcg[:, :KEY_DIM] * (1.0 / math.sqrt(KEY_DIM))).astype(BF16).astype(F32)
    conv_in = qcg[:, KEY_DIM : KEY_DIM + 256].astype(BF16)
    gate = qcg[:, KEY_DIM + 256 :].astype(BF16).astype(F32)
    CI[...] = conv_in
    CP[8 : 8 + LEN, :] = conv_in.astype(F32)
    send(CI.at[pl.ds(LEN - 16, 16)], HP, "hp", next_dev)
    send(CI.at[pl.ds(0, 16)], HN, "hn", prev_dev)
    ring_c.column(5, 13)
    ring_c.fan_out(7)
    ring_c.fan_out(15)
    ring_c.fan_out(8)

    lower = lax.broadcasted_iota(jnp.int32, (BLOCK, BLOCK), 0) >= lax.broadcasted_iota(jnp.int32, (BLOCK, BLOCK), 1)
    upper = lax.broadcasted_iota(jnp.int32, (BLOCK, BLOCK), 0) <= lax.broadcasted_iota(jnp.int32, (BLOCK, BLOCK), 1)
    within = []
    fwd_inc, back_inc, fwd_query, back_query = [], [], [], []
    for n in range(blocks):
        cum_n, bef_n, key_n, query_n, value_n = (part(a, n) for a in (cumul, before, key_f, query_f, value))
        fq = (query_n * jnp.exp(cum_n)).astype(BF16)
        ks = (key_n * jnp.exp(bef_n)).astype(BF16)
        fwd_scores = mm_nt(fq, (key_n * jnp.exp(-cum_n)).astype(BF16))
        back_scores = mm_nt((query_n * jnp.exp(-bef_n)).astype(BF16), ks)
        scores = jnp.where(lower, fwd_scores, 0.0) + jnp.where(upper, back_scores, 0.0)
        within.append(mm(scores.astype(BF16), value_n))
        fwd_inc.append(mm_tn(value_n, (key_n * jnp.exp(totals[n] - cum_n)).astype(BF16)))
        back_inc.append(mm_tn(value_n, ks))
        fwd_query.append(fq)
        back_query.append((query_n * jnp.exp(totals[n] - bef_n)).astype(BF16))
    state = fwd_inc[0]
    for n in range(1, blocks):
        within[n] = within[n] + mm_nt(fwd_query[n], state.astype(BF16))
        state = jnp.exp(totals[n]) * state + fwd_inc[n]
    state = back_inc[blocks - 1]
    for n in reversed(range(blocks - 1)):
        within[n] = within[n] + mm_nt(back_query[n], state.astype(BF16))
        state = jnp.exp(totals[n]) * state + back_inc[n]
    local = jnp.concatenate(within, axis=0)
    far_fwd = jnp.concatenate(
        [part(query_f, n) * jnp.exp(offsets[n] + part(cumul, n)) for n in range(blocks)], axis=0
    ).astype(BF16)
    far_back = jnp.concatenate(
        [part(query_f, n) * jnp.exp(suffix[n] + (totals[n] - part(before, n))) for n in range(blocks)], axis=0
    ).astype(BF16)

    ring_c.column(6, 14)
    arrived(HP, "hp")
    arrived(HN, "hn")
    first = HP[...].astype(F32)[15:16]
    last = HN[...].astype(F32)[0:1]
    CP[7:8, :] = jnp.where(s > 0, first, 0.0)
    CP[8 + LEN : 9 + LEN, :] = jnp.where(s < NZ * NY - 1, last, 0.0)
    tap = taps[:, val_cols]
    mixed = CP[7 : 7 + LEN, :] * tap[0:1] + CP[8 : 8 + LEN, :] * tap[1:2] + CP[9 : 9 + LEN, :] * tap[2:3]
    XC[:, 0:256] = (mixed * (gate * (1.0 / (1.0 + jnp.exp(-gate))))).astype(BF16)

    ring_c.column(7, 15, 8)
    for d in range(1, NZ):
        arrived(R2.at[depth(-d)], ("s2", d))
    sum_f = jnp.zeros((64, KEY_DIM), F32)
    sum_b = jnp.zeros((64, KEY_DIM), F32)
    for k in range(NZ):
        step = jnp.exp(log_total(R2[k * 80 + 64 : k * 80 + 80, :])) * sum_f + R2[k * 80 : k * 80 + 64, :].astype(F32)
        sum_f = jnp.where(k < z, step, sum_f)
    for k in reversed(range(NZ)):
        step = jnp.exp(log_total(R2[k * 80 + 64 : k * 80 + 80, :])) * sum_b + R2[k * 80 : k * 80 + 64, :].astype(F32)
        sum_b = jnp.where(k > z, step, sum_b)
    for q in range(NY):
        M3[q * 128 : q * 128 + 64, :] = (plane_f[q] + jnp.exp(gap_f[q]) * sum_f).astype(BF16)
        M3[q * 128 + 64 : q * 128 + 128, :] = (plane_b[q] + jnp.exp(gap_b[q]) * sum_b).astype(BF16)

    def quarter(dy=0):
        return pl.ds(pl.multiple_of(wrap(y + dy, NY) * 64, 64), 64)

    def answer(dy, which):
        return pl.ds(pl.multiple_of(wrap(y + dy, NY) * 128 + 64 * which, 64), 64)

    for d in range(1, NY):
        send(M3.at[answer(d, 0)], IF.at[quarter()], ("s3f", d), at(dy=d))
        send(M3.at[answer(d, 1)], IB.at[quarter()], ("s3b", d), at(dy=d))
    IF[quarter(), :] = M3[answer(0, 0), :]
    IB[quarter(), :] = M3[answer(0, 1), :]
    for d in range(1, NY):
        arrived(IF.at[quarter(-d)], ("s3f", d))
        arrived(IB.at[quarter(-d)], ("s3b", d))
    raw = local + mm_nt(far_fwd, IF[...]) + mm_nt(far_back, IB[...])
    norm = lax.rsqrt(jnp.mean(raw * raw, axis=-1, keepdims=True) + EPSILON)
    XC[:, 256:512] = (raw * norm * hgain[:, val_cols]).astype(BF16)
    ring_c.last_column()

    order = (2, 1, 3, 0)
    pieces, piece = 4, WIDTH // 4
    there = jnp.concatenate([XC[token_rows(dx=r, flip=True), :] for r in order], axis=0)
    here = jnp.concatenate([XC[token_rows(dx=r), :] for r in order], axis=0)

    def rows4(n, i=0, count=4):
        return pl.ds((n * 4 + i) * ROWS, count * ROWS)

    def pair_send(n):
        PS[rows4(n), :] = mm_nt(there, WC[n * piece : (n + 1) * piece, :]).astype(BF16)
        send(PS.at[rows4(n)], PR.at[rows4(n)], ("pr", n), at(flip=True))

    def x_send(n):
        mine = mm_nt(here, WC[n * piece : (n + 1) * piece, :])
        arrived(PR.at[rows4(n)], ("pr", n))
        both = mine + PR[rows4(n), :].astype(F32)
        XS[rows4(n), :] = both.astype(BF16)
        for i in range(3):
            send(XS.at[rows4(n, i, 1)], XR.at[rows4(n, i, 1)], ("xr", n, i), at(dx=order[i]))
        PO[pl.ds(n * ROWS, ROWS), :] = both[3 * ROWS :]

    pair_send(0)
    pair_send(1)
    for n in range(pieces):
        x_send(n)
        if n + 2 < pieces:
            pair_send(n + 2)
    for n in range(pieces):
        total = PO[n * ROWS : (n + 1) * ROWS, :]
        for i in (1, 2, 0):
            arrived(XR.at[rows4(n, i, 1)], ("xr", n, i))
            total = total + XR[rows4(n, i, 1), :].astype(F32)
        out[:, n * piece : (n + 1) * piece] = total.astype(BF16)

    for copy in sends:
        copy.wait_send()
    assert len(sends) <= N_SEND and len(names) <= N_RECV, (len(sends), len(names))


def local(
    tokens, norm_gain, conv_in_weight, conv_gate_weight, conv_taps, query_weight, key_weight, value_weight,
    decay_down, decay_up, decay_bias, decay_extra, head_gain, conv_out_weight, value_out_weight,
):
    hbm = pl.BlockSpec(memory_space=pl.ANY)
    return pl.pallas_call(
        kernel,
        out_shape=jax.ShapeDtypeStruct((ROWS, WIDTH), BF16),
        in_specs=[hbm] * 15,
        out_specs=pl.BlockSpec(memory_space=pltpu.VMEM),
        scratch_shapes=[
            pltpu.VMEM((ROWS, WIDTH), BF16),
            pltpu.VMEM((1, WIDTH), F32),
            pltpu.VMEM((3, WIDTH), F32),
            pltpu.VMEM((16, WIDTH), BF16),
            pltpu.VMEM((16, 1024), BF16),
            pltpu.VMEM((1, 1024), F32),
            pltpu.VMEM((1, LEN), F32),
            pltpu.VMEM((1, WIDTH), F32),
            pltpu.VMEM((2048, 384), BF16),
            pltpu.VMEM((2048, 640), BF16),
            pltpu.VMEM((2048, 512), BF16),
            pltpu.VMEM((LEN, WIDTH), BF16),
            pltpu.VMEM((NY * 144, KEY_DIM), BF16),
            pltpu.VMEM((NY * 144, KEY_DIM), BF16),
            pltpu.VMEM((160, KEY_DIM), BF16),
            pltpu.VMEM((NZ * 80, KEY_DIM), BF16),
            pltpu.VMEM((NY * 128, KEY_DIM), BF16),
            pltpu.VMEM((VAL_DIM, KEY_DIM), BF16),
            pltpu.VMEM((VAL_DIM, KEY_DIM), BF16),
            pltpu.VMEM((LEN, 256), BF16),
            pltpu.VMEM((LEN + 16, 256), F32),
            pltpu.VMEM((16, 256), BF16),
            pltpu.VMEM((16, 256), BF16),
            pltpu.VMEM((LEN, 512), BF16),
            pltpu.VMEM((4 * ROWS, WIDTH // 4), F32),
            pltpu.VMEM((16 * ROWS, WIDTH // 4), BF16),
            pltpu.VMEM((16 * ROWS, WIDTH // 4), BF16),
            pltpu.VMEM((16 * ROWS, WIDTH // 4), BF16),
            pltpu.VMEM((16 * ROWS, WIDTH // 4), BF16),
            pltpu.SemaphoreType.DMA((N_SEND,)),
            pltpu.SemaphoreType.DMA((N_RECV,)),
            pltpu.SemaphoreType.DMA((15,)),
        ],
        compiler_params=pltpu.CompilerParams(collective_id=0, has_side_effects=True, vmem_limit_bytes=60 * 1024 * 1024),
        cost_estimate=pl.CostEstimate(flops=3_000_000_000, bytes_accessed=1_000_000, transcendentals=0),
    )(
        tokens, norm_gain.reshape(1, -1), conv_in_weight, conv_gate_weight, conv_taps, query_weight, key_weight,
        value_weight, decay_down.T, decay_up, decay_bias.reshape(1, -1), decay_extra, head_gain.reshape(1, -1),
        conv_out_weight.T, value_out_weight.T,
    )


def solution(mesh):
    torus = Mesh(mesh.devices.reshape(NZ, NY, NX, NC), SP_TP)
    return jax.shard_map(
        local,
        mesh=torus,
        in_specs=(
            P(SP_TP, None), P(), P(SP, TP), P(SP, TP), P(), P(SP, TP), P(SP, TP), P(SP, TP),
            P(), P(), P(), P(TP, SP), P(), P(TP, SP), P(TP, SP),
        ),
        out_specs=P(SP_TP, None),
        check_vma=False,
    )
```

```python
import functools
import math

import jax
import jax.numpy as jnp
from jax import lax
from jax.experimental import pallas as pl
from jax.experimental.pallas import tpu as pltpu
from jax.sharding import Mesh
from jax.sharding import PartitionSpec as P

NZ, NY, NX, NC = 16, 4, 4, 2
KEY_DIM = 128
VAL_DIM = 256
BLOCK = 64
ROWS = 48
LEN = 384
WIDTH = 2048
EPSILON = 1e-06
SP = ("z", "y")
TP = ("x", "c")
SP_TP = ("z", "y", "x", "c")
F32 = jnp.float32
BF16 = jnp.bfloat16
MESH = pl.DeviceIdType.MESH
N_SEND = 256
N_RECV = 256


def mm(a, b):
    return lax.dot_general(a, b, (((1,), (0,)), ((), ())), preferred_element_type=F32)


def mm_nt(a, b):
    return lax.dot_general(a, b, (((1,), (1,)), ((), ())), preferred_element_type=F32)


def mm_tn(a, b):
    return lax.dot_general(a, b, (((0,), (0,)), ((), ())), preferred_element_type=F32)


def wrap(value, size):
    return lax.rem(value + size, size)


def split3(row):
    hi = row.astype(BF16)
    rest = row - hi.astype(F32)
    mid = rest.astype(BF16)
    low = (rest - mid.astype(F32)).astype(BF16)
    return hi, mid, low


def log_rows(row):
    hi, mid, low = split3(row)
    index = lax.broadcasted_iota(jnp.int32, (16, KEY_DIM), 0)
    spread = [jnp.broadcast_to(p.astype(F32), (16, KEY_DIM)) for p in (hi, mid, low)]
    out = jnp.where(index == 0, spread[0], jnp.where(index == 1, spread[1], jnp.where(index == 2, spread[2], 0.0)))
    return out.astype(BF16)


def log_total(rows16):
    return jnp.sum(rows16.astype(F32), axis=0, keepdims=True)


def kernel(
    tok_h, gain_h, ci_h, cg_h, taps_h, q_h, k_h, v_h, dd_h, du_h, db_h, de_h, hg_h, co_h, vo_h,
    out,
    tok, norm_gain, taps, ddown, dup, dbias, dextra, hgain,
    WA, WB, WC, T, SS, R1, M2, NEAR, M4, R2, M3, IF, IB, CI, CP, HP, HN, XC, PO, PS, PR, XS, XR,
    ssem, rsem, lsem,
):
    z, y, x, c = (lax.axis_index(a) for a in SP_TP)
    tp = x * 2 + c
    s = z * 4 + y
    other = 1 - c
    names = {}
    sends = []

    def at(dz=0, dy=0, dx=0, flip=False):
        return (wrap(z + dz, NZ), wrap(y + dy, NY), wrap(x + dx, NX), other if flip else c)

    def sem(name):
        return rsem.at[names.setdefault(name, len(names))]

    def send(src, dst, name, device):
        copy = pltpu.make_async_remote_copy(
            src_ref=src, dst_ref=dst, send_sem=ssem.at[len(sends)], recv_sem=sem(name),
            device_id=device, device_id_type=MESH,
        )
        copy.start()
        sends.append(copy)

    def arrived(dst, name):
        pltpu.make_async_remote_copy(
            src_ref=dst, dst_ref=dst, send_sem=ssem.at[0], recv_sem=sem(name),
            device_id=(z, y, x, c), device_id_type=MESH,
        ).wait_recv()

    after = lax.rem(s + 1, NZ * NY)
    ahead = lax.rem(s + NZ * NY - 1, NZ * NY)
    next_dev = (after // NY, lax.rem(after, NY), x, c)
    prev_dev = (ahead // NY, lax.rem(ahead, NY), x, c)
    peers = [at(dz=d) for d in (1, -1, 2, -2)]
    peers += [at(dy=d) for d in range(1, NY)]
    peers += [at(dx=d) for d in range(1, NX)]
    peers += [at(flip=True), next_dev, prev_dev]
    barrier = pltpu.get_barrier_semaphore()
    for peer in peers:
        pl.semaphore_signal(barrier, inc=1, device_id=peer, device_id_type=MESH)

    def slot(dz=0, dy=0):
        index = wrap(z + dz, NZ) * NY + wrap(y + dy, NY)
        return pl.ds(pl.multiple_of(index * 32, 32), 32)

    def plane(dz=0):
        return pl.ds(pl.multiple_of(wrap(z + dz, NZ) * 128, 128), 128)

    def token_rows(dx=0, flip=False):
        index = wrap(x + dx, NX) * 2 + (other if flip else c)
        return pl.ds(pl.multiple_of(index * ROWS, 16), ROWS)

    loads = []

    def load(src, dst):
        copy = pltpu.make_async_copy(src, dst, lsem.at[len(loads)])
        copy.start()
        loads.append(copy)

    load(k_h, WA.at[slot(), pl.ds(0, 128)])
    load(v_h, WA.at[slot(), pl.ds(128, 256)])
    load(tok_h, tok)
    load(gain_h, norm_gain)
    load(q_h, WB.at[slot(), pl.ds(0, 128)])
    load(ci_h, WB.at[slot(), pl.ds(128, 256)])
    load(cg_h, WB.at[slot(), pl.ds(384, 256)])
    load(co_h, WC.at[slot(), pl.ds(0, 256)])
    load(vo_h, WC.at[slot(), pl.ds(256, 256)])
    load(dd_h, ddown)
    load(du_h, dup)
    load(db_h, dbias)
    load(de_h, dextra)
    load(taps_h, taps)
    load(hg_h, hgain)
    for copy in loads[:4]:
        copy.wait()
    raw_rows = tok[...].astype(F32)
    scale = lax.rsqrt(jnp.mean(raw_rows * raw_rows, axis=-1, keepdims=True) + EPSILON)
    T[token_rows(), :] = (raw_rows * scale * norm_gain[...]).astype(BF16)
    for copy in loads[4:]:
        copy.wait()

    pl.semaphore_wait(barrier, len(peers))

    def place(j):
        return 0 if j == 0 else (-j if j <= 8 else j - 8)

    class Ring:
        def __init__(self, W, tag):
            self.W, self.tag = W, tag

        def hop(self, chain, sign, k):
            ref = self.W.at[slot(-sign * (k - 1), 2 * chain)]
            send(ref, ref, (self.tag, chain, sign, k), at(dz=sign))

        def fan_out(self, j):
            ref = self.W.at[slot(place(j))]
            send(ref, ref, (self.tag, "ym", j), at(dy=1))
            send(ref, ref, (self.tag, "yp", j), at(dy=-1))

        def across(self):
            ref = self.W.at[slot()]
            send(ref, ref, (self.tag, "y2"), at(dy=2))

        def around(self, chain):
            if chain:
                arrived(self.W.at[slot(0, 2)], (self.tag, "y2"))
            self.hop(chain, 1, 1)
            self.hop(chain, -1, 1)

        def step(self, k, chains=(0, 1), fan=True):
            for chain in chains:
                for sign in (1, -1):
                    if sign == -1 and k == 8:
                        continue
                    arrived(self.W.at[slot(-sign * k, 2 * chain)], (self.tag, chain, sign, k))
                    if k < (8 if sign == 1 else 7):
                        self.hop(chain, sign, k + 1)
                    if chain == 0 and fan:
                        self.fan_out(k if sign == 1 else 8 + k)

        def column(self, *js):
            for j in js:
                plus = (j % 2 == 0) if j <= 8 else ((j - 8) % 2 == 1)
                for dy, name in ((-1, "ym"), (1, "yp")):
                    ref = self.W.at[slot(place(j), dy)]
                    arrived(ref, (self.tag, name, j))
                    if plus == (dy == -1):
                        send(ref, ref, (self.tag, "y2", j), at(dy=-dy))

        def last_column(self):
            for j in range(16):
                arrived(self.W.at[slot(place(j), 2)], (self.tag, "y2", j))

        def finish(self):
            for j in range(16):
                arrived(self.W.at[slot(place(j), -1)], (self.tag, "ym", j))
                arrived(self.W.at[slot(place(j), 1)], (self.tag, "yp", j))

    class Jumps(Ring):
        def leap(self, sign, base):
            ref = self.W.at[slot(-sign * base)]
            for d in (2, 1):
                if base + d <= (8 if sign == 1 else 7):
                    send(ref, ref, (self.tag, 0, sign, base + d), at(dz=sign * d))

        def stage(self, i):
            for d in (2, 1):
                for sign in (1, -1):
                    k = 2 * i - 2 + d
                    if k > (8 if sign == 1 else 7):
                        continue
                    arrived(self.W.at[slot(-sign * k)], (self.tag, 0, sign, k))
                    if d == 2:
                        self.leap(sign, k)
                    self.fan_out(k if sign == 1 else 8 + k)

    ring_a, ring_b, ring_c = Jumps(WA, "a"), Ring(WB, "b"), Ring(WC, "c")
    ring_a.leap(1, 0)
    ring_a.leap(-1, 0)
    ring_a.fan_out(0)
    own_rows = T.at[token_rows()]
    send(own_rows, own_rows, "tm", at(dx=1))
    send(own_rows, own_rows, "tp", at(dx=-1))
    send(own_rows, own_rows, ("tc", 0), at(flip=True))
    ring_b.across()
    ring_b.around(0)
    ring_c.across()
    ring_c.around(0)
    ring_b.fan_out(0)

    def weights_step(k, fan=True):
        if k <= 8:
            ring_b.step(k, (0,))
            ring_c.step(k, (0,), fan=fan)
        if k == 1:
            ring_b.around(1)
            ring_c.around(1)
        else:
            ring_b.step(k - 1, (1,))
            ring_c.step(k - 1, (1,))

    def late_fan(*js):
        for j in js:
            ring_c.fan_out(j)

    half = WIDTH // 2
    blocks = LEN // BLOCK
    key_cols = pl.ds(pl.multiple_of(tp * KEY_DIM, KEY_DIM), KEY_DIM)
    val_cols = pl.ds(pl.multiple_of(tp * VAL_DIM, VAL_DIM), VAL_DIM)

    def token_step(stage):
        if stage == 0:
            ref = T.at[token_rows(dx=-1)]
            arrived(ref, "tm")
            piece = T.at[token_rows(dx=-1), pl.ds(0, half)]
            send(piece, piece, "t2a", at(dx=1))
            send(ref, ref, ("tc", 1), at(flip=True))
            ref = T.at[token_rows(dx=1)]
            arrived(ref, "tp")
            piece = T.at[token_rows(dx=1), pl.ds(half, half)]
            send(piece, piece, "t2b", at(dx=-1))
            send(ref, ref, ("tc", 2), at(flip=True))
        elif stage == 1:
            arrived(T.at[token_rows(dx=2), pl.ds(0, half)], "t2a")
            arrived(T.at[token_rows(dx=2), pl.ds(half, half)], "t2b")
            ref = T.at[token_rows(dx=2)]
            send(ref, ref, ("tc", 3), at(flip=True))
        else:
            for j in range(4):
                arrived(T.at[token_rows(dx=(0, -1, 1, 2)[j], flip=True)], ("tc", j))

    def part(array, n):
        return array[n * BLOCK : (n + 1) * BLOCK]

    def decay():
        low = mm_nt(T[...], ddown[...]).astype(BF16)
        pre = mm(low, dup[:, key_cols]) + dbias[:, key_cols]
        log_sig = jnp.minimum(pre, 0.0) - jnp.log1p(jnp.exp(-jnp.abs(pre)))
        extra = jnp.transpose(jnp.broadcast_to(dextra[...], (KEY_DIM, LEN)))
        log_decay = log_sig / 16.0 + extra
        ri = lax.broadcasted_iota(jnp.int32, (LEN, LEN), 0)
        ci = lax.broadcasted_iota(jnp.int32, (LEN, LEN), 1)
        tri = jnp.where((ri >= ci) & (ri // BLOCK == ci // BLOCK), 1.0, 0.0).astype(F32)
        cumul = lax.dot_general(
            tri, log_decay, (((1,), (0,)), ((), ())), precision=lax.Precision.HIGHEST, preferred_element_type=F32
        )
        return cumul, cumul - log_decay

    ring_a.stage(1)
    ring_a.column(0)
    weights_step(1, fan=False)
    token_step(0)
    ring_a.stage(2)
    ring_a.column(1, 9)
    weights_step(2, fan=False)
    ring_a.column(2, 10)
    ring_a.stage(3)
    ring_a.column(3, 11)
    token_step(1)
    weights_step(3, fan=False)
    ring_a.column(4, 12)
    ring_a.stage(4)
    ring_a.column(5, 13)
    token_step(2)
    cumul, before = decay()
    totals = [cumul[(n + 1) * BLOCK - 1 : (n + 1) * BLOCK] for n in range(blocks)]
    offsets = [jnp.zeros((1, KEY_DIM), F32)]
    for n in range(blocks):
        offsets.append(offsets[-1] + totals[n])
    whole = offsets[blocks]
    suffix = [jnp.zeros((1, KEY_DIM), F32)]
    for n in reversed(range(blocks)):
        suffix.append(suffix[-1] + totals[n])
    suffix = suffix[::-1][1:]
    to_end = jnp.concatenate([suffix[n] + totals[n] - part(cumul, n) for n in range(blocks)], axis=0)
    from_start = jnp.concatenate([offsets[n] + part(before, n) for n in range(blocks)], axis=0)
    to_end, from_start = jnp.exp(to_end), jnp.exp(from_start)
    marks = log_rows(whole)
    weights_step(4, fan=False)
    ring_a.column(6, 14)
    ring_a.column(7, 15, 8)
    weights_step(5, fan=False)
    ring_a.last_column()

    normed = T[...]
    kv = mm(normed, WA[...])
    key_f = kv[:, :KEY_DIM].astype(BF16).astype(F32)
    value = kv[:, KEY_DIM:].astype(BF16)
    fwd_device = mm_tn(value, (key_f * to_end).astype(BF16))
    back_device = mm_tn(value, (key_f * from_start).astype(BF16))

    for q in range(NY):
        SS[q * 144 : q * 144 + 64, :] = fwd_device[q * 64 : q * 64 + 64].astype(BF16)
        SS[q * 144 + 64 : q * 144 + 128, :] = back_device[q * 64 : q * 64 + 64].astype(BF16)
        SS[q * 144 + 128 : q * 144 + 144, :] = marks

    def message(dy=0):
        return pl.ds(pl.multiple_of(wrap(y + dy, NY) * 144, 16), 144)

    R1[message(), :] = SS[message(), :]
    for d in range(1, NY):
        send(SS.at[message(d)], R1.at[message()], ("s1", d), at(dy=d))

    late_fan(0, 1, 9)
    weights_step(6)
    for d in range(1, NY):
        arrived(R1.at[message(-d)], ("s1", d))
    in_f, in_b, in_l = [], [], []
    for q in range(NY):
        in_f.append(R1[q * 144 : q * 144 + 64, :].astype(F32))
        in_b.append(R1[q * 144 + 64 : q * 144 + 128, :].astype(F32))
        in_l.append(log_total(R1[q * 144 + 128 : q * 144 + 144, :]))
    total_f = jnp.zeros((64, KEY_DIM), F32)
    total_b = jnp.zeros((64, KEY_DIM), F32)
    log_f = jnp.zeros((1, KEY_DIM), F32)
    log_b = jnp.zeros((1, KEY_DIM), F32)
    plane_f, plane_b, gap_f, gap_b = ([None] * NY for _ in range(4))
    for q in range(NY):
        plane_f[q], gap_f[q] = total_f, log_f
        total_f = jnp.exp(in_l[q]) * total_f + in_f[q]
        log_f = log_f + in_l[q]
    for q in reversed(range(NY)):
        plane_b[q], gap_b[q] = total_b, log_b
        total_b = jnp.exp(in_l[q]) * total_b + in_b[q]
        log_b = log_b + in_l[q]
    marks = log_rows(log_f)
    M2[0:64, :] = total_f.astype(BF16)
    M2[64:80, :] = marks
    M2[80:144, :] = total_b.astype(BF16)
    M2[144:160, :] = marks

    def depth(dz=0):
        return pl.ds(pl.multiple_of(wrap(z + dz, NZ) * 80, 16), 80)

    R2[depth(), :] = M2[0:80, :]
    send(M2.at[pl.ds(0, 80)], NEAR.at[pl.ds(0, 80)], "s2f", at(dz=1))
    send(M2.at[pl.ds(80, 80)], NEAR.at[pl.ds(80, 80)], "s2b", at(dz=-1))
    late_fan(2, 10)
    weights_step(7)
    arrived(NEAR.at[pl.ds(0, 80)], "s2f")
    arrived(NEAR.at[pl.ds(80, 80)], "s2b")
    near_f = jnp.where(z > 0, NEAR[0:64, :].astype(F32), 0.0)
    near_b = jnp.where(z < NZ - 1, NEAR[80:144, :].astype(F32), 0.0)
    near_lf, near_lb = log_total(NEAR[64:80, :]), log_total(NEAR[144:160, :])
    fade = jnp.exp(log_f)
    M4[0:64, :] = (total_f + fade * near_f).astype(BF16)
    M4[64:80, :] = log_rows(log_f + near_lf)
    M4[80:144, :] = (total_b + fade * near_b).astype(BF16)
    M4[144:160, :] = log_rows(log_f + near_lb)
    for d in (8, 6, 10, 4, 12, 2, 14):
        start = pl.multiple_of(((z + d) // NZ) * 80, 16)
        send(M4.at[pl.ds(start, 80)], R2.at[depth()], ("s2", d), at(dz=d))

    late_fan(3, 11)
    weights_step(8)
    late_fan(4, 12)
    weights_step(9)
    late_fan(5, 13)
    ring_b.finish()
    qcg = mm(normed, WB[...])
    query_f = (qcg[:, :KEY_DIM] * (1.0 / math.sqrt(KEY_DIM))).astype(BF16).astype(F32)
    conv_in = qcg[:, KEY_DIM : KEY_DIM + 256].astype(BF16)
    gate = qcg[:, KEY_DIM + 256 :].astype(BF16).astype(F32)
    CI[...] = conv_in
    CP[8 : 8 + LEN, :] = conv_in.astype(F32)
    send(CI.at[pl.ds(LEN - 16, 16)], HP, "hp", next_dev)
    send(CI.at[pl.ds(0, 16)], HN, "hn", prev_dev)
    for d in range(2, NZ, 2):
        arrived(R2.at[depth(-d)], ("s2", d))
    sum_f = jnp.zeros((64, KEY_DIM), F32)
    sum_b = jnp.zeros((64, KEY_DIM), F32)
    for d in range(NZ - 2, 0, -2):
        got = R2[depth(-d), :]
        step = jnp.exp(log_total(got[64:80])) * sum_f + got[0:64].astype(F32)
        sum_f = jnp.where(z >= d, step, sum_f)
        got = R2[depth(d), :]
        step = jnp.exp(log_total(got[64:80])) * sum_b + got[0:64].astype(F32)
        sum_b = jnp.where(z + d < NZ, step, sum_b)
    sum_f = jnp.where(z > 0, jnp.exp(near_lf) * sum_f + near_f, 0.0)
    sum_b = jnp.where(z < NZ - 1, jnp.exp(near_lb) * sum_b + near_b, 0.0)
    for q in range(NY):
        M3[q * 128 : q * 128 + 64, :] = (plane_f[q] + jnp.exp(gap_f[q]) * sum_f).astype(BF16)
        M3[q * 128 + 64 : q * 128 + 128, :] = (plane_b[q] + jnp.exp(gap_b[q]) * sum_b).astype(BF16)

    def quarter(dy=0):
        return pl.ds(pl.multiple_of(wrap(y + dy, NY) * 64, 64), 64)

    def answer(dy, which):
        return pl.ds(pl.multiple_of(wrap(y + dy, NY) * 128 + 64 * which, 64), 64)

    for d in range(1, NY):
        send(M3.at[answer(d, 0)], IF.at[quarter()], ("s3f", d), at(dy=d))
        send(M3.at[answer(d, 1)], IB.at[quarter()], ("s3b", d), at(dy=d))
    IF[quarter(), :] = M3[answer(0, 0), :]
    IB[quarter(), :] = M3[answer(0, 1), :]
    lower = lax.broadcasted_iota(jnp.int32, (BLOCK, BLOCK), 0) >= lax.broadcasted_iota(jnp.int32, (BLOCK, BLOCK), 1)
    upper = lax.broadcasted_iota(jnp.int32, (BLOCK, BLOCK), 0) <= lax.broadcasted_iota(jnp.int32, (BLOCK, BLOCK), 1)
    within = []
    fwd_inc, back_inc, fwd_query, back_query = [], [], [], []
    for n in range(blocks):
        cum_n, bef_n, key_n, query_n, value_n = (part(a, n) for a in (cumul, before, key_f, query_f, value))
        fq = (query_n * jnp.exp(cum_n)).astype(BF16)
        ks = (key_n * jnp.exp(bef_n)).astype(BF16)
        fwd_scores = mm_nt(fq, (key_n * jnp.exp(-cum_n)).astype(BF16))
        back_scores = mm_nt((query_n * jnp.exp(-bef_n)).astype(BF16), ks)
        scores = jnp.where(lower, fwd_scores, 0.0) + jnp.where(upper, back_scores, 0.0)
        within.append(mm(scores.astype(BF16), value_n))
        fwd_inc.append(mm_tn(value_n, (key_n * jnp.exp(totals[n] - cum_n)).astype(BF16)))
        back_inc.append(mm_tn(value_n, ks))
        fwd_query.append(fq)
        back_query.append((query_n * jnp.exp(totals[n] - bef_n)).astype(BF16))
    state = fwd_inc[0]
    for n in range(1, blocks):
        within[n] = within[n] + mm_nt(fwd_query[n], state.astype(BF16))
        state = jnp.exp(totals[n]) * state + fwd_inc[n]
    state = back_inc[blocks - 1]
    for n in reversed(range(blocks - 1)):
        within[n] = within[n] + mm_nt(back_query[n], state.astype(BF16))
        state = jnp.exp(totals[n]) * state + back_inc[n]
    local = jnp.concatenate(within, axis=0)
    far_fwd = jnp.concatenate(
        [part(query_f, n) * jnp.exp(offsets[n] + part(cumul, n)) for n in range(blocks)], axis=0
    ).astype(BF16)
    far_back = jnp.concatenate(
        [part(query_f, n) * jnp.exp(suffix[n] + (totals[n] - part(before, n))) for n in range(blocks)], axis=0
    ).astype(BF16)

    arrived(HP, "hp")
    arrived(HN, "hn")
    first = HP[...].astype(F32)[15:16]
    last = HN[...].astype(F32)[0:1]
    CP[7:8, :] = jnp.where(s > 0, first, 0.0)
    CP[8 + LEN : 9 + LEN, :] = jnp.where(s < NZ * NY - 1, last, 0.0)
    tap = taps[:, val_cols]
    mixed = CP[7 : 7 + LEN, :] * tap[0:1] + CP[8 : 8 + LEN, :] * tap[1:2] + CP[9 : 9 + LEN, :] * tap[2:3]
    XC[:, 0:256] = (mixed * (gate * (1.0 / (1.0 + jnp.exp(-gate))))).astype(BF16)

    for d in range(1, NY):
        arrived(IF.at[quarter(-d)], ("s3f", d))
        arrived(IB.at[quarter(-d)], ("s3b", d))
    raw = local + mm_nt(far_fwd, IF[...]) + mm_nt(far_back, IB[...])
    norm = lax.rsqrt(jnp.mean(raw * raw, axis=-1, keepdims=True) + EPSILON)
    XC[:, 256:512] = (raw * norm * hgain[:, val_cols]).astype(BF16)
    ring_c.finish()

    order = (2, 1, 3, 0)
    pieces, piece = 4, WIDTH // 4
    there = jnp.concatenate([XC[token_rows(dx=r, flip=True), :] for r in order], axis=0)
    here = jnp.concatenate([XC[token_rows(dx=r), :] for r in order], axis=0)

    def rows4(n, i=0, count=4):
        return pl.ds((n * 4 + i) * ROWS, count * ROWS)

    def pair_send(n):
        PS[rows4(n), :] = mm_nt(there, WC[n * piece : (n + 1) * piece, :]).astype(BF16)
        send(PS.at[rows4(n)], PR.at[rows4(n)], ("pr", n), at(flip=True))

    def x_send(n):
        mine = mm_nt(here, WC[n * piece : (n + 1) * piece, :])
        arrived(PR.at[rows4(n)], ("pr", n))
        both = mine + PR[rows4(n), :].astype(F32)
        XS[rows4(n), :] = both.astype(BF16)
        for i in range(3):
            send(XS.at[rows4(n, i, 1)], XR.at[rows4(n, i, 1)], ("xr", n, i), at(dx=order[i]))
        PO[pl.ds(n * ROWS, ROWS), :] = both[3 * ROWS :]

    pair_send(0)
    pair_send(1)
    for n in range(pieces):
        x_send(n)
        if n + 2 < pieces:
            pair_send(n + 2)
    for n in range(pieces):
        total = PO[n * ROWS : (n + 1) * ROWS, :]
        for i in (1, 2, 0):
            arrived(XR.at[rows4(n, i, 1)], ("xr", n, i))
            total = total + XR[rows4(n, i, 1), :].astype(F32)
        out[:, n * piece : (n + 1) * piece] = total.astype(BF16)

    for copy in sends:
        copy.wait_send()
    assert len(sends) <= N_SEND and len(names) <= N_RECV, (len(sends), len(names))


def local(
    tokens, norm_gain, conv_in_weight, conv_gate_weight, conv_taps, query_weight, key_weight, value_weight,
    decay_down, decay_up, decay_bias, decay_extra, head_gain, conv_out_weight, value_out_weight,
):
    hbm = pl.BlockSpec(memory_space=pl.ANY)
    return pl.pallas_call(
        kernel,
        out_shape=jax.ShapeDtypeStruct((ROWS, WIDTH), BF16),
        in_specs=[hbm] * 15,
        out_specs=pl.BlockSpec(memory_space=pltpu.VMEM),
        scratch_shapes=[
            pltpu.VMEM((ROWS, WIDTH), BF16),
            pltpu.VMEM((1, WIDTH), F32),
            pltpu.VMEM((3, WIDTH), F32),
            pltpu.VMEM((16, WIDTH), BF16),
            pltpu.VMEM((16, 1024), BF16),
            pltpu.VMEM((1, 1024), F32),
            pltpu.VMEM((1, LEN), F32),
            pltpu.VMEM((1, WIDTH), F32),
            pltpu.VMEM((2048, 384), BF16),
            pltpu.VMEM((2048, 640), BF16),
            pltpu.VMEM((2048, 512), BF16),
            pltpu.VMEM((LEN, WIDTH), BF16),
            pltpu.VMEM((NY * 144, KEY_DIM), BF16),
            pltpu.VMEM((NY * 144, KEY_DIM), BF16),
            pltpu.VMEM((160, KEY_DIM), BF16),
            pltpu.VMEM((160, KEY_DIM), BF16),
            pltpu.VMEM((160, KEY_DIM), BF16),
            pltpu.VMEM((NZ * 80, KEY_DIM), BF16),
            pltpu.VMEM((NY * 128, KEY_DIM), BF16),
            pltpu.VMEM((VAL_DIM, KEY_DIM), BF16),
            pltpu.VMEM((VAL_DIM, KEY_DIM), BF16),
            pltpu.VMEM((LEN, 256), BF16),
            pltpu.VMEM((LEN + 16, 256), F32),
            pltpu.VMEM((16, 256), BF16),
            pltpu.VMEM((16, 256), BF16),
            pltpu.VMEM((LEN, 512), BF16),
            pltpu.VMEM((4 * ROWS, WIDTH // 4), F32),
            pltpu.VMEM((16 * ROWS, WIDTH // 4), BF16),
            pltpu.VMEM((16 * ROWS, WIDTH // 4), BF16),
            pltpu.VMEM((16 * ROWS, WIDTH // 4), BF16),
            pltpu.VMEM((16 * ROWS, WIDTH // 4), BF16),
            pltpu.SemaphoreType.DMA((N_SEND,)),
            pltpu.SemaphoreType.DMA((N_RECV,)),
            pltpu.SemaphoreType.DMA((15,)),
        ],
        compiler_params=pltpu.CompilerParams(collective_id=0, has_side_effects=True, vmem_limit_bytes=60 * 1024 * 1024),
        cost_estimate=pl.CostEstimate(flops=3_000_000_000, bytes_accessed=1_000_000, transcendentals=0),
    )(
        tokens, norm_gain.reshape(1, -1), conv_in_weight, conv_gate_weight, conv_taps, query_weight, key_weight,
        value_weight, decay_down.T, decay_up, decay_bias.reshape(1, -1), decay_extra, head_gain.reshape(1, -1),
        conv_out_weight.T, value_out_weight.T,
    )


def solution(mesh):
    torus = Mesh(mesh.devices.reshape(NZ, NY, NX, NC), SP_TP)
    return jax.shard_map(
        local,
        mesh=torus,
        in_specs=(
            P(SP_TP, None), P(), P(SP, TP), P(SP, TP), P(), P(SP, TP), P(SP, TP), P(SP, TP),
            P(), P(), P(), P(TP, SP), P(), P(TP, SP), P(TP, SP),
        ),
        out_specs=P(SP_TP, None),
        check_vma=False,
    )
```

```python
import functools
import math

import jax
import jax.numpy as jnp
from jax import lax
from jax.experimental import pallas as pl
from jax.experimental.pallas import tpu as pltpu
from jax.sharding import Mesh
from jax.sharding import PartitionSpec as P

NZ, NY, NX, NC = 16, 4, 4, 2
KEY_DIM = 128
VAL_DIM = 256
BLOCK = 64
ROWS = 48
LEN = 384
WIDTH = 2048
EPSILON = 1e-06
SP = ("z", "y")
TP = ("x", "c")
SP_TP = ("z", "y", "x", "c")
F32 = jnp.float32
BF16 = jnp.bfloat16
MESH = pl.DeviceIdType.MESH
N_SEND = 256
N_RECV = 256


def mm(a, b):
    return lax.dot_general(a, b, (((1,), (0,)), ((), ())), preferred_element_type=F32)


def mm_nt(a, b):
    return lax.dot_general(a, b, (((1,), (1,)), ((), ())), preferred_element_type=F32)


def mm_tn(a, b):
    return lax.dot_general(a, b, (((0,), (0,)), ((), ())), preferred_element_type=F32)


def wrap(value, size):
    return lax.rem(value + size, size)


def split3(row):
    hi = row.astype(BF16)
    rest = row - hi.astype(F32)
    mid = rest.astype(BF16)
    low = (rest - mid.astype(F32)).astype(BF16)
    return hi, mid, low


def log_rows(row):
    hi, mid, low = split3(row)
    index = lax.broadcasted_iota(jnp.int32, (16, KEY_DIM), 0)
    spread = [jnp.broadcast_to(p.astype(F32), (16, KEY_DIM)) for p in (hi, mid, low)]
    out = jnp.where(index == 0, spread[0], jnp.where(index == 1, spread[1], jnp.where(index == 2, spread[2], 0.0)))
    return out.astype(BF16)


def log_total(rows16):
    return jnp.sum(rows16.astype(F32), axis=0, keepdims=True)


def kernel(
    tok_h, gain_h, ci_h, cg_h, taps_h, q_h, k_h, v_h, dd_h, du_h, db_h, de_h, hg_h, co_h, vo_h,
    out,
    tok, norm_gain, taps, ddown, dup, dbias, dextra, hgain,
    WA, WB, WC, T, SS, R1, M2, NEAR, M4, R2, M3, IF, IB, CI, CP, HP, HN, XC, PO, PS, PR, XS, XQ, XP, XR,
    ssem, rsem, lsem,
):
    z, y, x, c = (lax.axis_index(a) for a in SP_TP)
    tp = x * 2 + c
    s = z * 4 + y
    other = 1 - c
    names = {}
    sends = []

    def at(dz=0, dy=0, dx=0, flip=False):
        return (wrap(z + dz, NZ), wrap(y + dy, NY), wrap(x + dx, NX), other if flip else c)

    def sem(name):
        return rsem.at[names.setdefault(name, len(names))]

    def send(src, dst, name, device):
        copy = pltpu.make_async_remote_copy(
            src_ref=src, dst_ref=dst, send_sem=ssem.at[len(sends)], recv_sem=sem(name),
            device_id=device, device_id_type=MESH,
        )
        copy.start()
        sends.append(copy)

    def arrived(dst, name):
        pltpu.make_async_remote_copy(
            src_ref=dst, dst_ref=dst, send_sem=ssem.at[0], recv_sem=sem(name),
            device_id=(z, y, x, c), device_id_type=MESH,
        ).wait_recv()

    after = lax.rem(s + 1, NZ * NY)
    ahead = lax.rem(s + NZ * NY - 1, NZ * NY)
    next_dev = (after // NY, lax.rem(after, NY), x, c)
    prev_dev = (ahead // NY, lax.rem(ahead, NY), x, c)
    peers = [at(dz=d) for d in (1, -1, 2, -2)]
    peers += [at(dy=d) for d in range(1, NY)]
    peers += [at(dx=d) for d in range(1, NX)]
    peers += [at(flip=True), next_dev, prev_dev]
    barrier = pltpu.get_barrier_semaphore()
    for peer in peers:
        pl.semaphore_signal(barrier, inc=1, device_id=peer, device_id_type=MESH)

    def slot(dz=0, dy=0):
        index = wrap(z + dz, NZ) * NY + wrap(y + dy, NY)
        return pl.ds(pl.multiple_of(index * 32, 32), 32)

    def plane(dz=0):
        return pl.ds(pl.multiple_of(wrap(z + dz, NZ) * 128, 128), 128)

    def token_rows(dx=0, flip=False):
        index = wrap(x + dx, NX) * 2 + (other if flip else c)
        return pl.ds(pl.multiple_of(index * ROWS, 16), ROWS)

    loads = []

    def load(src, dst):
        copy = pltpu.make_async_copy(src, dst, lsem.at[len(loads)])
        copy.start()
        loads.append(copy)

    load(k_h, WA.at[slot(), pl.ds(0, 128)])
    load(v_h, WA.at[slot(), pl.ds(128, 256)])
    load(tok_h, tok)
    load(gain_h, norm_gain)
    load(q_h, WB.at[slot(), pl.ds(0, 128)])
    load(ci_h, WB.at[slot(), pl.ds(128, 256)])
    load(cg_h, WB.at[slot(), pl.ds(384, 256)])
    load(co_h, WC.at[slot(), pl.ds(0, 256)])
    load(vo_h, WC.at[slot(), pl.ds(256, 256)])
    load(dd_h, ddown)
    load(du_h, dup)
    load(db_h, dbias)
    load(de_h, dextra)
    load(taps_h, taps)
    load(hg_h, hgain)
    for copy in loads[:4]:
        copy.wait()
    raw_rows = tok[...].astype(F32)
    scale = lax.rsqrt(jnp.mean(raw_rows * raw_rows, axis=-1, keepdims=True) + EPSILON)
    T[token_rows(), :] = (raw_rows * scale * norm_gain[...]).astype(BF16)
    for copy in loads[4:]:
        copy.wait()

    pl.semaphore_wait(barrier, len(peers))

    def place(j):
        return 0 if j == 0 else (-j if j <= 8 else j - 8)

    class Ring:
        def __init__(self, W, tag):
            self.W, self.tag = W, tag

        def hop(self, chain, sign, k):
            ref = self.W.at[slot(-sign * (k - 1), 2 * chain)]
            send(ref, ref, (self.tag, chain, sign, k), at(dz=sign))

        def fan_out(self, j):
            ref = self.W.at[slot(place(j))]
            send(ref, ref, (self.tag, "ym", j), at(dy=1))
            send(ref, ref, (self.tag, "yp", j), at(dy=-1))

        def across(self):
            ref = self.W.at[slot()]
            send(ref, ref, (self.tag, "y2"), at(dy=2))

        def around(self, chain):
            if chain:
                arrived(self.W.at[slot(0, 2)], (self.tag, "y2"))
            self.hop(chain, 1, 1)
            self.hop(chain, -1, 1)

        def step(self, k, chains=(0, 1), fan=True):
            for chain in chains:
                for sign in (1, -1):
                    if sign == -1 and k == 8:
                        continue
                    arrived(self.W.at[slot(-sign * k, 2 * chain)], (self.tag, chain, sign, k))
                    if k < (8 if sign == 1 else 7):
                        self.hop(chain, sign, k + 1)
                    if chain == 0 and fan:
                        self.fan_out(k if sign == 1 else 8 + k)

        def column(self, *js):
            for j in js:
                plus = (j % 2 == 0) if j <= 8 else ((j - 8) % 2 == 1)
                for dy, name in ((-1, "ym"), (1, "yp")):
                    ref = self.W.at[slot(place(j), dy)]
                    arrived(ref, (self.tag, name, j))
                    if plus == (dy == -1):
                        send(ref, ref, (self.tag, "y2", j), at(dy=-dy))

        def last_column(self):
            for j in range(16):
                arrived(self.W.at[slot(place(j), 2)], (self.tag, "y2", j))

        def finish(self):
            for j in range(16):
                arrived(self.W.at[slot(place(j), -1)], (self.tag, "ym", j))
                arrived(self.W.at[slot(place(j), 1)], (self.tag, "yp", j))

    class Jumps(Ring):
        def leap(self, sign, base):
            ref = self.W.at[slot(-sign * base)]
            for d in (2, 1):
                if base + d <= (8 if sign == 1 else 7):
                    send(ref, ref, (self.tag, 0, sign, base + d), at(dz=sign * d))

        def stage(self, i):
            for d in (2, 1):
                for sign in (1, -1):
                    k = 2 * i - 2 + d
                    if k > (8 if sign == 1 else 7):
                        continue
                    arrived(self.W.at[slot(-sign * k)], (self.tag, 0, sign, k))
                    if d == 2:
                        self.leap(sign, k)
                    self.fan_out(k if sign == 1 else 8 + k)

    ring_a, ring_b, ring_c = Jumps(WA, "a"), Ring(WB, "b"), Ring(WC, "c")
    ring_a.leap(1, 0)
    ring_a.leap(-1, 0)
    ring_a.fan_out(0)
    own_rows = T.at[token_rows()]
    send(own_rows, own_rows, "tm", at(dx=1))
    send(own_rows, own_rows, "tp", at(dx=-1))
    send(own_rows, own_rows, ("tc", 0), at(flip=True))
    ring_b.across()
    ring_b.around(0)
    ring_c.across()
    ring_c.around(0)
    ring_b.fan_out(0)

    def weights_step(k, fan=True):
        if k <= 8:
            ring_b.step(k, (0,))
            ring_c.step(k, (0,), fan=fan)
        if k == 1:
            ring_b.around(1)
            ring_c.around(1)
        else:
            ring_b.step(k - 1, (1,))
            ring_c.step(k - 1, (1,))

    def late_fan(*js):
        for j in js:
            ring_c.fan_out(j)

    half = WIDTH // 2
    blocks = LEN // BLOCK
    key_cols = pl.ds(pl.multiple_of(tp * KEY_DIM, KEY_DIM), KEY_DIM)
    val_cols = pl.ds(pl.multiple_of(tp * VAL_DIM, VAL_DIM), VAL_DIM)

    def token_step(stage):
        if stage == 0:
            ref = T.at[token_rows(dx=-1)]
            arrived(ref, "tm")
            piece = T.at[token_rows(dx=-1), pl.ds(0, half)]
            send(piece, piece, "t2a", at(dx=1))
            send(ref, ref, ("tc", 1), at(flip=True))
            ref = T.at[token_rows(dx=1)]
            arrived(ref, "tp")
            piece = T.at[token_rows(dx=1), pl.ds(half, half)]
            send(piece, piece, "t2b", at(dx=-1))
            send(ref, ref, ("tc", 2), at(flip=True))
        elif stage == 1:
            arrived(T.at[token_rows(dx=2), pl.ds(0, half)], "t2a")
            arrived(T.at[token_rows(dx=2), pl.ds(half, half)], "t2b")
            ref = T.at[token_rows(dx=2)]
            send(ref, ref, ("tc", 3), at(flip=True))
        else:
            for j in range(4):
                arrived(T.at[token_rows(dx=(0, -1, 1, 2)[j], flip=True)], ("tc", j))

    def part(array, n):
        return array[n * BLOCK : (n + 1) * BLOCK]

    def decay():
        low = mm_nt(T[0:LEN, :], ddown[...]).astype(BF16)
        pre = mm(low, dup[:, key_cols]) + dbias[:, key_cols]
        log_sig = jnp.minimum(pre, 0.0) - jnp.log1p(jnp.exp(-jnp.abs(pre)))
        extra = jnp.transpose(jnp.broadcast_to(dextra[...], (KEY_DIM, LEN)))
        log_decay = log_sig / 16.0 + extra
        ri = lax.broadcasted_iota(jnp.int32, (LEN, LEN), 0)
        ci = lax.broadcasted_iota(jnp.int32, (LEN, LEN), 1)
        tri = jnp.where((ri >= ci) & (ri // BLOCK == ci // BLOCK), 1.0, 0.0).astype(F32)
        cumul = lax.dot_general(
            tri, log_decay, (((1,), (0,)), ((), ())), precision=lax.Precision.HIGHEST, preferred_element_type=F32
        )
        return cumul, cumul - log_decay

    ring_a.stage(1)
    ring_a.column(0)
    weights_step(1, fan=False)
    token_step(0)
    ring_a.stage(2)
    ring_a.column(1, 9)
    weights_step(2, fan=False)
    ring_a.column(2, 10)
    ring_a.stage(3)
    ring_a.column(3, 11)
    token_step(1)
    weights_step(3, fan=False)
    ring_a.column(4, 12)
    ring_a.stage(4)
    ring_a.column(5, 13)
    token_step(2)
    for name, device, edge, at_row in (("hp", next_dev, LEN - 16, 15), ("hn", prev_dev, 0, 0)):
        rows = T[edge : edge + 16, :].astype(F32)[at_row : at_row + 1]
        arow = lax.broadcasted_iota(jnp.int32, (16, 256), 0)
        spread = jnp.zeros((16, 256), F32)
        for i in range(8):
            spread = jnp.where(arow == i, rows[:, i * 256 : (i + 1) * 256], spread)
        to = pl.ds(16 if at_row == 0 else 0, 16)
        CI[to, :] = spread.astype(BF16)
        send(CI.at[to], HN if at_row == 0 else HP, name, device)
    cumul, before = decay()
    totals = [cumul[(n + 1) * BLOCK - 1 : (n + 1) * BLOCK] for n in range(blocks)]
    offsets = [jnp.zeros((1, KEY_DIM), F32)]
    for n in range(blocks):
        offsets.append(offsets[-1] + totals[n])
    whole = offsets[blocks]
    suffix = [jnp.zeros((1, KEY_DIM), F32)]
    for n in reversed(range(blocks)):
        suffix.append(suffix[-1] + totals[n])
    suffix = suffix[::-1][1:]
    to_end = jnp.concatenate([suffix[n] + totals[n] - part(cumul, n) for n in range(blocks)], axis=0)
    from_start = jnp.concatenate([offsets[n] + part(before, n) for n in range(blocks)], axis=0)
    to_end, from_start = jnp.exp(to_end), jnp.exp(from_start)
    marks = log_rows(whole)
    weights_step(4, fan=False)
    ring_a.column(6, 14)
    ring_a.column(7, 15, 8)
    weights_step(5, fan=False)
    ring_a.last_column()

    normed = T[0:LEN, :]
    kv = mm(normed, WA[...])
    key_f = kv[:, :KEY_DIM].astype(BF16).astype(F32)
    value = kv[:, KEY_DIM:].astype(BF16)
    fwd_device = mm_tn(value, (key_f * to_end).astype(BF16))
    back_device = mm_tn(value, (key_f * from_start).astype(BF16))

    for q in range(NY):
        SS[q * 144 : q * 144 + 64, :] = fwd_device[q * 64 : q * 64 + 64].astype(BF16)
        SS[q * 144 + 64 : q * 144 + 128, :] = back_device[q * 64 : q * 64 + 64].astype(BF16)
        SS[q * 144 + 128 : q * 144 + 144, :] = marks

    def message(dy=0):
        return pl.ds(pl.multiple_of(wrap(y + dy, NY) * 144, 16), 144)

    R1[message(), :] = SS[message(), :]
    for d in range(1, NY):
        send(SS.at[message(d)], R1.at[message()], ("s1", d), at(dy=d))

    late_fan(0, 1, 9)
    weights_step(6)
    for d in range(1, NY):
        arrived(R1.at[message(-d)], ("s1", d))
    in_f, in_b, in_l = [], [], []
    for q in range(NY):
        in_f.append(R1[q * 144 : q * 144 + 64, :].astype(F32))
        in_b.append(R1[q * 144 + 64 : q * 144 + 128, :].astype(F32))
        in_l.append(log_total(R1[q * 144 + 128 : q * 144 + 144, :]))
    total_f = jnp.zeros((64, KEY_DIM), F32)
    total_b = jnp.zeros((64, KEY_DIM), F32)
    log_f = jnp.zeros((1, KEY_DIM), F32)
    log_b = jnp.zeros((1, KEY_DIM), F32)
    plane_f, plane_b, gap_f, gap_b = ([None] * NY for _ in range(4))
    for q in range(NY):
        plane_f[q], gap_f[q] = total_f, log_f
        total_f = jnp.exp(in_l[q]) * total_f + in_f[q]
        log_f = log_f + in_l[q]
    for q in reversed(range(NY)):
        plane_b[q], gap_b[q] = total_b, log_b
        total_b = jnp.exp(in_l[q]) * total_b + in_b[q]
        log_b = log_b + in_l[q]
    marks = log_rows(log_f)
    M2[0:64, :] = total_f.astype(BF16)
    M2[64:80, :] = marks
    M2[80:144, :] = total_b.astype(BF16)
    M2[144:160, :] = marks

    def depth(dz=0):
        return pl.ds(pl.multiple_of(wrap(z + dz, NZ) * 80, 16), 80)

    R2[depth(), :] = M2[0:80, :]
    send(M2.at[pl.ds(0, 80)], NEAR.at[pl.ds(0, 80)], "s2f", at(dz=1))
    send(M2.at[pl.ds(80, 80)], NEAR.at[pl.ds(80, 80)], "s2b", at(dz=-1))
    late_fan(2, 10)
    weights_step(7)
    arrived(NEAR.at[pl.ds(0, 80)], "s2f")
    arrived(NEAR.at[pl.ds(80, 80)], "s2b")
    near_f = jnp.where(z > 0, NEAR[0:64, :].astype(F32), 0.0)
    near_b = jnp.where(z < NZ - 1, NEAR[80:144, :].astype(F32), 0.0)
    near_lf, near_lb = log_total(NEAR[64:80, :]), log_total(NEAR[144:160, :])
    fade = jnp.exp(log_f)
    M4[0:64, :] = (total_f + fade * near_f).astype(BF16)
    M4[64:80, :] = log_rows(log_f + near_lf)
    M4[80:144, :] = (total_b + fade * near_b).astype(BF16)
    M4[144:160, :] = log_rows(log_f + near_lb)
    for d in (8, 6, 10, 4, 12, 2, 14):
        start = pl.multiple_of(((z + d) // NZ) * 80, 16)
        send(M4.at[pl.ds(start, 80)], R2.at[depth()], ("s2", d), at(dz=d))

    late_fan(3, 11)
    weights_step(8)
    late_fan(4, 12)
    weights_step(9)
    late_fan(5, 13)
    for d in range(2, NZ, 2):
        arrived(R2.at[depth(-d)], ("s2", d))
    sum_f = jnp.zeros((64, KEY_DIM), F32)
    sum_b = jnp.zeros((64, KEY_DIM), F32)
    for d in range(NZ - 2, 0, -2):
        got = R2[depth(-d), :]
        step = jnp.exp(log_total(got[64:80])) * sum_f + got[0:64].astype(F32)
        sum_f = jnp.where(z >= d, step, sum_f)
        got = R2[depth(d), :]
        step = jnp.exp(log_total(got[64:80])) * sum_b + got[0:64].astype(F32)
        sum_b = jnp.where(z + d < NZ, step, sum_b)
    sum_f = jnp.where(z > 0, jnp.exp(near_lf) * sum_f + near_f, 0.0)
    sum_b = jnp.where(z < NZ - 1, jnp.exp(near_lb) * sum_b + near_b, 0.0)
    for q in range(NY):
        M3[q * 128 : q * 128 + 64, :] = (plane_f[q] + jnp.exp(gap_f[q]) * sum_f).astype(BF16)
        M3[q * 128 + 64 : q * 128 + 128, :] = (plane_b[q] + jnp.exp(gap_b[q]) * sum_b).astype(BF16)

    def quarter(dy=0):
        return pl.ds(pl.multiple_of(wrap(y + dy, NY) * 64, 64), 64)

    def answer(dy, which):
        return pl.ds(pl.multiple_of(wrap(y + dy, NY) * 128 + 64 * which, 64), 64)

    for d in range(1, NY):
        send(M3.at[answer(d, 0)], IF.at[quarter()], ("s3f", d), at(dy=d))
        send(M3.at[answer(d, 1)], IB.at[quarter()], ("s3b", d), at(dy=d))
    IF[quarter(), :] = M3[answer(0, 0), :]
    IB[quarter(), :] = M3[answer(0, 1), :]
    ring_b.finish()
    arrived(HP, "hp")
    arrived(HN, "hn")
    for i in range(8):
        seg = pl.ds(i * 256, 256)
        arow = lax.broadcasted_iota(jnp.int32, (16, 256), 0)
        row_p = jnp.where(s > 0, HP[i : i + 1, :].astype(F32), 0.0)
        row_n = jnp.where(s < NZ * NY - 1, HN[i : i + 1, :].astype(F32), 0.0)
        T[pl.ds(LEN, 16), seg] = jnp.where(arow == 0, row_p, jnp.where(arow == 1, row_n, 0.0)).astype(BF16)
    conv_in = mm(T[...], WB[:, 128:384]).astype(BF16).astype(F32)
    CP[8 : 8 + LEN, :] = conv_in[:LEN]
    CP[7:8, :] = conv_in[LEN : LEN + 1]
    CP[8 + LEN : 9 + LEN, :] = conv_in[LEN + 1 : LEN + 2]
    query_f = (mm(normed, WB[:, 0:128]) * (1.0 / math.sqrt(KEY_DIM))).astype(BF16).astype(F32)
    gate = mm(normed, WB[:, 384:640]).astype(BF16).astype(F32)
    lower = lax.broadcasted_iota(jnp.int32, (BLOCK, BLOCK), 0) >= lax.broadcasted_iota(jnp.int32, (BLOCK, BLOCK), 1)
    upper = lax.broadcasted_iota(jnp.int32, (BLOCK, BLOCK), 0) <= lax.broadcasted_iota(jnp.int32, (BLOCK, BLOCK), 1)
    within = []
    fwd_inc, back_inc, fwd_query, back_query = [], [], [], []
    for n in range(blocks):
        cum_n, bef_n, key_n, query_n, value_n = (part(a, n) for a in (cumul, before, key_f, query_f, value))
        fq = (query_n * jnp.exp(cum_n)).astype(BF16)
        ks = (key_n * jnp.exp(bef_n)).astype(BF16)
        fwd_scores = mm_nt(fq, (key_n * jnp.exp(-cum_n)).astype(BF16))
        back_scores = mm_nt((query_n * jnp.exp(-bef_n)).astype(BF16), ks)
        scores = jnp.where(lower, fwd_scores, 0.0) + jnp.where(upper, back_scores, 0.0)
        within.append(mm(scores.astype(BF16), value_n))
        fwd_inc.append(mm_tn(value_n, (key_n * jnp.exp(totals[n] - cum_n)).astype(BF16)))
        back_inc.append(mm_tn(value_n, ks))
        fwd_query.append(fq)
        back_query.append((query_n * jnp.exp(totals[n] - bef_n)).astype(BF16))
    state = fwd_inc[0]
    for n in range(1, blocks):
        within[n] = within[n] + mm_nt(fwd_query[n], state.astype(BF16))
        state = jnp.exp(totals[n]) * state + fwd_inc[n]
    state = back_inc[blocks - 1]
    for n in reversed(range(blocks - 1)):
        within[n] = within[n] + mm_nt(back_query[n], state.astype(BF16))
        state = jnp.exp(totals[n]) * state + back_inc[n]
    local = jnp.concatenate(within, axis=0)
    far_fwd = jnp.concatenate(
        [part(query_f, n) * jnp.exp(offsets[n] + part(cumul, n)) for n in range(blocks)], axis=0
    ).astype(BF16)
    far_back = jnp.concatenate(
        [part(query_f, n) * jnp.exp(suffix[n] + (totals[n] - part(before, n))) for n in range(blocks)], axis=0
    ).astype(BF16)

    tap = taps[:, val_cols]
    mixed = CP[7 : 7 + LEN, :] * tap[0:1] + CP[8 : 8 + LEN, :] * tap[1:2] + CP[9 : 9 + LEN, :] * tap[2:3]
    XC[:, 0:256] = (mixed * (gate * (1.0 / (1.0 + jnp.exp(-gate))))).astype(BF16)

    for d in range(1, NY):
        arrived(IF.at[quarter(-d)], ("s3f", d))
        arrived(IB.at[quarter(-d)], ("s3b", d))
    raw = local + mm_nt(far_fwd, IF[...]) + mm_nt(far_back, IB[...])
    norm = lax.rsqrt(jnp.mean(raw * raw, axis=-1, keepdims=True) + EPSILON)
    XC[:, 256:512] = (raw * norm * hgain[:, val_cols]).astype(BF16)
    ring_c.finish()

    order = (2, 1, 3, 0)
    pieces, piece = 4, WIDTH // 4
    there = jnp.concatenate([XC[token_rows(dx=r, flip=True), :] for r in order], axis=0)
    here = jnp.concatenate([XC[token_rows(dx=r), :] for r in order], axis=0)

    def rows4(n, i=0, count=4):
        return pl.ds((n * 4 + i) * ROWS, count * ROWS)

    def pair_send(n):
        PS[rows4(n), :] = mm_nt(there, WC[n * piece : (n + 1) * piece, :]).astype(BF16)
        send(PS.at[rows4(n)], PR.at[rows4(n)], ("pr", n), at(flip=True))

    side = piece // 2
    near, far_side = pl.ds(0, side), pl.ds(side, side)

    def x_send(n):
        mine = mm_nt(here, WC[n * piece : (n + 1) * piece, :])
        arrived(PR.at[rows4(n)], ("pr", n))
        both = mine + PR[rows4(n), :].astype(F32)
        XS[rows4(n), :] = both.astype(BF16)
        send(XS.at[rows4(n, 0, 1), near], XQ.at[rows2(n, 0)], ("xq", n, 0), at(dx=1))
        send(XS.at[rows4(n, 0, 1), far_side], XQ.at[rows2(n, 1)], ("xq", n, 1), at(dx=-1))
        send(XS.at[rows4(n, 1, 1), far_side], XR.at[rows2(n, 0), far_side], ("xr", n, 0), at(dx=1))
        send(XS.at[rows4(n, 2, 1), near], XR.at[rows2(n, 1), near], ("xr", n, 1), at(dx=-1))
        PO[pl.ds(n * ROWS * 3, ROWS * 3), :] = both[ROWS:]

    def rows2(n, i):
        return pl.ds((n * 2 + i) * ROWS, ROWS)

    def x_pass(n):
        base = n * ROWS * 3
        arrived(XQ.at[rows2(n, 0)], ("xq", n, 0))
        XP[rows2(n, 0), :] = (PO[base : base + ROWS, 0:side] + XQ[rows2(n, 0), :].astype(F32)).astype(BF16)
        send(XP.at[rows2(n, 0)], XR.at[rows2(n, 0), near], ("xs", n, 0), at(dx=1))
        arrived(XQ.at[rows2(n, 1)], ("xq", n, 1))
        XP[rows2(n, 1), :] = (PO[base + ROWS : base + 2 * ROWS, side:] + XQ[rows2(n, 1), :].astype(F32)).astype(BF16)
        send(XP.at[rows2(n, 1)], XR.at[rows2(n, 1), far_side], ("xs", n, 1), at(dx=-1))

    pair_send(0)
    pair_send(1)
    for n in range(pieces):
        x_send(n)
        if n + 2 < pieces:
            pair_send(n + 2)
    for n in range(pieces):
        x_pass(n)
    for n in range(pieces):
        total = PO[n * ROWS * 3 + 2 * ROWS : (n + 1) * ROWS * 3, :]
        arrived(XR.at[rows2(n, 0), far_side], ("xr", n, 0))
        arrived(XR.at[rows2(n, 1), near], ("xr", n, 1))
        arrived(XR.at[rows2(n, 0), near], ("xs", n, 0))
        arrived(XR.at[rows2(n, 1), far_side], ("xs", n, 1))
        total = total + XR[rows2(n, 0), :].astype(F32) + XR[rows2(n, 1), :].astype(F32)
        out[:, n * piece : (n + 1) * piece] = total.astype(BF16)

    for copy in sends:
        copy.wait_send()
    assert len(sends) <= N_SEND and len(names) <= N_RECV, (len(sends), len(names))


def local(
    tokens, norm_gain, conv_in_weight, conv_gate_weight, conv_taps, query_weight, key_weight, value_weight,
    decay_down, decay_up, decay_bias, decay_extra, head_gain, conv_out_weight, value_out_weight,
):
    hbm = pl.BlockSpec(memory_space=pl.ANY)
    return pl.pallas_call(
        kernel,
        out_shape=pltpu.VMEM((ROWS, WIDTH), BF16),
        in_specs=[hbm] * 15,
        out_specs=pl.BlockSpec(memory_space=pltpu.VMEM),
        scratch_shapes=[
            pltpu.VMEM((ROWS, WIDTH), BF16),
            pltpu.VMEM((1, WIDTH), F32),
            pltpu.VMEM((3, WIDTH), F32),
            pltpu.VMEM((16, WIDTH), BF16),
            pltpu.VMEM((16, 1024), BF16),
            pltpu.VMEM((1, 1024), F32),
            pltpu.VMEM((1, LEN), F32),
            pltpu.VMEM((1, WIDTH), F32),
            pltpu.VMEM((2048, 384), BF16),
            pltpu.VMEM((2048, 640), BF16),
            pltpu.VMEM((2048, 512), BF16),
            pltpu.VMEM((LEN + 16, WIDTH), BF16),
            pltpu.VMEM((NY * 144, KEY_DIM), BF16),
            pltpu.VMEM((NY * 144, KEY_DIM), BF16),
            pltpu.VMEM((160, KEY_DIM), BF16),
            pltpu.VMEM((160, KEY_DIM), BF16),
            pltpu.VMEM((160, KEY_DIM), BF16),
            pltpu.VMEM((NZ * 80, KEY_DIM), BF16),
            pltpu.VMEM((NY * 128, KEY_DIM), BF16),
            pltpu.VMEM((VAL_DIM, KEY_DIM), BF16),
            pltpu.VMEM((VAL_DIM, KEY_DIM), BF16),
            pltpu.VMEM((32, 256), BF16),
            pltpu.VMEM((LEN + 16, 256), F32),
            pltpu.VMEM((16, 256), BF16),
            pltpu.VMEM((16, 256), BF16),
            pltpu.VMEM((LEN, 512), BF16),
            pltpu.VMEM((12 * ROWS, WIDTH // 4), F32),
            pltpu.VMEM((16 * ROWS, WIDTH // 4), BF16),
            pltpu.VMEM((16 * ROWS, WIDTH // 4), BF16),
            pltpu.VMEM((16 * ROWS, WIDTH // 4), BF16),
            pltpu.VMEM((8 * ROWS, WIDTH // 8), BF16),
            pltpu.VMEM((8 * ROWS, WIDTH // 8), BF16),
            pltpu.VMEM((8 * ROWS, WIDTH // 4), BF16),
            pltpu.SemaphoreType.DMA((N_SEND,)),
            pltpu.SemaphoreType.DMA((N_RECV,)),
            pltpu.SemaphoreType.DMA((15,)),
        ],
        compiler_params=pltpu.CompilerParams(collective_id=0, has_side_effects=True, vmem_limit_bytes=60 * 1024 * 1024),
        cost_estimate=pl.CostEstimate(flops=3_000_000_000, bytes_accessed=1_000_000, transcendentals=0),
    )(
        tokens, norm_gain.reshape(1, -1), conv_in_weight, conv_gate_weight, conv_taps, query_weight, key_weight,
        value_weight, decay_down.T, decay_up, decay_bias.reshape(1, -1), decay_extra, head_gain.reshape(1, -1),
        conv_out_weight.T, value_out_weight.T,
    )


def solution(mesh):
    torus = Mesh(mesh.devices.reshape(NZ, NY, NX, NC), SP_TP)
    return jax.shard_map(
        local,
        mesh=torus,
        in_specs=(
            P(SP_TP, None), P(), P(SP, TP), P(SP, TP), P(), P(SP, TP), P(SP, TP), P(SP, TP),
            P(), P(), P(), P(TP, SP), P(), P(TP, SP), P(TP, SP),
        ),
        out_specs=P(SP_TP, None),
        check_vma=False,
    )
```

```python
import functools
import math

import jax
import jax.numpy as jnp
from jax import lax
from jax.experimental import pallas as pl
from jax.experimental.pallas import tpu as pltpu
from jax.sharding import Mesh
from jax.sharding import PartitionSpec as P

NZ, NY, NX, NC = 16, 4, 4, 2
KEY_DIM = 128
VAL_DIM = 256
BLOCK = 64
ROWS = 48
LEN = 384
WIDTH = 2048
EPSILON = 1e-06
SP = ("z", "y")
TP = ("x", "c")
SP_TP = ("z", "y", "x", "c")
F32 = jnp.float32
BF16 = jnp.bfloat16
MESH = pl.DeviceIdType.MESH
N_SEND = 256
N_RECV = 256


def mm(a, b):
    return lax.dot_general(a, b, (((1,), (0,)), ((), ())), preferred_element_type=F32)


def mm_nt(a, b):
    return lax.dot_general(a, b, (((1,), (1,)), ((), ())), preferred_element_type=F32)


def mm_tn(a, b):
    return lax.dot_general(a, b, (((0,), (0,)), ((), ())), preferred_element_type=F32)


def wrap(value, size):
    return lax.rem(value + size, size)


def split3(row):
    hi = row.astype(BF16)
    rest = row - hi.astype(F32)
    mid = rest.astype(BF16)
    low = (rest - mid.astype(F32)).astype(BF16)
    return hi, mid, low


def log_rows(row):
    hi, mid, low = split3(row)
    index = lax.broadcasted_iota(jnp.int32, (16, KEY_DIM), 0)
    spread = [jnp.broadcast_to(p.astype(F32), (16, KEY_DIM)) for p in (hi, mid, low)]
    out = jnp.where(index == 0, spread[0], jnp.where(index == 1, spread[1], jnp.where(index == 2, spread[2], 0.0)))
    return out.astype(BF16)


def log_total(rows16):
    return jnp.sum(rows16.astype(F32), axis=0, keepdims=True)


def kernel(
    tok_h, gain_h, ci_h, cg_h, taps_h, q_h, k_h, v_h, dd_h, du_h, db_h, de_h, hg_h, co_h, vo_h,
    out,
    tok, norm_gain, taps, ddown, dup, dbias, dextra, hgain,
    WA, WB, WC, T, SS, R1, M2, NEAR, M4, R2, M3, IF, IB, CI, CP, HP, HN, XC, PO, PS, PR, XS, XQ, XP, XR,
    ssem, rsem, lsem,
):
    z, y, x, c = (lax.axis_index(a) for a in SP_TP)
    tp = x * 2 + c
    s = z * 4 + y
    other = 1 - c
    names = {}
    sends = []

    def at(dz=0, dy=0, dx=0, flip=False):
        return (wrap(z + dz, NZ), wrap(y + dy, NY), wrap(x + dx, NX), other if flip else c)

    def sem(name):
        return rsem.at[names.setdefault(name, len(names))]

    def send(src, dst, name, device):
        copy = pltpu.make_async_remote_copy(
            src_ref=src, dst_ref=dst, send_sem=ssem.at[len(sends)], recv_sem=sem(name),
            device_id=device, device_id_type=MESH,
        )
        copy.start()
        sends.append(copy)

    def arrived(dst, name):
        pltpu.make_async_remote_copy(
            src_ref=dst, dst_ref=dst, send_sem=ssem.at[0], recv_sem=sem(name),
            device_id=(z, y, x, c), device_id_type=MESH,
        ).wait_recv()

    after = lax.rem(s + 1, NZ * NY)
    ahead = lax.rem(s + NZ * NY - 1, NZ * NY)
    next_dev = (after // NY, lax.rem(after, NY), x, c)
    prev_dev = (ahead // NY, lax.rem(ahead, NY), x, c)
    peers = [at(dz=d) for d in (1, -1, 2, -2)]
    peers += [at(dy=d) for d in range(1, NY)]
    peers += [at(dx=d) for d in range(1, NX)]
    peers += [at(flip=True), next_dev, prev_dev]
    def slot(dz=0, dy=0):
        index = wrap(z + dz, NZ) * NY + wrap(y + dy, NY)
        return pl.ds(pl.multiple_of(index * 32, 32), 32)

    def plane(dz=0):
        return pl.ds(pl.multiple_of(wrap(z + dz, NZ) * 128, 128), 128)

    def token_rows(dx=0, flip=False):
        index = wrap(x + dx, NX) * 2 + (other if flip else c)
        return pl.ds(pl.multiple_of(index * ROWS, 16), ROWS)

    loads = []

    def load(src, dst):
        copy = pltpu.make_async_copy(src, dst, lsem.at[len(loads)])
        copy.start()
        loads.append(copy)

    load(k_h, WA.at[slot(), pl.ds(0, 128)])
    load(v_h, WA.at[slot(), pl.ds(128, 256)])
    load(tok_h, tok)
    load(gain_h, norm_gain)
    barrier = pltpu.get_barrier_semaphore()
    for peer in peers:
        pl.semaphore_signal(barrier, inc=1, device_id=peer, device_id_type=MESH)
    load(q_h, WB.at[slot(), pl.ds(0, 128)])
    load(ci_h, WB.at[slot(), pl.ds(128, 256)])
    load(cg_h, WB.at[slot(), pl.ds(384, 256)])
    load(co_h, WC.at[slot(), pl.ds(0, 256)])
    load(vo_h, WC.at[slot(), pl.ds(256, 256)])
    load(dd_h, ddown)
    load(du_h, dup)
    load(db_h, dbias)
    load(de_h, dextra)
    load(taps_h, taps)
    load(hg_h, hgain)
    for copy in loads[:2]:
        copy.wait()
    pl.semaphore_wait(barrier, len(peers))

    def place(j):
        return 0 if j == 0 else (-j if j <= 8 else j - 8)

    class Ring:
        def __init__(self, W, tag):
            self.W, self.tag = W, tag

        def hop(self, chain, sign, k):
            ref = self.W.at[slot(-sign * (k - 1), 2 * chain)]
            send(ref, ref, (self.tag, chain, sign, k), at(dz=sign))

        def fan_out(self, j):
            ref = self.W.at[slot(place(j))]
            send(ref, ref, (self.tag, "ym", j), at(dy=1))
            send(ref, ref, (self.tag, "yp", j), at(dy=-1))

        def across(self):
            ref = self.W.at[slot()]
            send(ref, ref, (self.tag, "y2"), at(dy=2))

        def around(self, chain):
            if chain:
                arrived(self.W.at[slot(0, 2)], (self.tag, "y2"))
            self.hop(chain, 1, 1)
            self.hop(chain, -1, 1)

        def step(self, k, chains=(0, 1), fan=True):
            for chain in chains:
                for sign in (1, -1):
                    most = 8 if (sign == 1) == (chain == 0) else 7
                    if k > most:
                        continue
                    arrived(self.W.at[slot(-sign * k, 2 * chain)], (self.tag, chain, sign, k))
                    if k < most:
                        self.hop(chain, sign, k + 1)
                    if chain == 0 and fan:
                        self.fan_out(k if sign == 1 else 8 + k)

        def column(self, *js):
            for j in js:
                plus = (j % 2 == 0 and j < 8) if j <= 8 else ((j - 8) % 2 == 1)
                for dy, name in ((-1, "ym"), (1, "yp")):
                    ref = self.W.at[slot(place(j), dy)]
                    arrived(ref, (self.tag, name, j))
                    if plus == (dy == -1):
                        send(ref, ref, (self.tag, "y2", j), at(dy=-dy))

        def last_column(self):
            for j in range(16):
                arrived(self.W.at[slot(place(j), 2)], (self.tag, "y2", j))

        def finish(self):
            for j in range(16):
                arrived(self.W.at[slot(place(j), -1)], (self.tag, "ym", j))
                arrived(self.W.at[slot(place(j), 1)], (self.tag, "yp", j))

    class Jumps(Ring):
        def leap(self, sign, base):
            ref = self.W.at[slot(-sign * base)]
            for d in (2, 1):
                if base + d <= (8 if sign == 1 else 7):
                    send(ref, ref, (self.tag, 0, sign, base + d), at(dz=sign * d))

        def stage(self, i):
            for d in (2, 1):
                for sign in (1, -1):
                    k = 2 * i - 2 + d
                    if k > (8 if sign == 1 else 7):
                        continue
                    arrived(self.W.at[slot(-sign * k)], (self.tag, 0, sign, k))
                    if d == 2:
                        self.leap(sign, k)
                    self.fan_out(k if sign == 1 else 8 + k)

    ring_a, ring_b, ring_c = Jumps(WA, "a"), Ring(WB, "b"), Ring(WC, "c")
    ring_a.leap(1, 0)
    ring_a.leap(-1, 0)
    ring_a.fan_out(0)
    for copy in loads[2:]:
        copy.wait()
    raw_rows = tok[...].astype(F32)
    scale = lax.rsqrt(jnp.mean(raw_rows * raw_rows, axis=-1, keepdims=True) + EPSILON)
    T[token_rows(), :] = (raw_rows * scale * norm_gain[...]).astype(BF16)
    own_rows = T.at[token_rows()]
    send(own_rows, own_rows, "tm", at(dx=1))
    send(own_rows, own_rows, "tp", at(dx=-1))
    send(own_rows, own_rows, ("tc", 0), at(flip=True))
    ring_b.across()
    ring_b.around(0)
    ring_c.across()
    ring_c.around(0)
    ring_b.fan_out(0)

    def weights_step(k, fan=True):
        if k <= 8:
            ring_b.step(k, (0,))
            ring_c.step(k, (0,), fan=fan)
        if k == 1:
            ring_b.around(1)
            ring_c.around(1)
        else:
            ring_b.step(k - 1, (1,))
            ring_c.step(k - 1, (1,))

    def late_fan(*js):
        for j in js:
            ring_c.fan_out(j)

    half = WIDTH // 2
    blocks = LEN // BLOCK
    key_cols = pl.ds(pl.multiple_of(tp * KEY_DIM, KEY_DIM), KEY_DIM)
    val_cols = pl.ds(pl.multiple_of(tp * VAL_DIM, VAL_DIM), VAL_DIM)

    def token_step(stage):
        if stage == 0:
            ref = T.at[token_rows(dx=-1)]
            arrived(ref, "tm")
            piece = T.at[token_rows(dx=-1), pl.ds(0, half)]
            send(piece, piece, "t2a", at(dx=1))
            send(ref, ref, ("tc", 1), at(flip=True))
            ref = T.at[token_rows(dx=1)]
            arrived(ref, "tp")
            piece = T.at[token_rows(dx=1), pl.ds(half, half)]
            send(piece, piece, "t2b", at(dx=-1))
            send(ref, ref, ("tc", 2), at(flip=True))
        elif stage == 1:
            arrived(T.at[token_rows(dx=2), pl.ds(0, half)], "t2a")
            arrived(T.at[token_rows(dx=2), pl.ds(half, half)], "t2b")
            ref = T.at[token_rows(dx=2)]
            send(ref, ref, ("tc", 3), at(flip=True))
        else:
            for j in range(4):
                arrived(T.at[token_rows(dx=(0, -1, 1, 2)[j], flip=True)], ("tc", j))

    def part(array, n):
        return array[n * BLOCK : (n + 1) * BLOCK]

    def decay():
        low = mm_nt(T[0:LEN, :], ddown[...]).astype(BF16)
        pre = mm(low, dup[:, key_cols]) + dbias[:, key_cols]
        log_sig = jnp.minimum(pre, 0.0) - jnp.log1p(jnp.exp(-jnp.abs(pre)))
        extra = jnp.transpose(jnp.broadcast_to(dextra[...], (KEY_DIM, LEN)))
        log_decay = log_sig / 16.0 + extra
        ri = lax.broadcasted_iota(jnp.int32, (LEN, LEN), 0)
        ci = lax.broadcasted_iota(jnp.int32, (LEN, LEN), 1)
        tri = jnp.where((ri >= ci) & (ri // BLOCK == ci // BLOCK), 1.0, 0.0).astype(F32)
        cumul = lax.dot_general(
            tri, log_decay, (((1,), (0,)), ((), ())), precision=lax.Precision.HIGHEST, preferred_element_type=F32
        )
        return cumul, cumul - log_decay

    ring_a.stage(1)
    ring_a.column(0)
    weights_step(1, fan=False)
    token_step(0)
    ring_a.stage(2)
    ring_a.column(1, 9)
    weights_step(2, fan=False)
    ring_a.column(2, 10)
    ring_a.stage(3)
    ring_a.column(3, 11)
    token_step(1)
    weights_step(3, fan=False)
    ring_a.column(4, 12)
    ring_a.stage(4)
    ring_a.column(5, 13)
    token_step(2)
    for name, device, edge, at_row in (("hp", next_dev, LEN - 16, 15), ("hn", prev_dev, 0, 0)):
        rows = T[edge : edge + 16, :].astype(F32)[at_row : at_row + 1]
        arow = lax.broadcasted_iota(jnp.int32, (16, 256), 0)
        spread = jnp.zeros((16, 256), F32)
        for i in range(8):
            spread = jnp.where(arow == i, rows[:, i * 256 : (i + 1) * 256], spread)
        to = pl.ds(16 if at_row == 0 else 0, 16)
        CI[to, :] = spread.astype(BF16)
        send(CI.at[to], HN if at_row == 0 else HP, name, device)
    cumul, before = decay()
    totals = [cumul[(n + 1) * BLOCK - 1 : (n + 1) * BLOCK] for n in range(blocks)]
    offsets = [jnp.zeros((1, KEY_DIM), F32)]
    for n in range(blocks):
        offsets.append(offsets[-1] + totals[n])
    whole = offsets[blocks]
    suffix = [jnp.zeros((1, KEY_DIM), F32)]
    for n in reversed(range(blocks)):
        suffix.append(suffix[-1] + totals[n])
    suffix = suffix[::-1][1:]
    to_end = jnp.concatenate([suffix[n] + totals[n] - part(cumul, n) for n in range(blocks)], axis=0)
    from_start = jnp.concatenate([offsets[n] + part(before, n) for n in range(blocks)], axis=0)
    to_end, from_start = jnp.exp(to_end), jnp.exp(from_start)
    marks = log_rows(whole)
    weights_step(4, fan=False)
    ring_a.column(6, 14)
    ring_a.column(7, 15, 8)
    weights_step(5, fan=False)
    ring_a.last_column()

    normed = T[0:LEN, :]
    kv = mm(normed, WA[...])
    key_f = kv[:, :KEY_DIM].astype(BF16).astype(F32)
    value = kv[:, KEY_DIM:].astype(BF16)
    fwd_device = mm_tn(value, (key_f * to_end).astype(BF16))
    back_device = mm_tn(value, (key_f * from_start).astype(BF16))

    for q in range(NY):
        SS[q * 144 : q * 144 + 64, :] = fwd_device[q * 64 : q * 64 + 64].astype(BF16)
        SS[q * 144 + 64 : q * 144 + 128, :] = back_device[q * 64 : q * 64 + 64].astype(BF16)
        SS[q * 144 + 128 : q * 144 + 144, :] = marks

    def message(dy=0):
        return pl.ds(pl.multiple_of(wrap(y + dy, NY) * 144, 16), 144)

    R1[message(), :] = SS[message(), :]
    for d in range(1, NY):
        send(SS.at[message(d)], R1.at[message()], ("s1", d), at(dy=d))

    late_fan(0, 1, 9)
    weights_step(6)
    for d in range(1, NY):
        arrived(R1.at[message(-d)], ("s1", d))
    in_f, in_b, in_l = [], [], []
    for q in range(NY):
        in_f.append(R1[q * 144 : q * 144 + 64, :].astype(F32))
        in_b.append(R1[q * 144 + 64 : q * 144 + 128, :].astype(F32))
        in_l.append(log_total(R1[q * 144 + 128 : q * 144 + 144, :]))
    total_f = jnp.zeros((64, KEY_DIM), F32)
    total_b = jnp.zeros((64, KEY_DIM), F32)
    log_f = jnp.zeros((1, KEY_DIM), F32)
    log_b = jnp.zeros((1, KEY_DIM), F32)
    plane_f, plane_b, gap_f, gap_b = ([None] * NY for _ in range(4))
    for q in range(NY):
        plane_f[q], gap_f[q] = total_f, log_f
        total_f = jnp.exp(in_l[q]) * total_f + in_f[q]
        log_f = log_f + in_l[q]
    for q in reversed(range(NY)):
        plane_b[q], gap_b[q] = total_b, log_b
        total_b = jnp.exp(in_l[q]) * total_b + in_b[q]
        log_b = log_b + in_l[q]
    marks = log_rows(log_f)
    M2[0:64, :] = total_f.astype(BF16)
    M2[64:80, :] = marks
    M2[80:144, :] = total_b.astype(BF16)
    M2[144:160, :] = marks

    def depth(dz=0):
        return pl.ds(pl.multiple_of(wrap(z + dz, NZ) * 80, 16), 80)

    R2[depth(), :] = M2[0:80, :]
    send(M2.at[pl.ds(0, 80)], NEAR.at[pl.ds(0, 80)], "s2f", at(dz=1))
    send(M2.at[pl.ds(80, 80)], NEAR.at[pl.ds(80, 80)], "s2b", at(dz=-1))
    late_fan(2, 10)
    weights_step(7)
    arrived(NEAR.at[pl.ds(0, 80)], "s2f")
    arrived(NEAR.at[pl.ds(80, 80)], "s2b")
    near_f = jnp.where(z > 0, NEAR[0:64, :].astype(F32), 0.0)
    near_b = jnp.where(z < NZ - 1, NEAR[80:144, :].astype(F32), 0.0)
    near_lf, near_lb = log_total(NEAR[64:80, :]), log_total(NEAR[144:160, :])
    fade = jnp.exp(log_f)
    M4[0:64, :] = (total_f + fade * near_f).astype(BF16)
    M4[64:80, :] = log_rows(log_f + near_lf)
    M4[80:144, :] = (total_b + fade * near_b).astype(BF16)
    M4[144:160, :] = log_rows(log_f + near_lb)
    for d in (8, 6, 10, 4, 12, 2, 14):
        start = pl.multiple_of(((z + d) // NZ) * 80, 16)
        send(M4.at[pl.ds(start, 80)], R2.at[depth()], ("s2", d), at(dz=d))

    late_fan(3, 11)
    weights_step(8)
    late_fan(4, 12)
    weights_step(9)
    late_fan(5, 13)
    for d in range(2, NZ, 2):
        arrived(R2.at[depth(-d)], ("s2", d))
    sum_f = jnp.zeros((64, KEY_DIM), F32)
    sum_b = jnp.zeros((64, KEY_DIM), F32)
    for d in range(NZ - 2, 0, -2):
        got = R2[depth(-d), :]
        step = jnp.exp(log_total(got[64:80])) * sum_f + got[0:64].astype(F32)
        sum_f = jnp.where(z >= d, step, sum_f)
        got = R2[depth(d), :]
        step = jnp.exp(log_total(got[64:80])) * sum_b + got[0:64].astype(F32)
        sum_b = jnp.where(z + d < NZ, step, sum_b)
    sum_f = jnp.where(z > 0, jnp.exp(near_lf) * sum_f + near_f, 0.0)
    sum_b = jnp.where(z < NZ - 1, jnp.exp(near_lb) * sum_b + near_b, 0.0)
    for q in range(NY):
        M3[q * 128 : q * 128 + 64, :] = (plane_f[q] + jnp.exp(gap_f[q]) * sum_f).astype(BF16)
        M3[q * 128 + 64 : q * 128 + 128, :] = (plane_b[q] + jnp.exp(gap_b[q]) * sum_b).astype(BF16)

    def quarter(dy=0):
        return pl.ds(pl.multiple_of(wrap(y + dy, NY) * 64, 64), 64)

    def answer(dy, which):
        return pl.ds(pl.multiple_of(wrap(y + dy, NY) * 128 + 64 * which, 64), 64)

    for d in range(1, NY):
        send(M3.at[answer(d, 0)], IF.at[quarter()], ("s3f", d), at(dy=d))
        send(M3.at[answer(d, 1)], IB.at[quarter()], ("s3b", d), at(dy=d))
    IF[quarter(), :] = M3[answer(0, 0), :]
    IB[quarter(), :] = M3[answer(0, 1), :]
    ring_b.finish()
    arrived(HP, "hp")
    arrived(HN, "hn")
    for i in range(8):
        seg = pl.ds(i * 256, 256)
        arow = lax.broadcasted_iota(jnp.int32, (16, 256), 0)
        row_p = jnp.where(s > 0, HP[i : i + 1, :].astype(F32), 0.0)
        row_n = jnp.where(s < NZ * NY - 1, HN[i : i + 1, :].astype(F32), 0.0)
        T[pl.ds(LEN, 16), seg] = jnp.where(arow == 0, row_p, jnp.where(arow == 1, row_n, 0.0)).astype(BF16)
    conv_in = mm(T[...], WB[:, 128:384]).astype(BF16).astype(F32)
    CP[8 : 8 + LEN, :] = conv_in[:LEN]
    CP[7:8, :] = conv_in[LEN : LEN + 1]
    CP[8 + LEN : 9 + LEN, :] = conv_in[LEN + 1 : LEN + 2]
    query_f = (mm(normed, WB[:, 0:128]) * (1.0 / math.sqrt(KEY_DIM))).astype(BF16).astype(F32)
    gate = mm(normed, WB[:, 384:640]).astype(BF16).astype(F32)
    lower = lax.broadcasted_iota(jnp.int32, (BLOCK, BLOCK), 0) >= lax.broadcasted_iota(jnp.int32, (BLOCK, BLOCK), 1)
    upper = lax.broadcasted_iota(jnp.int32, (BLOCK, BLOCK), 0) <= lax.broadcasted_iota(jnp.int32, (BLOCK, BLOCK), 1)
    within = []
    fwd_inc, back_inc, fwd_query, back_query = [], [], [], []
    for n in range(blocks):
        cum_n, bef_n, key_n, query_n, value_n = (part(a, n) for a in (cumul, before, key_f, query_f, value))
        fq = (query_n * jnp.exp(cum_n)).astype(BF16)
        ks = (key_n * jnp.exp(bef_n)).astype(BF16)
        fwd_scores = mm_nt(fq, (key_n * jnp.exp(-cum_n)).astype(BF16))
        back_scores = mm_nt((query_n * jnp.exp(-bef_n)).astype(BF16), ks)
        scores = jnp.where(lower, fwd_scores, 0.0) + jnp.where(upper, back_scores, 0.0)
        within.append(mm(scores.astype(BF16), value_n))
        fwd_inc.append(mm_tn(value_n, (key_n * jnp.exp(totals[n] - cum_n)).astype(BF16)))
        back_inc.append(mm_tn(value_n, ks))
        fwd_query.append(fq)
        back_query.append((query_n * jnp.exp(totals[n] - bef_n)).astype(BF16))
    state = fwd_inc[0]
    for n in range(1, blocks):
        within[n] = within[n] + mm_nt(fwd_query[n], state.astype(BF16))
        state = jnp.exp(totals[n]) * state + fwd_inc[n]
    state = back_inc[blocks - 1]
    for n in reversed(range(blocks - 1)):
        within[n] = within[n] + mm_nt(back_query[n], state.astype(BF16))
        state = jnp.exp(totals[n]) * state + back_inc[n]
    local = jnp.concatenate(within, axis=0)
    far_fwd = jnp.concatenate(
        [part(query_f, n) * jnp.exp(offsets[n] + part(cumul, n)) for n in range(blocks)], axis=0
    ).astype(BF16)
    far_back = jnp.concatenate(
        [part(query_f, n) * jnp.exp(suffix[n] + (totals[n] - part(before, n))) for n in range(blocks)], axis=0
    ).astype(BF16)

    tap = taps[:, val_cols]
    mixed = CP[7 : 7 + LEN, :] * tap[0:1] + CP[8 : 8 + LEN, :] * tap[1:2] + CP[9 : 9 + LEN, :] * tap[2:3]
    XC[:, 0:256] = (mixed * (gate * (1.0 / (1.0 + jnp.exp(-gate))))).astype(BF16)

    early = len(sends) - 6
    for copy in sends[:early]:
        copy.wait_send()
    for d in range(1, NY):
        arrived(IF.at[quarter(-d)], ("s3f", d))
        arrived(IB.at[quarter(-d)], ("s3b", d))
    raw = local + mm_nt(far_fwd, IF[...]) + mm_nt(far_back, IB[...])
    norm = lax.rsqrt(jnp.mean(raw * raw, axis=-1, keepdims=True) + EPSILON)
    XC[:, 256:512] = (raw * norm * hgain[:, val_cols]).astype(BF16)
    ring_c.finish()

    order = (2, 1, 3, 0)
    pieces, piece = 4, WIDTH // 4
    there = jnp.concatenate([XC[token_rows(dx=r, flip=True), :] for r in order], axis=0)
    here = jnp.concatenate([XC[token_rows(dx=r), :] for r in order], axis=0)

    def rows4(n, i=0, count=4):
        return pl.ds((n * 4 + i) * ROWS, count * ROWS)

    def pair_send(n):
        PS[rows4(n), :] = mm_nt(there, WC[n * piece : (n + 1) * piece, :]).astype(BF16)
        send(PS.at[rows4(n)], PR.at[rows4(n)], ("pr", n), at(flip=True))

    side = piece // 2
    near, far_side = pl.ds(0, side), pl.ds(side, side)

    def keep(n):
        PO[rows4(n), :] = mm_nt(here, WC[n * piece : (n + 1) * piece, :])

    def x_send(n):
        arrived(PR.at[rows4(n)], ("pr", n))
        both = PO[rows4(n), :] + PR[rows4(n), :].astype(F32)
        XS[rows4(n), :] = both.astype(BF16)
        send(XS.at[rows4(n, 0, 1), near], XQ.at[rows2(n, 0)], ("xq", n, 0), at(dx=1))
        send(XS.at[rows4(n, 0, 1), far_side], XQ.at[rows2(n, 1)], ("xq", n, 1), at(dx=-1))
        PO[rows4(n, 1, 3), :] = both[ROWS:]

    def x_direct(n):
        send(XS.at[rows4(n, 1, 1), far_side], XR.at[rows2(n, 0), far_side], ("xr", n, 0), at(dx=1))
        send(XS.at[rows4(n, 2, 1), near], XR.at[rows2(n, 1), near], ("xr", n, 1), at(dx=-1))

    def rows2(n, i):
        return pl.ds((n * 2 + i) * ROWS, ROWS)

    def x_pass(n):
        base = (n * 4 + 1) * ROWS
        arrived(XQ.at[rows2(n, 0)], ("xq", n, 0))
        XP[rows2(n, 0), :] = (PO[base : base + ROWS, 0:side] + XQ[rows2(n, 0), :].astype(F32)).astype(BF16)
        send(XP.at[rows2(n, 0)], XR.at[rows2(n, 0), near], ("xs", n, 0), at(dx=1))
        arrived(XQ.at[rows2(n, 1)], ("xq", n, 1))
        XP[rows2(n, 1), :] = (PO[base + ROWS : base + 2 * ROWS, side:] + XQ[rows2(n, 1), :].astype(F32)).astype(BF16)
        send(XP.at[rows2(n, 1)], XR.at[rows2(n, 1), far_side], ("xs", n, 1), at(dx=-1))

    for n in range(pieces):
        pair_send(n)
    for n in range(pieces):
        keep(n)
    for n in range(pieces):
        x_send(n)
    for n in range(pieces):
        x_direct(n)
    for n in range(pieces):
        x_pass(n)
    for n in range(pieces):
        total = PO[rows4(n, 3, 1), :]
        arrived(XR.at[rows2(n, 0), far_side], ("xr", n, 0))
        arrived(XR.at[rows2(n, 1), near], ("xr", n, 1))
        arrived(XR.at[rows2(n, 0), near], ("xs", n, 0))
        arrived(XR.at[rows2(n, 1), far_side], ("xs", n, 1))
        total = total + XR[rows2(n, 0), :].astype(F32) + XR[rows2(n, 1), :].astype(F32)
        out[:, n * piece : (n + 1) * piece] = total.astype(BF16)

    for copy in sends[early:]:
        copy.wait_send()
    assert len(sends) <= N_SEND and len(names) <= N_RECV, (len(sends), len(names))


def local(
    tokens, norm_gain, conv_in_weight, conv_gate_weight, conv_taps, query_weight, key_weight, value_weight,
    decay_down, decay_up, decay_bias, decay_extra, head_gain, conv_out_weight, value_out_weight,
):
    hbm = pl.BlockSpec(memory_space=pl.ANY)
    return pl.pallas_call(
        kernel,
        out_shape=pltpu.VMEM((ROWS, WIDTH), BF16),
        in_specs=[hbm] * 15,
        out_specs=pl.BlockSpec(memory_space=pltpu.VMEM),
        scratch_shapes=[
            pltpu.VMEM((ROWS, WIDTH), BF16),
            pltpu.VMEM((1, WIDTH), F32),
            pltpu.VMEM((3, WIDTH), F32),
            pltpu.VMEM((16, WIDTH), BF16),
            pltpu.VMEM((16, 1024), BF16),
            pltpu.VMEM((1, 1024), F32),
            pltpu.VMEM((1, LEN), F32),
            pltpu.VMEM((1, WIDTH), F32),
            pltpu.VMEM((2048, 384), BF16),
            pltpu.VMEM((2048, 640), BF16),
            pltpu.VMEM((2048, 512), BF16),
            pltpu.VMEM((LEN + 16, WIDTH), BF16),
            pltpu.VMEM((NY * 144, KEY_DIM), BF16),
            pltpu.VMEM((NY * 144, KEY_DIM), BF16),
            pltpu.VMEM((160, KEY_DIM), BF16),
            pltpu.VMEM((160, KEY_DIM), BF16),
            pltpu.VMEM((160, KEY_DIM), BF16),
            pltpu.VMEM((NZ * 80, KEY_DIM), BF16),
            pltpu.VMEM((NY * 128, KEY_DIM), BF16),
            pltpu.VMEM((VAL_DIM, KEY_DIM), BF16),
            pltpu.VMEM((VAL_DIM, KEY_DIM), BF16),
            pltpu.VMEM((32, 256), BF16),
            pltpu.VMEM((LEN + 16, 256), F32),
            pltpu.VMEM((16, 256), BF16),
            pltpu.VMEM((16, 256), BF16),
            pltpu.VMEM((LEN, 512), BF16),
            pltpu.VMEM((16 * ROWS, WIDTH // 4), F32),
            pltpu.VMEM((16 * ROWS, WIDTH // 4), BF16),
            pltpu.VMEM((16 * ROWS, WIDTH // 4), BF16),
            pltpu.VMEM((16 * ROWS, WIDTH // 4), BF16),
            pltpu.VMEM((8 * ROWS, WIDTH // 8), BF16),
            pltpu.VMEM((8 * ROWS, WIDTH // 8), BF16),
            pltpu.VMEM((8 * ROWS, WIDTH // 4), BF16),
            pltpu.SemaphoreType.DMA((N_SEND,)),
            pltpu.SemaphoreType.DMA((N_RECV,)),
            pltpu.SemaphoreType.DMA((15,)),
        ],
        compiler_params=pltpu.CompilerParams(collective_id=0, has_side_effects=True, vmem_limit_bytes=60 * 1024 * 1024),
        cost_estimate=pl.CostEstimate(flops=3_000_000_000, bytes_accessed=1_000_000, transcendentals=0),
    )(
        tokens, norm_gain.reshape(1, -1), conv_in_weight, conv_gate_weight, conv_taps, query_weight, key_weight,
        value_weight, decay_down.T, decay_up, decay_bias.reshape(1, -1), decay_extra, head_gain.reshape(1, -1),
        conv_out_weight.T, value_out_weight.T,
    )


def solution(mesh):
    torus = Mesh(mesh.devices.reshape(NZ, NY, NX, NC), SP_TP)
    return jax.shard_map(
        local,
        mesh=torus,
        in_specs=(
            P(SP_TP, None), P(), P(SP, TP), P(SP, TP), P(), P(SP, TP), P(SP, TP), P(SP, TP),
            P(), P(), P(), P(TP, SP), P(), P(TP, SP), P(TP, SP),
        ),
        out_specs=P(SP_TP, None),
        check_vma=False,
    )
```

```python
import functools
import math

import jax
import jax.numpy as jnp
from jax import lax
from jax.experimental import pallas as pl
from jax.experimental.pallas import tpu as pltpu
from jax.sharding import Mesh
from jax.sharding import PartitionSpec as P

NZ, NY, NX, NC = 16, 4, 4, 2
KEY_DIM = 128
VAL_DIM = 256
BLOCK = 64
ROWS = 48
LEN = 384
WIDTH = 2048
EPSILON = 1e-06
SP = ("z", "y")
TP = ("x", "c")
SP_TP = ("z", "y", "x", "c")
F32 = jnp.float32
BF16 = jnp.bfloat16
MESH = pl.DeviceIdType.MESH
N_SEND = 256
N_RECV = 256


def mm(a, b):
    return lax.dot_general(a, b, (((1,), (0,)), ((), ())), preferred_element_type=F32)


def mm_nt(a, b):
    return lax.dot_general(a, b, (((1,), (1,)), ((), ())), preferred_element_type=F32)


def mm_tn(a, b):
    return lax.dot_general(a, b, (((0,), (0,)), ((), ())), preferred_element_type=F32)


def wrap(value, size):
    return lax.rem(value + size, size)


def split3(row):
    hi = row.astype(BF16)
    rest = row - hi.astype(F32)
    mid = rest.astype(BF16)
    low = (rest - mid.astype(F32)).astype(BF16)
    return hi, mid, low


def log_rows(row):
    hi, mid, low = split3(row)
    index = lax.broadcasted_iota(jnp.int32, (16, KEY_DIM), 0)
    spread = [jnp.broadcast_to(p.astype(F32), (16, KEY_DIM)) for p in (hi, mid, low)]
    out = jnp.where(index == 0, spread[0], jnp.where(index == 1, spread[1], jnp.where(index == 2, spread[2], 0.0)))
    return out.astype(BF16)


def log_total(rows16):
    return jnp.sum(rows16.astype(F32), axis=0, keepdims=True)


def kernel(
    tok_h, gain_h, ci_h, cg_h, taps_h, q_h, k_h, v_h, dd_h, du_h, db_h, de_h, hg_h, co_h, vo_h,
    out,
    tok, norm_gain, taps, ddown, dup, dbias, dextra, hgain,
    WA, WB, WC, T, SS, R1, M2, NEAR, M4, R2, M3, IF, IB, CI, CP, HP, HN, XC, PO, PS, PR, XS, XQ, XP, XR,
    ssem, rsem, lsem,
):
    z, y, x, c = (lax.axis_index(a) for a in SP_TP)
    tp = x * 2 + c
    s = z * 4 + y
    other = 1 - c
    names = {}
    sends = []

    def at(dz=0, dy=0, dx=0, flip=False):
        return (wrap(z + dz, NZ), wrap(y + dy, NY), wrap(x + dx, NX), other if flip else c)

    def sem(name):
        return rsem.at[names.setdefault(name, len(names))]

    def send(src, dst, name, device):
        copy = pltpu.make_async_remote_copy(
            src_ref=src, dst_ref=dst, send_sem=ssem.at[len(sends)], recv_sem=sem(name),
            device_id=device, device_id_type=MESH,
        )
        copy.start()
        sends.append(copy)

    def arrived(dst, name):
        pltpu.make_async_remote_copy(
            src_ref=dst, dst_ref=dst, send_sem=ssem.at[0], recv_sem=sem(name),
            device_id=(z, y, x, c), device_id_type=MESH,
        ).wait_recv()

    after = lax.rem(s + 1, NZ * NY)
    ahead = lax.rem(s + NZ * NY - 1, NZ * NY)
    next_dev = (after // NY, lax.rem(after, NY), x, c)
    prev_dev = (ahead // NY, lax.rem(ahead, NY), x, c)
    peers = [at(dz=d) for d in (1, -1, 2, -2)]
    peers += [at(dy=d) for d in range(1, NY)]
    peers += [at(dx=d) for d in range(1, NX)]
    peers += [at(flip=True), next_dev, prev_dev]
    def slot(dz=0, dy=0):
        index = wrap(z + dz, NZ) * NY + wrap(y + dy, NY)
        return pl.ds(pl.multiple_of(index * 32, 32), 32)

    def plane(dz=0):
        return pl.ds(pl.multiple_of(wrap(z + dz, NZ) * 128, 128), 128)

    def token_rows(dx=0, flip=False):
        index = wrap(x + dx, NX) * 2 + (other if flip else c)
        return pl.ds(pl.multiple_of(index * ROWS, 16), ROWS)

    loads = []

    def load(src, dst):
        copy = pltpu.make_async_copy(src, dst, lsem.at[len(loads)])
        copy.start()
        loads.append(copy)

    load(k_h, WA.at[slot(), pl.ds(0, 128)])
    load(v_h, WA.at[slot(), pl.ds(128, 256)])
    load(tok_h, tok)
    load(gain_h, norm_gain)
    barrier = pltpu.get_barrier_semaphore()
    for peer in peers:
        pl.semaphore_signal(barrier, inc=1, device_id=peer, device_id_type=MESH)
    load(q_h, WB.at[slot(), pl.ds(0, 128)])
    load(ci_h, WB.at[slot(), pl.ds(128, 256)])
    load(cg_h, WB.at[slot(), pl.ds(384, 256)])
    load(co_h, WC.at[slot(), pl.ds(0, 256)])
    load(vo_h, WC.at[slot(), pl.ds(256, 256)])
    load(dd_h, ddown)
    load(du_h, dup)
    load(db_h, dbias)
    load(de_h, dextra)
    load(taps_h, taps)
    load(hg_h, hgain)
    for copy in loads[:2]:
        copy.wait()
    pl.semaphore_wait(barrier, len(peers))

    def place(j):
        return 0 if j == 0 else (-j if j <= 8 else j - 8)

    class Ring:
        def __init__(self, W, tag, reach=8):
            self.W, self.tag, self.reach, self.passed = W, tag, reach, []

        def hop(self, chain, sign, k):
            ref = self.W.at[slot(-sign * (k - 1), 2 * chain)]
            send(ref, ref, (self.tag, chain, sign, k), at(dz=sign))

        def fan_out(self, j):
            ref = self.W.at[slot(place(j))]
            send(ref, ref, (self.tag, "ym", j), at(dy=1))
            send(ref, ref, (self.tag, "yp", j), at(dy=-1))

        def across(self):
            ref = self.W.at[slot()]
            send(ref, ref, (self.tag, "y2"), at(dy=2))

        def around(self, chain):
            if chain:
                arrived(self.W.at[slot(0, 2)], (self.tag, "y2"))
            self.hop(chain, 1, 1)
            self.hop(chain, -1, 1)

        def step(self, k, chains=(0, 1), fan=True):
            for chain in chains:
                for sign in (1, -1):
                    most = min(8 if (sign == 1) == (chain == 0) else 7, self.reach if chain else 8)
                    if k > most:
                        continue
                    arrived(self.W.at[slot(-sign * k, 2 * chain)], (self.tag, chain, sign, k))
                    if k < most:
                        self.hop(chain, sign, k + 1)
                    if chain == 0 and fan:
                        self.fan_out(k if sign == 1 else 8 + k)

        def column(self, *js):
            for j in js:
                self.passed.append(j)
                plus = (j % 2 == 0 and j < 8) if j <= 8 else ((j - 8) % 2 == 1)
                for dy, name in ((-1, "ym"), (1, "yp")):
                    ref = self.W.at[slot(place(j), dy)]
                    arrived(ref, (self.tag, name, j))
                    if plus == (dy == -1):
                        send(ref, ref, (self.tag, "y2", j), at(dy=-dy))

        def last_column(self):
            for j in range(16):
                arrived(self.W.at[slot(place(j), 2)], (self.tag, "y2", j))

        def finish(self):
            for j in range(16):
                if j in self.passed:
                    arrived(self.W.at[slot(place(j), 2)], (self.tag, "y2", j))
                else:
                    arrived(self.W.at[slot(place(j), -1)], (self.tag, "ym", j))
                    arrived(self.W.at[slot(place(j), 1)], (self.tag, "yp", j))

    class Jumps(Ring):
        def leap(self, sign, base):
            ref = self.W.at[slot(-sign * base)]
            for d in (2, 1):
                if base + d <= (8 if sign == 1 else 7):
                    send(ref, ref, (self.tag, 0, sign, base + d), at(dz=sign * d))

        def stage(self, i):
            for d in (2, 1):
                for sign in (1, -1):
                    k = 2 * i - 2 + d
                    if k > (8 if sign == 1 else 7):
                        continue
                    arrived(self.W.at[slot(-sign * k)], (self.tag, 0, sign, k))
                    if d == 2:
                        self.leap(sign, k)
                    self.fan_out(k if sign == 1 else 8 + k)

    ring_a, ring_b, ring_c = Jumps(WA, "a"), Ring(WB, "b"), Ring(WC, "c", reach=4)
    ring_a.leap(1, 0)
    ring_a.leap(-1, 0)
    ring_a.fan_out(0)
    for copy in loads[2:]:
        copy.wait()
    raw_rows = tok[...].astype(F32)
    scale = lax.rsqrt(jnp.mean(raw_rows * raw_rows, axis=-1, keepdims=True) + EPSILON)
    T[token_rows(), :] = (raw_rows * scale * norm_gain[...]).astype(BF16)
    own_rows = T.at[token_rows()]
    send(own_rows, own_rows, "tm", at(dx=1))
    send(own_rows, own_rows, "tp", at(dx=-1))
    send(own_rows, own_rows, ("tc", 0), at(flip=True))
    ring_b.across()
    ring_b.around(0)
    ring_c.across()
    ring_c.around(0)
    ring_b.fan_out(0)

    def weights_step(k, fan=True):
        if k <= 8:
            ring_b.step(k, (0,))
            ring_c.step(k, (0,), fan=fan)
        if k == 1:
            ring_b.around(1)
            ring_c.around(1)
        else:
            ring_b.step(k - 1, (1,))
            ring_c.step(k - 1, (1,))

    def late_fan(*js):
        for j in js:
            ring_c.fan_out(j)

    half = WIDTH // 2
    blocks = LEN // BLOCK
    key_cols = pl.ds(pl.multiple_of(tp * KEY_DIM, KEY_DIM), KEY_DIM)
    val_cols = pl.ds(pl.multiple_of(tp * VAL_DIM, VAL_DIM), VAL_DIM)

    def token_step(stage):
        if stage == 0:
            ref = T.at[token_rows(dx=-1)]
            arrived(ref, "tm")
            piece = T.at[token_rows(dx=-1), pl.ds(0, half)]
            send(piece, piece, "t2a", at(dx=1))
            send(ref, ref, ("tc", 1), at(flip=True))
            ref = T.at[token_rows(dx=1)]
            arrived(ref, "tp")
            piece = T.at[token_rows(dx=1), pl.ds(half, half)]
            send(piece, piece, "t2b", at(dx=-1))
            send(ref, ref, ("tc", 2), at(flip=True))
        elif stage == 1:
            arrived(T.at[token_rows(dx=2), pl.ds(0, half)], "t2a")
            arrived(T.at[token_rows(dx=2), pl.ds(half, half)], "t2b")
            ref = T.at[token_rows(dx=2)]
            send(ref, ref, ("tc", 3), at(flip=True))
        else:
            for j in range(4):
                arrived(T.at[token_rows(dx=(0, -1, 1, 2)[j], flip=True)], ("tc", j))

    def part(array, n):
        return array[n * BLOCK : (n + 1) * BLOCK]

    def decay():
        low = mm_nt(T[0:LEN, :], ddown[...]).astype(BF16)
        pre = mm(low, dup[:, key_cols]) + dbias[:, key_cols]
        log_sig = jnp.minimum(pre, 0.0) - jnp.log1p(jnp.exp(-jnp.abs(pre)))
        extra = jnp.transpose(jnp.broadcast_to(dextra[...], (KEY_DIM, LEN)))
        log_decay = log_sig / 16.0 + extra
        ri = lax.broadcasted_iota(jnp.int32, (LEN, LEN), 0)
        ci = lax.broadcasted_iota(jnp.int32, (LEN, LEN), 1)
        tri = jnp.where((ri >= ci) & (ri // BLOCK == ci // BLOCK), 1.0, 0.0).astype(F32)
        cumul = lax.dot_general(
            tri, log_decay, (((1,), (0,)), ((), ())), precision=lax.Precision.HIGHEST, preferred_element_type=F32
        )
        return cumul, cumul - log_decay

    ring_a.stage(1)
    ring_a.column(0)
    weights_step(1, fan=False)
    token_step(0)
    ring_a.stage(2)
    ring_a.column(1, 9)
    weights_step(2, fan=False)
    ring_a.column(2, 10)
    ring_a.stage(3)
    ring_a.column(3, 11)
    token_step(1)
    weights_step(3, fan=False)
    ring_a.column(4, 12)
    ring_a.stage(4)
    ring_a.column(5, 13)
    token_step(2)
    for name, device, edge, at_row in (("hp", next_dev, LEN - 16, 15), ("hn", prev_dev, 0, 0)):
        rows = T[edge : edge + 16, :].astype(F32)[at_row : at_row + 1]
        arow = lax.broadcasted_iota(jnp.int32, (16, 256), 0)
        spread = jnp.zeros((16, 256), F32)
        for i in range(8):
            spread = jnp.where(arow == i, rows[:, i * 256 : (i + 1) * 256], spread)
        to = pl.ds(16 if at_row == 0 else 0, 16)
        CI[to, :] = spread.astype(BF16)
        send(CI.at[to], HN if at_row == 0 else HP, name, device)
    cumul, before = decay()
    totals = [cumul[(n + 1) * BLOCK - 1 : (n + 1) * BLOCK] for n in range(blocks)]
    offsets = [jnp.zeros((1, KEY_DIM), F32)]
    for n in range(blocks):
        offsets.append(offsets[-1] + totals[n])
    whole = offsets[blocks]
    suffix = [jnp.zeros((1, KEY_DIM), F32)]
    for n in reversed(range(blocks)):
        suffix.append(suffix[-1] + totals[n])
    suffix = suffix[::-1][1:]
    to_end = jnp.concatenate([suffix[n] + totals[n] - part(cumul, n) for n in range(blocks)], axis=0)
    from_start = jnp.concatenate([offsets[n] + part(before, n) for n in range(blocks)], axis=0)
    to_end, from_start = jnp.exp(to_end), jnp.exp(from_start)
    marks = log_rows(whole)
    weights_step(4, fan=False)
    ring_a.column(6, 14)
    ring_a.column(7, 15, 8)
    weights_step(5, fan=False)
    ring_a.last_column()

    normed = T[0:LEN, :]
    kv = mm(normed, WA[...])
    key_f = kv[:, :KEY_DIM].astype(BF16).astype(F32)
    value = kv[:, KEY_DIM:].astype(BF16)
    fwd_device = mm_tn(value, (key_f * to_end).astype(BF16))
    back_device = mm_tn(value, (key_f * from_start).astype(BF16))

    for q in range(NY):
        SS[q * 144 : q * 144 + 64, :] = fwd_device[q * 64 : q * 64 + 64].astype(BF16)
        SS[q * 144 + 64 : q * 144 + 128, :] = back_device[q * 64 : q * 64 + 64].astype(BF16)
        SS[q * 144 + 128 : q * 144 + 144, :] = marks

    def message(dy=0):
        return pl.ds(pl.multiple_of(wrap(y + dy, NY) * 144, 16), 144)

    R1[message(), :] = SS[message(), :]
    for d in range(1, NY):
        send(SS.at[message(d)], R1.at[message()], ("s1", d), at(dy=d))

    late_fan(5, 13, 0)
    weights_step(6)
    for d in range(1, NY):
        arrived(R1.at[message(-d)], ("s1", d))
    in_f, in_b, in_l = [], [], []
    for q in range(NY):
        in_f.append(R1[q * 144 : q * 144 + 64, :].astype(F32))
        in_b.append(R1[q * 144 + 64 : q * 144 + 128, :].astype(F32))
        in_l.append(log_total(R1[q * 144 + 128 : q * 144 + 144, :]))
    total_f = jnp.zeros((64, KEY_DIM), F32)
    total_b = jnp.zeros((64, KEY_DIM), F32)
    log_f = jnp.zeros((1, KEY_DIM), F32)
    log_b = jnp.zeros((1, KEY_DIM), F32)
    plane_f, plane_b, gap_f, gap_b = ([None] * NY for _ in range(4))
    for q in range(NY):
        plane_f[q], gap_f[q] = total_f, log_f
        total_f = jnp.exp(in_l[q]) * total_f + in_f[q]
        log_f = log_f + in_l[q]
    for q in reversed(range(NY)):
        plane_b[q], gap_b[q] = total_b, log_b
        total_b = jnp.exp(in_l[q]) * total_b + in_b[q]
        log_b = log_b + in_l[q]
    marks = log_rows(log_f)
    M2[0:64, :] = total_f.astype(BF16)
    M2[64:80, :] = marks
    M2[80:144, :] = total_b.astype(BF16)
    M2[144:160, :] = marks

    def depth(dz=0):
        return pl.ds(pl.multiple_of(wrap(z + dz, NZ) * 80, 16), 80)

    R2[depth(), :] = M2[0:80, :]
    send(M2.at[pl.ds(0, 80)], NEAR.at[pl.ds(0, 80)], "s2f", at(dz=1))
    send(M2.at[pl.ds(80, 80)], NEAR.at[pl.ds(80, 80)], "s2b", at(dz=-1))
    late_fan(1, 9)
    weights_step(7)
    arrived(NEAR.at[pl.ds(0, 80)], "s2f")
    arrived(NEAR.at[pl.ds(80, 80)], "s2b")
    near_f = jnp.where(z > 0, NEAR[0:64, :].astype(F32), 0.0)
    near_b = jnp.where(z < NZ - 1, NEAR[80:144, :].astype(F32), 0.0)
    near_lf, near_lb = log_total(NEAR[64:80, :]), log_total(NEAR[144:160, :])
    fade = jnp.exp(log_f)
    M4[0:64, :] = (total_f + fade * near_f).astype(BF16)
    M4[64:80, :] = log_rows(log_f + near_lf)
    M4[80:144, :] = (total_b + fade * near_b).astype(BF16)
    M4[144:160, :] = log_rows(log_f + near_lb)
    for d in (8, 6, 10, 4, 12, 2, 14):
        start = pl.multiple_of(((z + d) // NZ) * 80, 16)
        send(M4.at[pl.ds(start, 80)], R2.at[depth()], ("s2", d), at(dz=d))

    late_fan(2, 10)
    weights_step(8)
    ring_c.column(5, 13)
    late_fan(3, 11)
    weights_step(9)
    ring_c.column(6, 14, 7, 15)
    late_fan(4, 12)
    for d in range(2, NZ, 2):
        arrived(R2.at[depth(-d)], ("s2", d))
    sum_f = jnp.zeros((64, KEY_DIM), F32)
    sum_b = jnp.zeros((64, KEY_DIM), F32)
    for d in range(NZ - 2, 0, -2):
        got = R2[depth(-d), :]
        step = jnp.exp(log_total(got[64:80])) * sum_f + got[0:64].astype(F32)
        sum_f = jnp.where(z >= d, step, sum_f)
        got = R2[depth(d), :]
        step = jnp.exp(log_total(got[64:80])) * sum_b + got[0:64].astype(F32)
        sum_b = jnp.where(z + d < NZ, step, sum_b)
    sum_f = jnp.where(z > 0, jnp.exp(near_lf) * sum_f + near_f, 0.0)
    sum_b = jnp.where(z < NZ - 1, jnp.exp(near_lb) * sum_b + near_b, 0.0)
    for q in range(NY):
        M3[q * 128 : q * 128 + 64, :] = (plane_f[q] + jnp.exp(gap_f[q]) * sum_f).astype(BF16)
        M3[q * 128 + 64 : q * 128 + 128, :] = (plane_b[q] + jnp.exp(gap_b[q]) * sum_b).astype(BF16)

    def quarter(dy=0):
        return pl.ds(pl.multiple_of(wrap(y + dy, NY) * 64, 64), 64)

    def answer(dy, which):
        return pl.ds(pl.multiple_of(wrap(y + dy, NY) * 128 + 64 * which, 64), 64)

    for d in range(1, NY):
        send(M3.at[answer(d, 0)], IF.at[quarter()], ("s3f", d), at(dy=d))
        send(M3.at[answer(d, 1)], IB.at[quarter()], ("s3b", d), at(dy=d))
    IF[quarter(), :] = M3[answer(0, 0), :]
    IB[quarter(), :] = M3[answer(0, 1), :]
    ring_c.column(8)
    ring_b.finish()
    arrived(HP, "hp")
    arrived(HN, "hn")
    for i in range(8):
        seg = pl.ds(i * 256, 256)
        arow = lax.broadcasted_iota(jnp.int32, (16, 256), 0)
        row_p = jnp.where(s > 0, HP[i : i + 1, :].astype(F32), 0.0)
        row_n = jnp.where(s < NZ * NY - 1, HN[i : i + 1, :].astype(F32), 0.0)
        T[pl.ds(LEN, 16), seg] = jnp.where(arow == 0, row_p, jnp.where(arow == 1, row_n, 0.0)).astype(BF16)
    conv_in = mm(T[...], WB[:, 128:384]).astype(BF16).astype(F32)
    CP[8 : 8 + LEN, :] = conv_in[:LEN]
    CP[7:8, :] = conv_in[LEN : LEN + 1]
    CP[8 + LEN : 9 + LEN, :] = conv_in[LEN + 1 : LEN + 2]
    query_f = (mm(normed, WB[:, 0:128]) * (1.0 / math.sqrt(KEY_DIM))).astype(BF16).astype(F32)
    gate = mm(normed, WB[:, 384:640]).astype(BF16).astype(F32)
    lower = lax.broadcasted_iota(jnp.int32, (BLOCK, BLOCK), 0) >= lax.broadcasted_iota(jnp.int32, (BLOCK, BLOCK), 1)
    upper = lax.broadcasted_iota(jnp.int32, (BLOCK, BLOCK), 0) <= lax.broadcasted_iota(jnp.int32, (BLOCK, BLOCK), 1)
    within = []
    fwd_inc, back_inc, fwd_query, back_query = [], [], [], []
    for n in range(blocks):
        cum_n, bef_n, key_n, query_n, value_n = (part(a, n) for a in (cumul, before, key_f, query_f, value))
        fq = (query_n * jnp.exp(cum_n)).astype(BF16)
        ks = (key_n * jnp.exp(bef_n)).astype(BF16)
        fwd_scores = mm_nt(fq, (key_n * jnp.exp(-cum_n)).astype(BF16))
        back_scores = mm_nt((query_n * jnp.exp(-bef_n)).astype(BF16), ks)
        scores = jnp.where(lower, fwd_scores, 0.0) + jnp.where(upper, back_scores, 0.0)
        within.append(mm(scores.astype(BF16), value_n))
        fwd_inc.append(mm_tn(value_n, (key_n * jnp.exp(totals[n] - cum_n)).astype(BF16)))
        back_inc.append(mm_tn(value_n, ks))
        fwd_query.append(fq)
        back_query.append((query_n * jnp.exp(totals[n] - bef_n)).astype(BF16))
    state = fwd_inc[0]
    for n in range(1, blocks):
        within[n] = within[n] + mm_nt(fwd_query[n], state.astype(BF16))
        state = jnp.exp(totals[n]) * state + fwd_inc[n]
    state = back_inc[blocks - 1]
    for n in reversed(range(blocks - 1)):
        within[n] = within[n] + mm_nt(back_query[n], state.astype(BF16))
        state = jnp.exp(totals[n]) * state + back_inc[n]
    local = jnp.concatenate(within, axis=0)
    far_fwd = jnp.concatenate(
        [part(query_f, n) * jnp.exp(offsets[n] + part(cumul, n)) for n in range(blocks)], axis=0
    ).astype(BF16)
    far_back = jnp.concatenate(
        [part(query_f, n) * jnp.exp(suffix[n] + (totals[n] - part(before, n))) for n in range(blocks)], axis=0
    ).astype(BF16)

    tap = taps[:, val_cols]
    mixed = CP[7 : 7 + LEN, :] * tap[0:1] + CP[8 : 8 + LEN, :] * tap[1:2] + CP[9 : 9 + LEN, :] * tap[2:3]
    XC[:, 0:256] = (mixed * (gate * (1.0 / (1.0 + jnp.exp(-gate))))).astype(BF16)

    early = len(sends) - 6
    for copy in sends[:early]:
        copy.wait_send()
    for d in range(1, NY):
        arrived(IF.at[quarter(-d)], ("s3f", d))
        arrived(IB.at[quarter(-d)], ("s3b", d))
    raw = local + mm_nt(far_fwd, IF[...]) + mm_nt(far_back, IB[...])
    norm = lax.rsqrt(jnp.mean(raw * raw, axis=-1, keepdims=True) + EPSILON)
    XC[:, 256:512] = (raw * norm * hgain[:, val_cols]).astype(BF16)
    ring_c.finish()

    order = (2, 1, 3, 0)
    pieces, piece = 4, WIDTH // 4
    there = jnp.concatenate([XC[token_rows(dx=r, flip=True), :] for r in order], axis=0)
    here = jnp.concatenate([XC[token_rows(dx=r), :] for r in order], axis=0)

    def rows4(n, i=0, count=4):
        return pl.ds((n * 4 + i) * ROWS, count * ROWS)

    def pair_send(n):
        PS[rows4(n), :] = mm_nt(there, WC[n * piece : (n + 1) * piece, :]).astype(BF16)
        send(PS.at[rows4(n)], PR.at[rows4(n)], ("pr", n), at(flip=True))

    side = piece // 2
    near, far_side = pl.ds(0, side), pl.ds(side, side)

    def keep(n):
        PO[rows4(n), :] = mm_nt(here, WC[n * piece : (n + 1) * piece, :])

    def x_send(n):
        arrived(PR.at[rows4(n)], ("pr", n))
        both = PO[rows4(n), :] + PR[rows4(n), :].astype(F32)
        XS[rows4(n), :] = both.astype(BF16)
        send(XS.at[rows4(n, 0, 1), near], XQ.at[rows2(n, 0)], ("xq", n, 0), at(dx=1))
        send(XS.at[rows4(n, 0, 1), far_side], XQ.at[rows2(n, 1)], ("xq", n, 1), at(dx=-1))
        PO[rows4(n, 1, 3), :] = both[ROWS:]

    def x_direct(n):
        send(XS.at[rows4(n, 1, 1), far_side], XR.at[rows2(n, 0), far_side], ("xr", n, 0), at(dx=1))
        send(XS.at[rows4(n, 2, 1), near], XR.at[rows2(n, 1), near], ("xr", n, 1), at(dx=-1))

    def rows2(n, i):
        return pl.ds((n * 2 + i) * ROWS, ROWS)

    def x_pass(n):
        base = (n * 4 + 1) * ROWS
        arrived(XQ.at[rows2(n, 0)], ("xq", n, 0))
        XP[rows2(n, 0), :] = (PO[base : base + ROWS, 0:side] + XQ[rows2(n, 0), :].astype(F32)).astype(BF16)
        send(XP.at[rows2(n, 0)], XR.at[rows2(n, 0), near], ("xs", n, 0), at(dx=1))
        arrived(XQ.at[rows2(n, 1)], ("xq", n, 1))
        XP[rows2(n, 1), :] = (PO[base + ROWS : base + 2 * ROWS, side:] + XQ[rows2(n, 1), :].astype(F32)).astype(BF16)
        send(XP.at[rows2(n, 1)], XR.at[rows2(n, 1), far_side], ("xs", n, 1), at(dx=-1))

    for n in range(pieces):
        pair_send(n)
    for n in range(pieces):
        keep(n)
    for n in range(pieces):
        x_send(n)
    for n in range(pieces):
        x_direct(n)
    for n in range(pieces):
        x_pass(n)
    for n in range(pieces):
        total = PO[rows4(n, 3, 1), :]
        arrived(XR.at[rows2(n, 0), far_side], ("xr", n, 0))
        arrived(XR.at[rows2(n, 1), near], ("xr", n, 1))
        arrived(XR.at[rows2(n, 0), near], ("xs", n, 0))
        arrived(XR.at[rows2(n, 1), far_side], ("xs", n, 1))
        total = total + XR[rows2(n, 0), :].astype(F32) + XR[rows2(n, 1), :].astype(F32)
        out[:, n * piece : (n + 1) * piece] = total.astype(BF16)

    for copy in sends[early:]:
        copy.wait_send()
    assert len(sends) <= N_SEND and len(names) <= N_RECV, (len(sends), len(names))


def local(
    tokens, norm_gain, conv_in_weight, conv_gate_weight, conv_taps, query_weight, key_weight, value_weight,
    decay_down, decay_up, decay_bias, decay_extra, head_gain, conv_out_weight, value_out_weight,
):
    hbm = pl.BlockSpec(memory_space=pl.ANY)
    return pl.pallas_call(
        kernel,
        out_shape=pltpu.VMEM((ROWS, WIDTH), BF16),
        in_specs=[hbm] * 15,
        out_specs=pl.BlockSpec(memory_space=pltpu.VMEM),
        scratch_shapes=[
            pltpu.VMEM((ROWS, WIDTH), BF16),
            pltpu.VMEM((1, WIDTH), F32),
            pltpu.VMEM((3, WIDTH), F32),
            pltpu.VMEM((16, WIDTH), BF16),
            pltpu.VMEM((16, 1024), BF16),
            pltpu.VMEM((1, 1024), F32),
            pltpu.VMEM((1, LEN), F32),
            pltpu.VMEM((1, WIDTH), F32),
            pltpu.VMEM((2048, 384), BF16),
            pltpu.VMEM((2048, 640), BF16),
            pltpu.VMEM((2048, 512), BF16),
            pltpu.VMEM((LEN + 16, WIDTH), BF16),
            pltpu.VMEM((NY * 144, KEY_DIM), BF16),
            pltpu.VMEM((NY * 144, KEY_DIM), BF16),
            pltpu.VMEM((160, KEY_DIM), BF16),
            pltpu.VMEM((160, KEY_DIM), BF16),
            pltpu.VMEM((160, KEY_DIM), BF16),
            pltpu.VMEM((NZ * 80, KEY_DIM), BF16),
            pltpu.VMEM((NY * 128, KEY_DIM), BF16),
            pltpu.VMEM((VAL_DIM, KEY_DIM), BF16),
            pltpu.VMEM((VAL_DIM, KEY_DIM), BF16),
            pltpu.VMEM((32, 256), BF16),
            pltpu.VMEM((LEN + 16, 256), F32),
            pltpu.VMEM((16, 256), BF16),
            pltpu.VMEM((16, 256), BF16),
            pltpu.VMEM((LEN, 512), BF16),
            pltpu.VMEM((16 * ROWS, WIDTH // 4), F32),
            pltpu.VMEM((16 * ROWS, WIDTH // 4), BF16),
            pltpu.VMEM((16 * ROWS, WIDTH // 4), BF16),
            pltpu.VMEM((16 * ROWS, WIDTH // 4), BF16),
            pltpu.VMEM((8 * ROWS, WIDTH // 8), BF16),
            pltpu.VMEM((8 * ROWS, WIDTH // 8), BF16),
            pltpu.VMEM((8 * ROWS, WIDTH // 4), BF16),
            pltpu.SemaphoreType.DMA((N_SEND,)),
            pltpu.SemaphoreType.DMA((N_RECV,)),
            pltpu.SemaphoreType.DMA((15,)),
        ],
        compiler_params=pltpu.CompilerParams(collective_id=0, has_side_effects=True, vmem_limit_bytes=60 * 1024 * 1024),
        cost_estimate=pl.CostEstimate(flops=3_000_000_000, bytes_accessed=1_000_000, transcendentals=0),
    )(
        tokens, norm_gain.reshape(1, -1), conv_in_weight, conv_gate_weight, conv_taps, query_weight, key_weight,
        value_weight, decay_down.T, decay_up, decay_bias.reshape(1, -1), decay_extra, head_gain.reshape(1, -1),
        conv_out_weight.T, value_out_weight.T,
    )


def solution(mesh):
    torus = Mesh(mesh.devices.reshape(NZ, NY, NX, NC), SP_TP)
    return jax.shard_map(
        local,
        mesh=torus,
        in_specs=(
            P(SP_TP, None), P(), P(SP, TP), P(SP, TP), P(), P(SP, TP), P(SP, TP), P(SP, TP),
            P(), P(), P(), P(TP, SP), P(), P(TP, SP), P(TP, SP),
        ),
        out_specs=P(SP_TP, None),
        check_vma=False,
    )
```

```python
import functools
import math

import jax
import jax.numpy as jnp
from jax import lax
from jax.experimental import pallas as pl
from jax.experimental.pallas import tpu as pltpu
from jax.sharding import Mesh
from jax.sharding import PartitionSpec as P

NZ, NY, NX, NC = 16, 4, 4, 2
KEY_DIM = 128
VAL_DIM = 256
BLOCK = 64
ROWS = 48
LEN = 384
WIDTH = 2048
EPSILON = 1e-06
SP = ("z", "y")
TP = ("x", "c")
SP_TP = ("z", "y", "x", "c")
F32 = jnp.float32
BF16 = jnp.bfloat16
MESH = pl.DeviceIdType.MESH
N_SEND = 256
N_RECV = 256


def mm(a, b):
    return lax.dot_general(a, b, (((1,), (0,)), ((), ())), preferred_element_type=F32)


def mm_nt(a, b):
    return lax.dot_general(a, b, (((1,), (1,)), ((), ())), preferred_element_type=F32)


def mm_tn(a, b):
    return lax.dot_general(a, b, (((0,), (0,)), ((), ())), preferred_element_type=F32)


def wrap(value, size):
    return lax.rem(value + size, size)


def split3(row):
    hi = row.astype(BF16)
    rest = row - hi.astype(F32)
    mid = rest.astype(BF16)
    low = (rest - mid.astype(F32)).astype(BF16)
    return hi, mid, low


def log_rows(row):
    hi, mid, low = split3(row)
    index = lax.broadcasted_iota(jnp.int32, (16, KEY_DIM), 0)
    spread = [jnp.broadcast_to(p.astype(F32), (16, KEY_DIM)) for p in (hi, mid, low)]
    out = jnp.where(index == 0, spread[0], jnp.where(index == 1, spread[1], jnp.where(index == 2, spread[2], 0.0)))
    return out.astype(BF16)


def log_total(rows16):
    return jnp.sum(rows16.astype(F32), axis=0, keepdims=True)


def kernel(
    tok_h, gain_h, ci_h, cg_h, taps_h, q_h, k_h, v_h, dd_h, du_h, db_h, de_h, hg_h, co_h, vo_h,
    out,
    tok, norm_gain, taps, ddown, dup, dbias, dextra, hgain,
    WA, WB, WC, T, SS, R1, M2, NEAR, M4, R2, M3, IF, IB, CI, CP, HP, HN, XC, PO, PS, PR, XS, XQ, XP, XR,
    ssem, rsem, lsem,
):
    z, y, x, c = (lax.axis_index(a) for a in SP_TP)
    tp = x * 2 + c
    s = z * 4 + y
    other = 1 - c
    names = {}
    sends = []

    def at(dz=0, dy=0, dx=0, flip=False):
        return (wrap(z + dz, NZ), wrap(y + dy, NY), wrap(x + dx, NX), other if flip else c)

    def sem(name):
        return rsem.at[names.setdefault(name, len(names))]

    def send(src, dst, name, device):
        copy = pltpu.make_async_remote_copy(
            src_ref=src, dst_ref=dst, send_sem=ssem.at[len(sends)], recv_sem=sem(name),
            device_id=device, device_id_type=MESH,
        )
        copy.start()
        sends.append(copy)

    def arrived(dst, name):
        pltpu.make_async_remote_copy(
            src_ref=dst, dst_ref=dst, send_sem=ssem.at[0], recv_sem=sem(name),
            device_id=(z, y, x, c), device_id_type=MESH,
        ).wait_recv()

    after = lax.rem(s + 1, NZ * NY)
    ahead = lax.rem(s + NZ * NY - 1, NZ * NY)
    next_dev = (after // NY, lax.rem(after, NY), x, c)
    prev_dev = (ahead // NY, lax.rem(ahead, NY), x, c)
    peers = [at(dz=d) for d in (1, -1, 2, -2)]
    peers += [at(dy=d) for d in range(1, NY)]
    peers += [at(dx=d) for d in range(1, NX)]
    peers += [at(flip=True), next_dev, prev_dev]
    def slot(dz=0, dy=0):
        index = wrap(z + dz, NZ) * NY + wrap(y + dy, NY)
        return pl.ds(pl.multiple_of(index * 32, 32), 32)

    def plane(dz=0):
        return pl.ds(pl.multiple_of(wrap(z + dz, NZ) * 128, 128), 128)

    def token_rows(dx=0, flip=False):
        index = wrap(x + dx, NX) * 2 + (other if flip else c)
        return pl.ds(pl.multiple_of(index * ROWS, 16), ROWS)

    loads = []

    def load(src, dst):
        copy = pltpu.make_async_copy(src, dst, lsem.at[len(loads)])
        copy.start()
        loads.append(copy)

    load(k_h, WA.at[slot(), pl.ds(0, 128)])
    load(v_h, WA.at[slot(), pl.ds(128, 256)])
    load(tok_h, tok)
    load(gain_h, norm_gain)
    barrier = pltpu.get_barrier_semaphore()
    for peer in peers:
        pl.semaphore_signal(barrier, inc=1, device_id=peer, device_id_type=MESH)
    load(q_h, WB.at[slot(), pl.ds(0, 128)])
    load(ci_h, WB.at[slot(), pl.ds(128, 256)])
    load(cg_h, WB.at[slot(), pl.ds(384, 256)])
    load(co_h, WC.at[slot(), pl.ds(0, 256)])
    load(vo_h, WC.at[slot(), pl.ds(256, 256)])
    load(dd_h, ddown)
    load(du_h, dup)
    load(db_h, dbias)
    load(de_h, dextra)
    load(taps_h, taps)
    load(hg_h, hgain)
    for copy in loads[:2]:
        copy.wait()
    pl.semaphore_wait(barrier, len(peers))

    def place(j):
        return 0 if j == 0 else (-j if j <= 8 else j - 8)

    class Ring:
        def __init__(self, W, tag, reach=8):
            self.W, self.tag, self.reach, self.passed = W, tag, reach, []

        def hop(self, chain, sign, k):
            ref = self.W.at[slot(-sign * (k - 1), 2 * chain)]
            send(ref, ref, (self.tag, chain, sign, k), at(dz=sign))

        def fan_out(self, j):
            ref = self.W.at[slot(place(j))]
            send(ref, ref, (self.tag, "ym", j), at(dy=1))
            send(ref, ref, (self.tag, "yp", j), at(dy=-1))

        def across(self):
            ref = self.W.at[slot()]
            send(ref, ref, (self.tag, "y2"), at(dy=2))

        def around(self, chain):
            if chain:
                arrived(self.W.at[slot(0, 2)], (self.tag, "y2"))
            self.hop(chain, 1, 1)
            self.hop(chain, -1, 1)

        def step(self, k, chains=(0, 1), fan=True):
            for chain in chains:
                for sign in (1, -1):
                    most = min(8 if (sign == 1) == (chain == 0) else 7, self.reach if chain else 8)
                    if k > most:
                        continue
                    arrived(self.W.at[slot(-sign * k, 2 * chain)], (self.tag, chain, sign, k))
                    if k < most:
                        self.hop(chain, sign, k + 1)
                    if chain == 0 and fan:
                        self.fan_out(k if sign == 1 else 8 + k)

        def column(self, *js):
            for j in js:
                self.passed.append(j)
                plus = (j % 2 == 0 and j < 8) if j <= 8 else ((j - 8) % 2 == 1)
                for dy, name in ((-1, "ym"), (1, "yp")):
                    ref = self.W.at[slot(place(j), dy)]
                    arrived(ref, (self.tag, name, j))
                    if plus == (dy == -1):
                        send(ref, ref, (self.tag, "y2", j), at(dy=-dy))

        def last_column(self):
            for j in range(16):
                arrived(self.W.at[slot(place(j), 2)], (self.tag, "y2", j))

        def finish(self):
            for j in range(16):
                if j in self.passed:
                    arrived(self.W.at[slot(place(j), 2)], (self.tag, "y2", j))
                else:
                    arrived(self.W.at[slot(place(j), -1)], (self.tag, "ym", j))
                    arrived(self.W.at[slot(place(j), 1)], (self.tag, "yp", j))

    class Jumps(Ring):
        def leap(self, sign, base):
            ref = self.W.at[slot(-sign * base)]
            for d in (2, 1):
                if base + d <= (8 if sign == 1 else 7):
                    send(ref, ref, (self.tag, 0, sign, base + d), at(dz=sign * d))

        def stage(self, i):
            for d in (2, 1):
                for sign in (1, -1):
                    k = 2 * i - 2 + d
                    if k > (8 if sign == 1 else 7):
                        continue
                    arrived(self.W.at[slot(-sign * k)], (self.tag, 0, sign, k))
                    if d == 2:
                        self.leap(sign, k)
                    self.fan_out(k if sign == 1 else 8 + k)

    ring_a, ring_b, ring_c = Jumps(WA, "a"), Ring(WB, "b"), Ring(WC, "c", reach=3)
    ring_a.leap(1, 0)
    ring_a.leap(-1, 0)
    ring_a.fan_out(0)
    for copy in loads[2:]:
        copy.wait()
    raw_rows = tok[...].astype(F32)
    scale = lax.rsqrt(jnp.mean(raw_rows * raw_rows, axis=-1, keepdims=True) + EPSILON)
    T[token_rows(), :] = (raw_rows * scale * norm_gain[...]).astype(BF16)
    own_rows = T.at[token_rows()]
    send(own_rows, own_rows, "tm", at(dx=1))
    send(own_rows, own_rows, "tp", at(dx=-1))
    send(own_rows, own_rows, ("tc", 0), at(flip=True))
    ring_b.across()
    ring_b.around(0)
    ring_c.across()
    ring_c.around(0)
    ring_b.fan_out(0)

    def weights_step(k, fan=True):
        if k <= 8:
            ring_b.step(k, (0,))
            ring_c.step(k, (0,), fan=fan)
        if k == 1:
            ring_b.around(1)
            ring_c.around(1)
        else:
            ring_b.step(k - 1, (1,))
            ring_c.step(k - 1, (1,))

    def late_fan(*js):
        for j in js:
            ring_c.fan_out(j)

    half = WIDTH // 2
    blocks = LEN // BLOCK
    key_cols = pl.ds(pl.multiple_of(tp * KEY_DIM, KEY_DIM), KEY_DIM)
    val_cols = pl.ds(pl.multiple_of(tp * VAL_DIM, VAL_DIM), VAL_DIM)

    def token_step(stage):
        if stage == 0:
            ref = T.at[token_rows(dx=-1)]
            arrived(ref, "tm")
            piece = T.at[token_rows(dx=-1), pl.ds(0, half)]
            send(piece, piece, "t2a", at(dx=1))
            send(ref, ref, ("tc", 1), at(flip=True))
            ref = T.at[token_rows(dx=1)]
            arrived(ref, "tp")
            piece = T.at[token_rows(dx=1), pl.ds(half, half)]
            send(piece, piece, "t2b", at(dx=-1))
            send(ref, ref, ("tc", 2), at(flip=True))
        elif stage == 1:
            arrived(T.at[token_rows(dx=2), pl.ds(0, half)], "t2a")
            arrived(T.at[token_rows(dx=2), pl.ds(half, half)], "t2b")
            ref = T.at[token_rows(dx=2)]
            send(ref, ref, ("tc", 3), at(flip=True))
        else:
            for j in range(4):
                arrived(T.at[token_rows(dx=(0, -1, 1, 2)[j], flip=True)], ("tc", j))

    def part(array, n):
        return array[n * BLOCK : (n + 1) * BLOCK]

    def decay():
        low = mm_nt(T[0:LEN, :], ddown[...]).astype(BF16)
        pre = mm(low, dup[:, key_cols]) + dbias[:, key_cols]
        log_sig = jnp.minimum(pre, 0.0) - jnp.log1p(jnp.exp(-jnp.abs(pre)))
        extra = jnp.transpose(jnp.broadcast_to(dextra[...], (KEY_DIM, LEN)))
        log_decay = log_sig / 16.0 + extra
        ri = lax.broadcasted_iota(jnp.int32, (LEN, LEN), 0)
        ci = lax.broadcasted_iota(jnp.int32, (LEN, LEN), 1)
        tri = jnp.where((ri >= ci) & (ri // BLOCK == ci // BLOCK), 1.0, 0.0).astype(F32)
        cumul = lax.dot_general(
            tri, log_decay, (((1,), (0,)), ((), ())), precision=lax.Precision.HIGHEST, preferred_element_type=F32
        )
        return cumul, cumul - log_decay

    ring_a.stage(1)
    ring_a.column(0)
    weights_step(1, fan=False)
    token_step(0)
    ring_a.stage(2)
    ring_a.column(1, 9)
    weights_step(2, fan=False)
    ring_a.column(2, 10)
    ring_a.stage(3)
    ring_a.column(3, 11)
    token_step(1)
    weights_step(3, fan=False)
    ring_a.column(4, 12)
    ring_a.stage(4)
    ring_a.column(5, 13)
    token_step(2)
    for name, device, edge, at_row in (("hp", next_dev, LEN - 16, 15), ("hn", prev_dev, 0, 0)):
        rows = T[edge : edge + 16, :].astype(F32)[at_row : at_row + 1]
        arow = lax.broadcasted_iota(jnp.int32, (16, 256), 0)
        spread = jnp.zeros((16, 256), F32)
        for i in range(8):
            spread = jnp.where(arow == i, rows[:, i * 256 : (i + 1) * 256], spread)
        to = pl.ds(16 if at_row == 0 else 0, 16)
        CI[to, :] = spread.astype(BF16)
        send(CI.at[to], HN if at_row == 0 else HP, name, device)
    cumul, before = decay()
    totals = [cumul[(n + 1) * BLOCK - 1 : (n + 1) * BLOCK] for n in range(blocks)]
    offsets = [jnp.zeros((1, KEY_DIM), F32)]
    for n in range(blocks):
        offsets.append(offsets[-1] + totals[n])
    whole = offsets[blocks]
    suffix = [jnp.zeros((1, KEY_DIM), F32)]
    for n in reversed(range(blocks)):
        suffix.append(suffix[-1] + totals[n])
    suffix = suffix[::-1][1:]
    to_end = jnp.concatenate([suffix[n] + totals[n] - part(cumul, n) for n in range(blocks)], axis=0)
    from_start = jnp.concatenate([offsets[n] + part(before, n) for n in range(blocks)], axis=0)
    to_end, from_start = jnp.exp(to_end), jnp.exp(from_start)
    marks = log_rows(whole)
    weights_step(4, fan=False)
    ring_a.column(6, 14)
    ring_a.column(7, 15, 8)
    weights_step(5, fan=False)
    ring_a.last_column()

    normed = T[0:LEN, :]
    kv = mm(normed, WA[...])
    key_f = kv[:, :KEY_DIM].astype(BF16).astype(F32)
    value = kv[:, KEY_DIM:].astype(BF16)
    fwd_device = mm_tn(value, (key_f * to_end).astype(BF16))
    back_device = mm_tn(value, (key_f * from_start).astype(BF16))

    for q in range(NY):
        SS[q * 144 : q * 144 + 64, :] = fwd_device[q * 64 : q * 64 + 64].astype(BF16)
        SS[q * 144 + 64 : q * 144 + 128, :] = back_device[q * 64 : q * 64 + 64].astype(BF16)
        SS[q * 144 + 128 : q * 144 + 144, :] = marks

    def message(dy=0):
        return pl.ds(pl.multiple_of(wrap(y + dy, NY) * 144, 16), 144)

    R1[message(), :] = SS[message(), :]
    for d in range(1, NY):
        send(SS.at[message(d)], R1.at[message()], ("s1", d), at(dy=d))

    late_fan(4, 12, 5, 13)
    weights_step(6)
    for d in range(1, NY):
        arrived(R1.at[message(-d)], ("s1", d))
    in_f, in_b, in_l = [], [], []
    for q in range(NY):
        in_f.append(R1[q * 144 : q * 144 + 64, :].astype(F32))
        in_b.append(R1[q * 144 + 64 : q * 144 + 128, :].astype(F32))
        in_l.append(log_total(R1[q * 144 + 128 : q * 144 + 144, :]))
    total_f = jnp.zeros((64, KEY_DIM), F32)
    total_b = jnp.zeros((64, KEY_DIM), F32)
    log_f = jnp.zeros((1, KEY_DIM), F32)
    log_b = jnp.zeros((1, KEY_DIM), F32)
    plane_f, plane_b, gap_f, gap_b = ([None] * NY for _ in range(4))
    for q in range(NY):
        plane_f[q], gap_f[q] = total_f, log_f
        total_f = jnp.exp(in_l[q]) * total_f + in_f[q]
        log_f = log_f + in_l[q]
    for q in reversed(range(NY)):
        plane_b[q], gap_b[q] = total_b, log_b
        total_b = jnp.exp(in_l[q]) * total_b + in_b[q]
        log_b = log_b + in_l[q]
    marks = log_rows(log_f)
    M2[0:64, :] = total_f.astype(BF16)
    M2[64:80, :] = marks
    M2[80:144, :] = total_b.astype(BF16)
    M2[144:160, :] = marks

    def depth(dz=0):
        return pl.ds(pl.multiple_of(wrap(z + dz, NZ) * 80, 16), 80)

    R2[depth(), :] = M2[0:80, :]
    send(M2.at[pl.ds(0, 80)], NEAR.at[pl.ds(0, 80)], "s2f", at(dz=1))
    send(M2.at[pl.ds(80, 80)], NEAR.at[pl.ds(80, 80)], "s2b", at(dz=-1))
    late_fan(0, 1, 9)
    weights_step(7)
    arrived(NEAR.at[pl.ds(0, 80)], "s2f")
    arrived(NEAR.at[pl.ds(80, 80)], "s2b")
    near_f = jnp.where(z > 0, NEAR[0:64, :].astype(F32), 0.0)
    near_b = jnp.where(z < NZ - 1, NEAR[80:144, :].astype(F32), 0.0)
    near_lf, near_lb = log_total(NEAR[64:80, :]), log_total(NEAR[144:160, :])
    fade = jnp.exp(log_f)
    M4[0:64, :] = (total_f + fade * near_f).astype(BF16)
    M4[64:80, :] = log_rows(log_f + near_lf)
    M4[80:144, :] = (total_b + fade * near_b).astype(BF16)
    M4[144:160, :] = log_rows(log_f + near_lb)
    for d in (8, 6, 10, 4, 12, 2, 14):
        start = pl.multiple_of(((z + d) // NZ) * 80, 16)
        send(M4.at[pl.ds(start, 80)], R2.at[depth()], ("s2", d), at(dz=d))

    late_fan(2, 10)
    weights_step(8)
    ring_c.column(4, 12, 5, 13)
    late_fan(3, 11)
    weights_step(9)
    ring_c.column(6, 14, 7, 15)
    for d in range(2, NZ, 2):
        arrived(R2.at[depth(-d)], ("s2", d))
    sum_f = jnp.zeros((64, KEY_DIM), F32)
    sum_b = jnp.zeros((64, KEY_DIM), F32)
    for d in range(NZ - 2, 0, -2):
        got = R2[depth(-d), :]
        step = jnp.exp(log_total(got[64:80])) * sum_f + got[0:64].astype(F32)
        sum_f = jnp.where(z >= d, step, sum_f)
        got = R2[depth(d), :]
        step = jnp.exp(log_total(got[64:80])) * sum_b + got[0:64].astype(F32)
        sum_b = jnp.where(z + d < NZ, step, sum_b)
    sum_f = jnp.where(z > 0, jnp.exp(near_lf) * sum_f + near_f, 0.0)
    sum_b = jnp.where(z < NZ - 1, jnp.exp(near_lb) * sum_b + near_b, 0.0)
    for q in range(NY):
        M3[q * 128 : q * 128 + 64, :] = (plane_f[q] + jnp.exp(gap_f[q]) * sum_f).astype(BF16)
        M3[q * 128 + 64 : q * 128 + 128, :] = (plane_b[q] + jnp.exp(gap_b[q]) * sum_b).astype(BF16)

    def quarter(dy=0):
        return pl.ds(pl.multiple_of(wrap(y + dy, NY) * 64, 64), 64)

    def answer(dy, which):
        return pl.ds(pl.multiple_of(wrap(y + dy, NY) * 128 + 64 * which, 64), 64)

    for d in range(1, NY):
        send(M3.at[answer(d, 0)], IF.at[quarter()], ("s3f", d), at(dy=d))
        send(M3.at[answer(d, 1)], IB.at[quarter()], ("s3b", d), at(dy=d))
    IF[quarter(), :] = M3[answer(0, 0), :]
    IB[quarter(), :] = M3[answer(0, 1), :]
    ring_c.column(8)
    ring_b.finish()
    arrived(HP, "hp")
    arrived(HN, "hn")
    for i in range(8):
        seg = pl.ds(i * 256, 256)
        arow = lax.broadcasted_iota(jnp.int32, (16, 256), 0)
        row_p = jnp.where(s > 0, HP[i : i + 1, :].astype(F32), 0.0)
        row_n = jnp.where(s < NZ * NY - 1, HN[i : i + 1, :].astype(F32), 0.0)
        T[pl.ds(LEN, 16), seg] = jnp.where(arow == 0, row_p, jnp.where(arow == 1, row_n, 0.0)).astype(BF16)
    conv_in = mm(T[...], WB[:, 128:384]).astype(BF16).astype(F32)
    CP[8 : 8 + LEN, :] = conv_in[:LEN]
    CP[7:8, :] = conv_in[LEN : LEN + 1]
    CP[8 + LEN : 9 + LEN, :] = conv_in[LEN + 1 : LEN + 2]
    query_f = (mm(normed, WB[:, 0:128]) * (1.0 / math.sqrt(KEY_DIM))).astype(BF16).astype(F32)
    gate = mm(normed, WB[:, 384:640]).astype(BF16).astype(F32)
    lower = lax.broadcasted_iota(jnp.int32, (BLOCK, BLOCK), 0) >= lax.broadcasted_iota(jnp.int32, (BLOCK, BLOCK), 1)
    upper = lax.broadcasted_iota(jnp.int32, (BLOCK, BLOCK), 0) <= lax.broadcasted_iota(jnp.int32, (BLOCK, BLOCK), 1)
    within = []
    fwd_inc, back_inc, fwd_query, back_query = [], [], [], []
    for n in range(blocks):
        cum_n, bef_n, key_n, query_n, value_n = (part(a, n) for a in (cumul, before, key_f, query_f, value))
        fq = (query_n * jnp.exp(cum_n)).astype(BF16)
        ks = (key_n * jnp.exp(bef_n)).astype(BF16)
        fwd_scores = mm_nt(fq, (key_n * jnp.exp(-cum_n)).astype(BF16))
        back_scores = mm_nt((query_n * jnp.exp(-bef_n)).astype(BF16), ks)
        scores = jnp.where(lower, fwd_scores, 0.0) + jnp.where(upper, back_scores, 0.0)
        within.append(mm(scores.astype(BF16), value_n))
        fwd_inc.append(mm_tn(value_n, (key_n * jnp.exp(totals[n] - cum_n)).astype(BF16)))
        back_inc.append(mm_tn(value_n, ks))
        fwd_query.append(fq)
        back_query.append((query_n * jnp.exp(totals[n] - bef_n)).astype(BF16))
    state = fwd_inc[0]
    for n in range(1, blocks):
        within[n] = within[n] + mm_nt(fwd_query[n], state.astype(BF16))
        state = jnp.exp(totals[n]) * state + fwd_inc[n]
    state = back_inc[blocks - 1]
    for n in reversed(range(blocks - 1)):
        within[n] = within[n] + mm_nt(back_query[n], state.astype(BF16))
        state = jnp.exp(totals[n]) * state + back_inc[n]
    local = jnp.concatenate(within, axis=0)
    far_fwd = jnp.concatenate(
        [part(query_f, n) * jnp.exp(offsets[n] + part(cumul, n)) for n in range(blocks)], axis=0
    ).astype(BF16)
    far_back = jnp.concatenate(
        [part(query_f, n) * jnp.exp(suffix[n] + (totals[n] - part(before, n))) for n in range(blocks)], axis=0
    ).astype(BF16)

    tap = taps[:, val_cols]
    mixed = CP[7 : 7 + LEN, :] * tap[0:1] + CP[8 : 8 + LEN, :] * tap[1:2] + CP[9 : 9 + LEN, :] * tap[2:3]
    XC[:, 0:256] = (mixed * (gate * (1.0 / (1.0 + jnp.exp(-gate))))).astype(BF16)

    early = len(sends) - 6
    for copy in sends[:early]:
        copy.wait_send()
    for d in range(1, NY):
        arrived(IF.at[quarter(-d)], ("s3f", d))
        arrived(IB.at[quarter(-d)], ("s3b", d))
    raw = local + mm_nt(far_fwd, IF[...]) + mm_nt(far_back, IB[...])
    norm = lax.rsqrt(jnp.mean(raw * raw, axis=-1, keepdims=True) + EPSILON)
    XC[:, 256:512] = (raw * norm * hgain[:, val_cols]).astype(BF16)
    ring_c.finish()

    order = (2, 1, 3, 0)
    pieces, piece = 4, WIDTH // 4
    there = jnp.concatenate([XC[token_rows(dx=r, flip=True), :] for r in order], axis=0)
    here = jnp.concatenate([XC[token_rows(dx=r), :] for r in order], axis=0)

    def rows4(n, i=0, count=4):
        return pl.ds((n * 4 + i) * ROWS, count * ROWS)

    def pair_send(n):
        PS[rows4(n), :] = mm_nt(there, WC[n * piece : (n + 1) * piece, :]).astype(BF16)
        send(PS.at[rows4(n)], PR.at[rows4(n)], ("pr", n), at(flip=True))

    side = piece // 2
    near, far_side = pl.ds(0, side), pl.ds(side, side)

    def keep(n):
        PO[rows4(n), :] = mm_nt(here, WC[n * piece : (n + 1) * piece, :])

    def x_send(n):
        arrived(PR.at[rows4(n)], ("pr", n))
        both = PO[rows4(n), :] + PR[rows4(n), :].astype(F32)
        XS[rows4(n), :] = both.astype(BF16)
        send(XS.at[rows4(n, 0, 1), near], XQ.at[rows2(n, 0)], ("xq", n, 0), at(dx=1))
        send(XS.at[rows4(n, 0, 1), far_side], XQ.at[rows2(n, 1)], ("xq", n, 1), at(dx=-1))
        PO[rows4(n, 1, 3), :] = both[ROWS:]

    def x_direct(n):
        send(XS.at[rows4(n, 1, 1), far_side], XR.at[rows2(n, 0), far_side], ("xr", n, 0), at(dx=1))
        send(XS.at[rows4(n, 2, 1), near], XR.at[rows2(n, 1), near], ("xr", n, 1), at(dx=-1))

    def rows2(n, i):
        return pl.ds((n * 2 + i) * ROWS, ROWS)

    def x_pass(n):
        base = (n * 4 + 1) * ROWS
        arrived(XQ.at[rows2(n, 0)], ("xq", n, 0))
        XP[rows2(n, 0), :] = (PO[base : base + ROWS, 0:side] + XQ[rows2(n, 0), :].astype(F32)).astype(BF16)
        send(XP.at[rows2(n, 0)], XR.at[rows2(n, 0), near], ("xs", n, 0), at(dx=1))
        arrived(XQ.at[rows2(n, 1)], ("xq", n, 1))
        XP[rows2(n, 1), :] = (PO[base + ROWS : base + 2 * ROWS, side:] + XQ[rows2(n, 1), :].astype(F32)).astype(BF16)
        send(XP.at[rows2(n, 1)], XR.at[rows2(n, 1), far_side], ("xs", n, 1), at(dx=-1))

    for n in range(pieces):
        pair_send(n)
    for n in range(pieces):
        keep(n)
    for n in range(pieces):
        x_send(n)
    for n in range(pieces):
        x_direct(n)
    for n in range(pieces):
        x_pass(n)
    for n in range(pieces):
        total = PO[rows4(n, 3, 1), :]
        arrived(XR.at[rows2(n, 0), far_side], ("xr", n, 0))
        arrived(XR.at[rows2(n, 1), near], ("xr", n, 1))
        arrived(XR.at[rows2(n, 0), near], ("xs", n, 0))
        arrived(XR.at[rows2(n, 1), far_side], ("xs", n, 1))
        total = total + XR[rows2(n, 0), :].astype(F32) + XR[rows2(n, 1), :].astype(F32)
        out[:, n * piece : (n + 1) * piece] = total.astype(BF16)

    for copy in sends[early:]:
        copy.wait_send()
    assert len(sends) <= N_SEND and len(names) <= N_RECV, (len(sends), len(names))


def local(
    tokens, norm_gain, conv_in_weight, conv_gate_weight, conv_taps, query_weight, key_weight, value_weight,
    decay_down, decay_up, decay_bias, decay_extra, head_gain, conv_out_weight, value_out_weight,
):
    hbm = pl.BlockSpec(memory_space=pl.ANY)
    return pl.pallas_call(
        kernel,
        out_shape=pltpu.VMEM((ROWS, WIDTH), BF16),
        in_specs=[hbm] * 15,
        out_specs=pl.BlockSpec(memory_space=pltpu.VMEM),
        scratch_shapes=[
            pltpu.VMEM((ROWS, WIDTH), BF16),
            pltpu.VMEM((1, WIDTH), F32),
            pltpu.VMEM((3, WIDTH), F32),
            pltpu.VMEM((16, WIDTH), BF16),
            pltpu.VMEM((16, 1024), BF16),
            pltpu.VMEM((1, 1024), F32),
            pltpu.VMEM((1, LEN), F32),
            pltpu.VMEM((1, WIDTH), F32),
            pltpu.VMEM((2048, 384), BF16),
            pltpu.VMEM((2048, 640), BF16),
            pltpu.VMEM((2048, 512), BF16),
            pltpu.VMEM((LEN + 16, WIDTH), BF16),
            pltpu.VMEM((NY * 144, KEY_DIM), BF16),
            pltpu.VMEM((NY * 144, KEY_DIM), BF16),
            pltpu.VMEM((160, KEY_DIM), BF16),
            pltpu.VMEM((160, KEY_DIM), BF16),
            pltpu.VMEM((160, KEY_DIM), BF16),
            pltpu.VMEM((NZ * 80, KEY_DIM), BF16),
            pltpu.VMEM((NY * 128, KEY_DIM), BF16),
            pltpu.VMEM((VAL_DIM, KEY_DIM), BF16),
            pltpu.VMEM((VAL_DIM, KEY_DIM), BF16),
            pltpu.VMEM((32, 256), BF16),
            pltpu.VMEM((LEN + 16, 256), F32),
            pltpu.VMEM((16, 256), BF16),
            pltpu.VMEM((16, 256), BF16),
            pltpu.VMEM((LEN, 512), BF16),
            pltpu.VMEM((16 * ROWS, WIDTH // 4), F32),
            pltpu.VMEM((16 * ROWS, WIDTH // 4), BF16),
            pltpu.VMEM((16 * ROWS, WIDTH // 4), BF16),
            pltpu.VMEM((16 * ROWS, WIDTH // 4), BF16),
            pltpu.VMEM((8 * ROWS, WIDTH // 8), BF16),
            pltpu.VMEM((8 * ROWS, WIDTH // 8), BF16),
            pltpu.VMEM((8 * ROWS, WIDTH // 4), BF16),
            pltpu.SemaphoreType.DMA((N_SEND,)),
            pltpu.SemaphoreType.DMA((N_RECV,)),
            pltpu.SemaphoreType.DMA((15,)),
        ],
        compiler_params=pltpu.CompilerParams(collective_id=0, has_side_effects=True, vmem_limit_bytes=60 * 1024 * 1024),
        cost_estimate=pl.CostEstimate(flops=3_000_000_000, bytes_accessed=1_000_000, transcendentals=0),
    )(
        tokens, norm_gain.reshape(1, -1), conv_in_weight, conv_gate_weight, conv_taps, query_weight, key_weight,
        value_weight, decay_down.T, decay_up, decay_bias.reshape(1, -1), decay_extra, head_gain.reshape(1, -1),
        conv_out_weight.T, value_out_weight.T,
    )


def solution(mesh):
    torus = Mesh(mesh.devices.reshape(NZ, NY, NX, NC), SP_TP)
    return jax.shard_map(
        local,
        mesh=torus,
        in_specs=(
            P(SP_TP, None), P(), P(SP, TP), P(SP, TP), P(), P(SP, TP), P(SP, TP), P(SP, TP),
            P(), P(), P(), P(TP, SP), P(), P(TP, SP), P(TP, SP),
        ),
        out_specs=P(SP_TP, None),
        check_vma=False,
    )
```
